32 devices in a mesh: ep: 8 (over z, x), tp: 4 (over y, core).
Axes of the slice: x: 2, y: 2, z: 4, core: 2. Of those that a mesh axis runs over, the one named last changes fastest.
Arguments:
- resid: bfloat16 [256, 2048], P('ep'), may hold values from -6 to 6
- norm_gain: bfloat16 [2048], replicated, may hold values from 0.099609375 to 1.8984375
- w_query: bfloat16 [2048, 1024], P(None, 'tp'), may hold values from -0.125 to 0.125
- w_key: bfloat16 [2048, 1024], P(None, 'tp'), may hold values from -0.125 to 0.125
- w_value: bfloat16 [2048, 1024], P(None, 'tp'), may hold values from -0.125 to 0.125
- w_gate: bfloat16 [2048, 1024], P(None, 'tp'), may hold values from -0.125 to 0.125
- head_gain: bfloat16 [1024], P('tp'), may hold values from 0.099609375 to 1.8984375
- w_output: bfloat16 [1024, 2048], P('tp'), may hold values from -0.1875 to 0.1875
- state: float32 [256, 8, 128, 128], P('ep', 'tp'), may hold values from -0.6 to 0.6
- positions: int32 [256], P('ep'), may hold values from 1024 to 8191
- ffn_gain: bfloat16 [2048], replicated, may hold values from 0.099609375 to 1.8984375
- w_mix: bfloat16 [2048], replicated, may hold values from -0.125 to 0.125
- dense_gate: bfloat16 [2048, 5632], P('tp', 'ep'), may hold values from -0.125 to 0.125
- dense_up: bfloat16 [2048, 5632], P('tp', 'ep'), may hold values from -0.125 to 0.125
- dense_down: bfloat16 [5632, 2048], P('ep', 'tp'), may hold values from -0.109375 to 0.109375
- routes: int32 [256, 2], P('ep'), may hold values from 0 to 7, all different within a row; in each aligned block of 32 rows (0 to 31, 32 to 63, ...) at most 16 rows name the same one
- route_weight: bfloat16 [256, 2], P('ep'), may hold values from 0.19921875 to 1
- expert_gate: bfloat16 [8, 2048, 4096], P('ep', None, 'tp'), may hold values from -0.125 to 0.125
- expert_up: bfloat16 [8, 2048, 4096], P('ep', None, 'tp'), may hold values from -0.125 to 0.125
- expert_down: bfloat16 [8, 4096, 2048], P('ep', 'tp'), may hold values from -0.09375 to 0.09375
Outputs:
- final: bfloat16 [256, 2048], P('ep', 'tp')
- new_state: float32 [256, 8, 128, 128], P('ep', 'tp')
The draws below stay inside these ranges and needn't reach their ends.
Inputs may be any that keep to these rules, and one draw needn't show every extreme that they name: `routes`: each row names 2 different experts; in the rows of one index of ep no expert is named by more than 16 rows, a bound that some block reaches; every expert is named by some row.
All inputs are finite; a program needn't handle non-finite values.
Results may differ from the reference program's by a relative error of at most 0.018.
Values may be sent and summed in bfloat16 or wider, within the bound.
A program may use at most 64 MiB of HBM per device.

```python
import math
import jax
import jax.numpy as jnp
import numpy as np
from jax import lax

D = 2048
RET_HEADS = 8
HEAD_DIM = 128
RET_W = 1024
FFD = 5632
FFE = 4096
TOPK = 2
SEQ_DEV = 32
SEQS = 256
EXPERTS = 8
CAP = 16
N_EP = 8
N_TP = 4


def place_ends(values, key, low, top_value):
    place = [jax.random.randint(jax.random.fold_in(key, axis), (), 0, length) for axis, length in enumerate(values.shape)]
    longest = values.shape.index(max(values.shape))
    neighbour = place[:longest] + [(place[longest] + 1) % values.shape[longest]] + place[longest + 1:]
    return values.at[tuple(place)].set(low).at[tuple(neighbour)].set(top_value)


def with_spikes(entries, own_key, source, target, parts, factor):
    def block_of(axis_at):
        return (jnp.arange(entries.shape[axis_at]) // (entries.shape[axis_at] // parts)).reshape((-1,) + (1,) * (entries.ndim - 1 - axis_at))

    near = jax.random.permutation(own_key, parts)[block_of(target)]
    far = (block_of(target) + parts // 2) % parts
    return jnp.where((block_of(source) == near) | (block_of(source) == far), factor * entries, entries)


def level_of(rng, dims, shards, low, top_value):
    factor_of = 1.0
    for dim, parts in shards:
        draws = jax.random.uniform(jax.random.fold_in(jax.random.fold_in(rng, 6), dim), (parts,), jnp.float32, low / len(shards), top_value / len(shards))
        factor_of = factor_of * jnp.repeat(jnp.exp(draws), dims[dim] // parts).reshape((-1,) + (1,) * (len(dims) - 1 - dim))
    return factor_of


def shared_out(rng, own, number, rows, count, top, bound, lean):
    sequence = jax.random.permutation(rng, count)
    heavy_load, usual = load_shares(count, rows * top, bound, lean, True), load_shares(count, rows * top, bound, lean, False)
    places = jnp.arange(count)

    def named(tallies, offset_by):
        used = int((tallies > 0).sum())
        fixed = max(1, used // 4)
        moved = fixed + (places - fixed + offset_by * (used - fixed)) % max(1, count - fixed)
        return jnp.zeros((count,), jnp.int32).at[sequence[jnp.where(places < fixed, places, moved)]].set(jnp.asarray(tallies, jnp.int32))

    tallies = jnp.where(number % 4 == 0, named(heavy_load, number // 4), named(usual, number - number // 4 - 1))
    mixed = jax.random.permutation(jax.random.fold_in(own, 3), count)
    source_of, receiver = mixed[0:count // 2 * 2:2], mixed[1:count // 2 * 2:2]
    margin = jnp.minimum(tallies[source_of] - 1, bound - tallies[receiver]) // 2
    margin = jnp.where((source_of == sequence[0]) | (receiver == sequence[0]) | (tallies[receiver] == 0), 0, jnp.maximum(margin, 0))
    moved = jax.random.randint(jax.random.fold_in(own, 4), (count // 2,), 0, 1 << 20) % (margin + 1)
    tallies = tallies.at[source_of].add(-moved).at[receiver].add(moved)
    labels = jnp.searchsorted(jnp.cumsum(tallies), jnp.arange(rows * top), side="right").astype(jnp.int32)
    grid = labels.reshape(top, rows).T
    grid = grid[jax.random.permutation(jax.random.fold_in(own, 1), rows)]
    offset_by = jax.random.randint(jax.random.fold_in(own, 2), (rows, 1), 0, top)
    return jnp.take_along_axis(grid, (jnp.arange(top)[None, :] + offset_by) % top, axis=1)


def load_shares(number_of, total, limit, skew, full):
    portions = [(1 << 20) // math.isqrt(rank ** skew) + 1 for rank in range(1, number_of + 1)]
    largest = limit if full else min(limit, max(-(-total // number_of), total * portions[0] // sum(portions)))
    least = 1 if total - largest >= number_of - 1 else 0
    given, rest = [largest] + [least] * (number_of - 1), total - largest - least * (number_of - 1)
    while rest > 0:
        free = [i for i in range(1, number_of) if given[i] < largest] or [i for i in range(1, number_of) if given[i] < limit]
        mass, remaining = sum([portions[i] for i in free]), rest
        for i in free:
            extra = min(limit - given[i], max(1, remaining * portions[i] // mass), rest)
            given[i] = given[i] + extra
            rest = rest - extra
    return np.array(given)


def scatter_about(stream_key, dims, deviation, limit, cuts=(), held_as=jnp.bfloat16):
    values = jax.random.normal(stream_key, dims, jnp.float32) * deviation
    if len(cuts) > 0:
        values = level_of(stream_key, dims, cuts, -0.22, 0.18) * values
    return jnp.clip(values, min=-limit, max=limit).astype(held_as)


def heavy_noise(own_key, dims, scale, most, cuts, heavy, kind=jnp.bfloat16):
    values = scale * jax.random.normal(own_key, dims, jnp.float32)
    if cuts:
        values = values * level_of(own_key, dims, cuts, -0.22, 0.18)
    return jnp.clip(with_spikes(values, jax.random.fold_in(own_key, 3), *heavy), -most, most).astype(kind)


def setup_inputs(seed: int = 0) -> dict:
    splits = jax.random.split(jax.random.key(seed), 21)
    resid = scatter_about(splits[0], (SEQS, D), 1.0, 6.0, ((0, 8),))
    norm_gain = jnp.clip(1.0 + 0.18 * jax.random.normal(splits[1], (D,), jnp.float32), 0.099609375, 1.8984375).astype(jnp.bfloat16)
    w_query = scatter_about(splits[2], (D, RET_W), D ** -0.5, 0.125, ((1, 4),))
    w_key = scatter_about(splits[3], (D, RET_W), D ** -0.5, 0.125, ((1, 4),))
    w_value = scatter_about(splits[4], (D, RET_W), D ** -0.5, 0.125, ((1, 4),))
    w_gate = scatter_about(splits[5], (D, RET_W), D ** -0.5, 0.125, ((1, 4),))
    head_gain = jnp.clip(1.0 + 0.18 * jax.random.normal(splits[6], (RET_W,), jnp.float32), 0.099609375, 1.8984375).astype(jnp.bfloat16)
    w_output = scatter_about(splits[7], (RET_W, D), RET_W ** -0.5, 0.1875, ((0, 4),))
    state = scatter_about(splits[8], (SEQS, RET_HEADS, HEAD_DIM, HEAD_DIM), 0.1, 0.6, ((0, 8), (1, 4)), jnp.float32)
    positions = place_ends(jax.random.randint(splits[9], (SEQS,), 1024, 8192), jax.random.fold_in(splits[9], 1), 1024, 8191).astype(jnp.int32)
    ffn_gain = jnp.clip(1.0 + 0.18 * jax.random.normal(splits[10], (D,), jnp.float32), 0.099609375, 1.8984375).astype(jnp.bfloat16)
    w_mix = scatter_about(splits[11], (D,), D ** -0.5, 0.125)
    dense_gate = scatter_about(splits[12], (D, FFD), D ** -0.5, 0.125, ((0, 4), (1, 8)))
    dense_up = scatter_about(splits[13], (D, FFD), D ** -0.5, 0.125, ((0, 4), (1, 8)))
    dense_down = heavy_noise(splits[14], (FFD, D), FFD ** -0.5, 0.109375, ((0, 8), (1, 4)), (0, 1, 8, 2.0))
    routes_keys = jax.random.split(jax.random.fold_in(splits[15], 1), SEQS // SEQ_DEV)
    routes_turns = jax.random.permutation(jax.random.fold_in(splits[15], 3), SEQS // SEQ_DEV)
    routes = jax.vmap(lambda own, number: shared_out(jax.random.fold_in(splits[15], 2), own, number, SEQ_DEV, EXPERTS, TOPK, CAP, 2))(routes_keys, routes_turns).reshape((SEQS, TOPK))
    route_weight = jnp.clip(0.19921875 + 0.80078125 * jax.random.uniform(splits[16], (SEQS, TOPK), jnp.float32) ** level_of(splits[16], (SEQS, TOPK), ((0, 8),), -0.2, 0.2), 0.19921875, 1.0).astype(jnp.bfloat16)
    expert_gate = scatter_about(splits[17], (EXPERTS, D, FFE), D ** -0.5, 0.125, ((0, 8), (2, 4)))
    expert_up = scatter_about(splits[18], (EXPERTS, D, FFE), D ** -0.5, 0.125, ((0, 8), (2, 4)))
    expert_down = scatter_about(splits[19], (EXPERTS, FFE, D), FFE ** -0.5, 0.09375, ((0, 8), (1, 4)))
    return dict(resid=resid, norm_gain=norm_gain, w_query=w_query, w_key=w_key, w_value=w_value, w_gate=w_gate, head_gain=head_gain, w_output=w_output, state=state, positions=positions, ffn_gain=ffn_gain, w_mix=w_mix, dense_gate=dense_gate, dense_up=dense_up, dense_down=dense_down, routes=routes, route_weight=route_weight, expert_gate=expert_gate, expert_up=expert_up, expert_down=expert_down)


EPSILON = 1e-06
THETA = 10000.0

def rms_norm(inputs, scaling):
    square = lax.optimization_barrier(jnp.mean(inputs * inputs, axis=-1, keepdims=True))
    return inputs * lax.rsqrt(square + EPSILON) * scaling.astype(jnp.float32)

def rounded(partial_value):
    return lax.optimization_barrier(partial_value.astype(jnp.bfloat16)).astype(jnp.float32)

def rotate(inputs, places):
    halfway = inputs.shape[-1] // 2
    inverse = THETA ** (-jnp.arange(halfway, dtype=jnp.float32) / halfway)
    angles = places.astype(jnp.float32)[:, None] * inverse[None, :]
    cosine = jnp.cos(angles)[:, None, :]
    sine_of = jnp.sin(angles)[:, None, :]
    former = inputs[..., :halfway]
    latter = inputs[..., halfway:]
    return jnp.concatenate([former * cosine - latter * sine_of, former * sine_of + latter * cosine], axis=-1)

def retain(queries, keys_in, values_in, gating, memory, places, head_first, head_gain):
    seqs_here = queries.shape[0]
    heads_here = memory.shape[1]
    head_size = memory.shape[2]
    head_shape = (seqs_here, heads_here, head_size)
    query_rot = rotate(queries.astype(jnp.float32).reshape(head_shape), places)
    key_rot = rotate(keys_in.astype(jnp.float32).reshape(head_shape), places) * head_size ** (-0.5)
    value_heads = values_in.astype(jnp.float32).reshape(head_shape)
    head_index = head_first + jnp.arange(heads_here, dtype=jnp.float32)
    decays = 1.0 - jnp.exp2(-1.0 - 1.5 * head_index)
    within = lax.optimization_barrier(jnp.sum(query_rot * key_rot, axis=-1, keepdims=True)) * value_heads
    carried = jnp.einsum('shd,shde->she', query_rot, memory, precision=lax.Precision.HIGHEST) * decays[None, :, None]
    mixture = within + carried
    new_memory = decays[None, :, None, None] * memory + key_rot[:, :, :, None] * value_heads[:, :, None, :]
    centre = lax.optimization_barrier(jnp.mean(mixture, axis=-1, keepdims=True))
    spread = lax.optimization_barrier(jnp.mean(jnp.square(mixture - centre), axis=-1, keepdims=True))
    normed = ((mixture - centre) * lax.rsqrt(spread + EPSILON)).reshape(seqs_here, heads_here * head_size)
    normed = normed * head_gain.astype(jnp.float32)
    output = (jax.nn.silu(gating.astype(jnp.float32)) * normed).astype(jnp.bfloat16)
    return (output, new_memory)

def select_slots(route_ids, expert, max_rows):
    flat_ids = route_ids.reshape(-1)
    hits = (flat_ids == expert).astype(jnp.int32)
    ranks = jnp.cumsum(hits) - 1
    slot_range = jnp.arange(max_rows, dtype=jnp.int32)
    matches = (hits[None, :] == 1) & (ranks[None, :] == slot_range[:, None])
    flat_index = jnp.arange(flat_ids.shape[0], dtype=jnp.int32)
    picked = lax.optimization_barrier(jnp.sum(jnp.where(matches, flat_index[None, :], 0), axis=1)).astype(jnp.int32)
    filled = jnp.any(matches, axis=1)
    return (picked, filled)

def expert_hidden(chosen, gate_weight, up_weight):
    gate_value = jnp.dot(chosen, gate_weight, preferred_element_type=jnp.float32)
    up_value = jnp.dot(chosen, up_weight, preferred_element_type=jnp.float32)
    return (jax.nn.silu(gate_value) * up_value).astype(jnp.bfloat16)

def reference(resid, norm_gain, w_query, w_key, w_value, w_gate, head_gain, w_output, state, positions, ffn_gain, w_mix, dense_gate, dense_up, dense_down, routes, route_weight, expert_gate, expert_up, expert_down):
    normed_in = rms_norm(resid.astype(jnp.float32), norm_gain).astype(jnp.bfloat16)

    def project(weight):
        return jnp.dot(normed_in, weight, preferred_element_type=jnp.float32).astype(jnp.bfloat16)
    retained, new_state = retain(project(w_query), project(w_key), project(w_value), project(w_gate), state, positions, 0.0, head_gain)
    width_tp = w_output.shape[0] // N_TP
    attention = jnp.zeros(resid.shape, jnp.float32)
    for block in range(N_TP):
        lower = block * width_tp
        attention = attention + rounded(jnp.dot(retained[:, lower:lower + width_tp], w_output[lower:lower + width_tp], preferred_element_type=jnp.float32))
    middle = resid.astype(jnp.float32) + attention
    normed_mid = rms_norm(middle, ffn_gain).astype(jnp.bfloat16)
    mixing = jax.nn.sigmoid(jnp.dot(normed_mid, w_mix[:, None], preferred_element_type=jnp.float32))
    model_tp = D // N_TP
    gate_sum = jnp.zeros((resid.shape[0], FFD), jnp.float32)
    up_sum = jnp.zeros((resid.shape[0], FFD), jnp.float32)
    for block in range(N_TP):
        lower = block * model_tp
        columns = normed_mid[:, lower:lower + model_tp]
        gate_sum = gate_sum + rounded(jnp.dot(columns, dense_gate[lower:lower + model_tp], preferred_element_type=jnp.float32))
        up_sum = up_sum + rounded(jnp.dot(columns, dense_up[lower:lower + model_tp], preferred_element_type=jnp.float32))
    dense_hidden = (jax.nn.silu(gate_sum) * up_sum).astype(jnp.bfloat16)
    hidden_ep = FFD // N_EP

    def dense_block(total, block):
        lower = block * hidden_ep
        part_hidden = lax.dynamic_slice_in_dim(dense_hidden, lower, hidden_ep, 1)
        part_down = lax.dynamic_slice_in_dim(dense_down, lower, hidden_ep, 0)
        return (total + rounded(jnp.dot(part_hidden, part_down, preferred_element_type=jnp.float32)), None)
    dense_out, _ = lax.scan(dense_block, jnp.zeros(resid.shape, jnp.float32), jnp.arange(N_EP, dtype=jnp.int32))
    max_rows = N_EP * CAP
    expert_tp = FFE // N_TP
    flat_weight = route_weight.reshape(-1).astype(jnp.float32)

    def one_expert(total, expert):
        picked, filled = select_slots(routes, expert, max_rows)
        token_rows = picked // TOPK
        chosen = normed_mid[token_rows]
        hidden_e = expert_hidden(chosen, expert_gate[expert], expert_up[expert])
        summed = jnp.zeros((max_rows, D), jnp.float32)
        for block in range(N_TP):
            lower = block * expert_tp
            summed = summed + rounded(jnp.dot(hidden_e[:, lower:lower + expert_tp], expert_down[expert, lower:lower + expert_tp], preferred_element_type=jnp.float32))
        result = rounded(summed)
        weights_e = jnp.where(filled, flat_weight[picked], 0.0)
        total = total.at[token_rows].add(weights_e[:, None] * result)
        return (total, None)
    moe_out, _ = lax.scan(one_expert, jnp.zeros(resid.shape, jnp.float32), jnp.arange(EXPERTS, dtype=jnp.int32))
    final = (middle + moe_out + mixing * dense_out).astype(jnp.bfloat16)
    return (final, new_state)
```

```python
import functools

import jax
import jax.numpy as jnp
import numpy as np
from jax import lax
from jax.experimental import pallas as pl
from jax.experimental.pallas import tpu as pltpu
from jax.sharding import PartitionSpec as P

EPSILON = 1e-06
THETA = 10000.0


def rms_norm(inputs, scaling):
    square = jnp.mean(inputs * inputs, axis=-1, keepdims=True)
    return inputs * lax.rsqrt(square + EPSILON) * scaling.astype(jnp.float32)


def front_kernel(
    key_scale,
    resid_ref,
    gain_ref,
    place_ref,
    freq_ref,
    head_gain_ref,
    w_query,
    w_key,
    w_value,
    w_gate,
    state,
    out_ref,
    new_state,
    weights,
    memory,
    carried,
    weight_sem,
    load_sem,
    store_sem,
):
    f32 = jnp.float32
    bf16 = jnp.bfloat16
    seqs, heads, size, _ = memory.shape
    chunks = load_sem.shape[0]
    chunk = seqs // chunks
    fetches = [
        pltpu.make_async_copy(source, weights.at[index], weight_sem.at[index])
        for index, source in enumerate((w_query, w_key, w_value, w_gate))
    ]
    loads = [
        pltpu.make_async_copy(
            state.at[pl.ds(c * chunk, chunk)], memory.at[pl.ds(c * chunk, chunk)], load_sem.at[c]
        )
        for c in range(chunks)
    ]
    stores = [
        pltpu.make_async_copy(
            memory.at[pl.ds(c * chunk, chunk)],
            new_state.at[pl.ds(c * chunk, chunk)],
            store_sem.at[c],
        )
        for c in range(chunks)
    ]
    for copy in fetches + loads:
        copy.start()
    resid = resid_ref[...].astype(f32)
    normed = rms_norm(resid, gain_ref[...].reshape(1, -1)).astype(bf16)
    places = jnp.broadcast_to(place_ref[...].astype(f32).reshape(1, seqs), (size, seqs)).T
    angles = places * freq_ref[...]
    cosine = jnp.cos(angles)
    lane = lax.broadcasted_iota(jnp.int32, (seqs, size), 1)
    sine = jnp.where(lane < size // 2, -jnp.sin(angles), jnp.sin(angles))

    def project(index):
        fetches[index].wait()
        return (
            jnp.dot(normed, weights[index], preferred_element_type=f32).astype(bf16).astype(f32)
        )

    def rotate(inputs):
        return inputs * cosine + pltpu.roll(inputs, size // 2, 1) * sine

    def split(inputs):
        return [inputs[:, h * size : (h + 1) * size] for h in range(heads)]

    query = [rotate(part) for part in split(project(0))]
    key = [rotate(part) * key_scale for part in split(project(1))]
    value = split(project(2))
    query_t = [part.T for part in query]
    key_t = [part.T for part in key]
    head_first = lax.axis_index("tp") * heads
    decays = [
        1.0 - jnp.exp2(-1.0 - 1.5 * jnp.full((1, size), head_first + h, jnp.int32).astype(f32))
        for h in range(heads)
    ]
    gating = split(project(3))
    for c in range(chunks):
        loads[c].wait()
        for s in range(c * chunk, (c + 1) * chunk):
            for h in range(heads):
                block = memory[s, h]
                carried[h, s : s + 1, :] = jnp.sum(
                    block * query_t[h][:, s : s + 1], axis=0, keepdims=True
                )
                memory[s, h] = (
                    block * decays[h] + key_t[h][:, s : s + 1] * value[h][s : s + 1, :]
                )
        stores[c].start()
    head_gain = head_gain_ref[...].astype(f32).reshape(1, -1)
    for h in range(heads):
        within = jnp.sum(query[h] * key[h], axis=-1, keepdims=True) * value[h]
        mixture = within + carried[h] * decays[h]
        centre = jnp.mean(mixture, axis=-1, keepdims=True)
        spread = jnp.mean(jnp.square(mixture - centre), axis=-1, keepdims=True)
        place = slice(h * size, (h + 1) * size)
        scaled = (mixture - centre) * lax.rsqrt(spread + EPSILON) * head_gain[:, place]
        out_ref[:, place] = (jax.nn.silu(gating[h]) * scaled).astype(bf16)
    for copy in stores:
        copy.wait()


def front(resid, norm_gain, positions, head_gain, weights, state):
    seqs, heads, size, _ = state.shape
    half = size // 2
    inverse = THETA ** (-np.arange(half, dtype=np.float64) / half)
    freq = jnp.asarray(np.concatenate([inverse, inverse])[None, :].astype(np.float32))
    chunks = min(8, seqs)
    vmem = pl.BlockSpec(memory_space=pltpu.VMEM)
    anywhere = pl.BlockSpec(memory_space=pltpu.HBM)
    return pl.pallas_call(
        functools.partial(front_kernel, size ** (-0.5)),
        out_shape=(
            jax.ShapeDtypeStruct((seqs, heads * size), jnp.bfloat16),
            jax.ShapeDtypeStruct(state.shape, jnp.float32),
        ),
        in_specs=[vmem] * 5 + [anywhere] * 5,
        out_specs=(vmem, anywhere),
        scratch_shapes=[
            pltpu.VMEM((4,) + weights[0].shape, jnp.bfloat16),
            pltpu.VMEM(state.shape, jnp.float32),
            pltpu.VMEM((heads, seqs, size), jnp.float32),
            pltpu.SemaphoreType.DMA((4,)),
            pltpu.SemaphoreType.DMA((chunks,)),
            pltpu.SemaphoreType.DMA((chunks,)),
        ],
        compiler_params=pltpu.CompilerParams(vmem_limit_bytes=40 * 1024 * 1024),
        name="front",
    )(resid, norm_gain, positions, freq, head_gain, *weights, state)


def flip(index, mask):
    result = index
    bit = 1
    while bit <= mask:
        if mask & bit:
            result = result + bit * (1 - 2 * lax.rem(lax.div(index, bit), 2))
        bit *= 2
    return result


def tail_kernel(
    tp_count,
    ep_count,
    slots,
    retained_ref,
    resid_ref,
    gain_ref,
    mix_ref,
    routes_ref,
    route_weight_ref,
    w_output,
    dense_gate,
    dense_up,
    dense_down,
    expert_gate,
    expert_up,
    expert_down,
    out_ref,
    wo,
    wg,
    wu,
    wd,
    eg,
    eu,
    ed,
    scales,
    dispatch,
    combine,
    part,
    att_rx,
    middle,
    stat_tx,
    stat_rx,
    inverses,
    rows,
    hot,
    tokens,
    token_scale,
    gu_tx,
    gu_rx,
    gu_pair,
    gu_far,
    hidden,
    eh,
    er_tx,
    er_rx,
    er_pair,
    er_far,
    do_tx,
    do_rx,
    mo_tx,
    mo_rx,
    load_sem,
    send_sem,
    recv_sem,
):
    me_t = lax.axis_index("tp")
    me_e = lax.axis_index("ep")
    seq_dev, model_width = resid_ref.shape
    width = model_width // tp_count
    block = hidden.shape[0] // tp_count
    f32 = jnp.float32
    bf16 = jnp.bfloat16

    loads = [
        pltpu.make_async_copy(source, target, load_sem.at[index])
        for index, (source, target) in enumerate(
            (
                (w_output, wo),
                (dense_gate, wg),
                (dense_up, wu),
                (expert_gate.at[0], eg),
                (expert_up.at[0], eu),
                (expert_down.at[0], ed),
                (dense_down, wd),
            )
        )
    ]
    for load in loads:
        load.start()

    def peer_t(step):
        return flip(me_t, step)

    def peer_e(step):
        return flip(me_e, step)

    tp_steps = list(range(1, tp_count))
    ep_steps = list(range(ep_count - 1, 0, -1))
    barrier = pltpu.get_barrier_semaphore()
    for step in tp_steps:
        pl.semaphore_signal(
            barrier,
            inc=1,
            device_id=(me_e, peer_t(step)),
            device_id_type=pl.DeviceIdType.MESH,
        )
    for step in ep_steps:
        pl.semaphore_signal(
            barrier,
            inc=1,
            device_id=(peer_e(step), me_t),
            device_id_type=pl.DeviceIdType.MESH,
        )

    used = [0]
    started = []

    def send(source, target, device):
        index = used[0]
        used[0] = index + 1
        copy = pltpu.make_async_remote_copy(
            src_ref=source,
            dst_ref=target,
            send_sem=send_sem.at[index],
            recv_sem=recv_sem.at[index],
            device_id=device,
            device_id_type=pl.DeviceIdType.MESH,
        )
        copy.start()
        started.append(copy)
        return copy

    def span(index, size):
        return pl.ds(pl.multiple_of(index * size, size), size)

    def dot(left, right):
        return jnp.dot(left, right, preferred_element_type=f32)

    def arrive(copies):
        for copy in copies:
            copy.wait_recv()

    half = tp_count // 2
    sibling = peer_t(1)

    def across(step):
        return peer_t(2 * step)

    def spread(at):
        return [
            send(at(me_t), at(me_t), (me_e, target))
            for target in [sibling] + [across(k) for k in range(1, half)]
        ]

    def pass_on(copies, at):
        waiting = [copies[0]]
        for k in range(1, half):
            copies[k].wait_recv()
            waiting.append(send(at(across(k)), at(across(k)), (me_e, sibling)))
        return waiting

    own = span(me_t, width)
    scales[0:1, :] = gain_ref[...].astype(f32).reshape(1, -1)
    scales[1:2, :] = mix_ref[...].astype(f32).reshape(1, -1)
    gain = scales[0:1, own]
    mix = scales[1:2, own]

    top_count = routes_ref.shape[0]
    expert_ids = lax.broadcasted_iota(jnp.int32, (ep_count, seq_dev), 0)
    taken = jnp.zeros((ep_count, seq_dev), f32)
    weight_of = jnp.zeros((ep_count, seq_dev), f32)
    for j in range(top_count):
        named = routes_ref[j : j + 1, :] == expert_ids
        taken = taken + jnp.where(named, 1.0, 0.0)
        weight_of = weight_of + jnp.where(
            named, route_weight_ref[j : j + 1, :].astype(f32), 0.0
        )
    earlier = lax.broadcasted_iota(jnp.int32, (seq_dev, seq_dev), 0)
    later = lax.broadcasted_iota(jnp.int32, (seq_dev, seq_dev), 1)
    ranks = dot(taken.astype(bf16), jnp.where(earlier < later, 1.0, 0.0).astype(bf16))
    slot_ids = lax.broadcasted_iota(jnp.int32, (slots, seq_dev), 0).astype(f32)
    for e in range(ep_count):
        hits = (ranks[e : e + 1, :] == slot_ids) & (taken[e : e + 1, :] > 0.0)
        dispatch[e] = jnp.where(hits, 1.0, 0.0).astype(bf16)
        combine[e * slots : (e + 1) * slots, :] = jnp.where(
            hits, weight_of[e : e + 1, :], 0.0
        ).astype(bf16)

    loads[0].wait()
    retained = retained_ref[...]
    for d in tp_steps[1:] + tp_steps[:1] + [0]:
        part[d] = dot(retained, wo[:, span(peer_t(d), width)]).astype(bf16)
    pl.semaphore_wait(barrier, tp_count - 1 + ep_count - 1)
    att = [
        send(part.at[d], att_rx.at[d - 1], (me_e, peer_t(d)))
        for d in tp_steps[1:] + tp_steps[:1]
    ]
    hots = [send(dispatch.at[peer_e(d)], hot.at[me_e], (peer_e(d), me_t)) for d in ep_steps]
    hot[me_e] = dispatch[me_e]
    arrive(att)
    total = part[0].astype(f32)
    for d in tp_steps:
        total = total + att_rx[d - 1].astype(f32)
    mid = resid_ref[:, own].astype(f32) + total
    scaled = mid * gain
    rows[me_e] = scaled.astype(bf16)
    gathered = [send(rows.at[me_e], rows.at[me_e], (peer_e(d), me_t)) for d in ep_steps]
    middle[...] = mid

    lane = lax.broadcasted_iota(jnp.int32, (seq_dev, 128), 1)
    diagonal = lane == lax.broadcasted_iota(jnp.int32, (seq_dev, 128), 0)

    def to_row(column):
        return jnp.sum(jnp.where(diagonal, column, 0.0), axis=0, keepdims=True)

    def to_column(row):
        return jnp.sum(jnp.where(diagonal, row, 0.0), axis=1, keepdims=True)

    stat_tx[0:1, :] = to_row(jnp.sum(mid * mid, axis=-1, keepdims=True))
    stat_tx[1:2, :] = to_row(jnp.sum(scaled * mix, axis=-1, keepdims=True))
    stats = [send(stat_tx, stat_rx.at[d - 1], (me_e, peer_t(d))) for d in tp_steps]
    arrive(stats)
    stat = stat_tx[0:2, :]
    for d in tp_steps:
        stat = stat + stat_rx[d - 1, 0:2, :]
    inverse = lax.rsqrt(stat[0:1, :] / model_width + EPSILON)
    mixing = to_column(jax.nn.sigmoid(inverse * stat[1:2, :]))
    inverses[me_e, 0:1, :] = inverse
    factors = [
        send(inverses.at[me_e], inverses.at[me_e], (peer_e(d), me_t)) for d in ep_steps
    ]

    arrive(hots)
    arrive(gathered)
    for s in range(ep_count):
        tokens[me_t, s * slots : (s + 1) * slots, :] = dot(hot[s], rows[s]).astype(bf16)
    toks = spread(lambda index: tokens.at[index])
    near = []
    all_rows = rows[...].reshape(ep_count * seq_dev, width)
    for which, weight in enumerate((wg, wu)):
        loads[1 + which].wait()
        gu_tx[which] = lax.dot_general(
            all_rows, weight[...], (((1,), (1,)), ((), ())), preferred_element_type=f32
        ).astype(bf16)
        near.append(
            [
                send(
                    gu_tx.at[which, span(flip(sibling, 2 * k), block), :],
                    gu_rx.at[which, k],
                    (me_e, sibling),
                )
                for k in range(half)
            ]
        )
    toks = pass_on(toks, lambda index: tokens.at[index])
    far = []
    for which in range(2):
        arrive(near[which])
        for k in range(1, half):
            target = across(k)
            gu_pair[which, k - 1] = (
                gu_tx[which, span(target, block), :].astype(f32) + gu_rx[which, k].astype(f32)
            ).astype(bf16)
            far.append(
                send(gu_pair.at[which, k - 1], gu_far.at[which, k - 1], (me_e, target))
            )
    arrive(factors)
    for s in range(ep_count):
        token_scale[s * slots : (s + 1) * slots, :] = jnp.sum(
            hot[s].astype(f32) * inverses[s, 0:1, 0:seq_dev], axis=1, keepdims=True
        )
    loads[3].wait()
    loads[4].wait()
    arrive(toks)
    tile = min(256, eg.shape[1])

    def expert_tile(index, carry):
        columns = span(index, tile)
        gate = jnp.zeros((tokens.shape[1], tile), f32)
        up = jnp.zeros((tokens.shape[1], tile), f32)
        for c in range(tp_count):
            features = slice(c * width, (c + 1) * width)
            gate = gate + dot(tokens[c], eg[features, columns])
            up = up + dot(tokens[c], eu[features, columns])
        factor = token_scale[...]
        eh[:, columns] = (jax.nn.silu(gate * factor) * (up * factor)).astype(bf16)
        return carry

    lax.fori_loop(0, eg.shape[1] // tile, expert_tile, 0)

    arrive(far)
    factor = jnp.concatenate(
        [
            to_column(inverses[me_t * (block // seq_dev) + i, 0:1, :])
            for i in range(block // seq_dev)
        ],
        axis=0,
    )
    gate = gu_tx[0, span(me_t, block), :].astype(f32) + gu_rx[0, 0].astype(f32)
    up = gu_tx[1, span(me_t, block), :].astype(f32) + gu_rx[1, 0].astype(f32)
    for k in range(1, half):
        gate = gate + gu_far[0, k - 1].astype(f32)
        up = up + gu_far[1, k - 1].astype(f32)
    hidden[span(me_t, block), :] = (jax.nn.silu(gate * factor) * (up * factor)).astype(bf16)
    hids = spread(lambda index: hidden.at[span(index, block), :])
    loads[5].wait()
    pairs = []
    for k in range(half):
        target = flip(sibling, 2 * k)
        er_tx[k] = dot(eh[...], ed[:, span(target, width)]).astype(bf16)
        pairs.append(send(er_tx.at[k], er_rx.at[k], (me_e, sibling)))
    hids = pass_on(hids, lambda index: hidden.at[span(index, block), :])
    partials = []
    for k in range(1, half):
        target = across(k)
        summed = dot(eh[...], ed[:, span(target, width)])
        arrive(pairs[k : k + 1])
        er_pair[k - 1] = (summed + er_rx[k].astype(f32)).astype(bf16)
        partials.append(send(er_pair.at[k - 1], er_far.at[k - 1], (me_e, target)))
    loads[6].wait()
    arrive(hids)
    do_tx[...] = dot(hidden[...], wd[...]).astype(bf16)
    outs = [
        send(do_tx.at[span(peer_e(d), seq_dev), :], do_rx.at[d - 1], (peer_e(d), me_t))
        for d in ep_steps
    ]
    result = dot(eh[...], ed[:, own])
    arrive(pairs[:1])
    result = result + er_rx[0].astype(f32)
    arrive(partials)
    for k in range(1, half):
        result = result + er_far[k - 1].astype(f32)
    mo_tx[...] = result.astype(bf16)
    place = span(me_e, slots)
    backs = [
        send(mo_tx.at[span(peer_e(d), slots), :], mo_rx.at[place, :], (peer_e(d), me_t))
        for d in ep_steps
    ]
    mo_rx[place, :] = mo_tx[place, :]
    arrive(outs)
    dense = do_tx[span(me_e, seq_dev), :].astype(f32)
    for d in ep_steps:
        dense = dense + do_rx[d - 1].astype(f32)
    partly = middle[...] + mixing * dense
    arrive(backs)
    returned = lax.dot_general(
        combine[...], mo_rx[...], (((0,), (0,)), ((), ())), preferred_element_type=f32
    )
    out_ref[...] = (partly + returned).astype(bf16)
    for copy in started:
        copy.wait_send()


def tail(retained, resid, gain, mix, routes, route_weight, slots, weights, tp_count, ep_count):
    seq_dev, model_width = resid.shape
    width = model_width // tp_count
    batch = seq_dev * ep_count
    block = batch // tp_count
    dense_units = weights[1].shape[0]
    half = tp_count // 2
    expert_units = weights[4].shape[2]
    items = ep_count * slots
    bf16 = jnp.bfloat16
    f32 = jnp.float32
    peers_t = tp_count - 1
    peers_e = ep_count - 1
    copies = 7 * peers_t + 5 * peers_e
    vmem = pl.BlockSpec(memory_space=pltpu.VMEM)
    anywhere = pl.BlockSpec(memory_space=pltpu.HBM)
    return pl.pallas_call(
        functools.partial(tail_kernel, tp_count, ep_count, slots),
        out_shape=jax.ShapeDtypeStruct((seq_dev, width), bf16),
        in_specs=[vmem] * 6 + [anywhere] * 7,
        out_specs=vmem,
        scratch_shapes=[
            pltpu.VMEM(weights[0].shape, bf16),
            pltpu.VMEM(weights[1].shape, bf16),
            pltpu.VMEM(weights[2].shape, bf16),
            pltpu.VMEM(weights[3].shape, bf16),
            pltpu.VMEM(weights[4].shape[1:], bf16),
            pltpu.VMEM(weights[5].shape[1:], bf16),
            pltpu.VMEM(weights[6].shape[1:], bf16),
            pltpu.VMEM((8, model_width), f32),
            pltpu.VMEM((ep_count, slots, seq_dev), bf16),
            pltpu.VMEM((items, seq_dev), bf16),
            pltpu.VMEM((tp_count, seq_dev, width), bf16),
            pltpu.VMEM((peers_t, seq_dev, width), bf16),
            pltpu.VMEM((seq_dev, width), f32),
            pltpu.VMEM((8, 128), f32),
            pltpu.VMEM((peers_t, 8, 128), f32),
            pltpu.VMEM((ep_count, 8, 128), f32),
            pltpu.VMEM((ep_count, seq_dev, width), bf16),
            pltpu.VMEM((ep_count, slots, seq_dev), bf16),
            pltpu.VMEM((tp_count, items, width), bf16),
            pltpu.VMEM((items, 1), f32),
            pltpu.VMEM((2, batch, dense_units), bf16),
            pltpu.VMEM((2, half, block, dense_units), bf16),
            pltpu.VMEM((2, half - 1, block, dense_units), bf16),
            pltpu.VMEM((2, half - 1, block, dense_units), bf16),
            pltpu.VMEM((batch, dense_units), bf16),
            pltpu.VMEM((items, expert_units), bf16),
            pltpu.VMEM((half, items, width), bf16),
            pltpu.VMEM((half, items, width), bf16),
            pltpu.VMEM((half - 1, items, width), bf16),
            pltpu.VMEM((half - 1, items, width), bf16),
            pltpu.VMEM((batch, width), bf16),
            pltpu.VMEM((peers_e, seq_dev, width), bf16),
            pltpu.VMEM((items, width), bf16),
            pltpu.VMEM((items, width), bf16),
            pltpu.SemaphoreType.DMA((7,)),
            pltpu.SemaphoreType.DMA((copies,)),
            pltpu.SemaphoreType.DMA((copies,)),
        ],
        compiler_params=pltpu.CompilerParams(
            collective_id=0, has_side_effects=True, vmem_limit_bytes=61 * 1024 * 1024
        ),
        name="tail",
    )(retained, resid, gain, mix, routes, route_weight, *weights)


def per_device(
    resid,
    norm_gain,
    w_query,
    w_key,
    w_value,
    w_gate,
    head_gain,
    w_output,
    state,
    positions,
    ffn_gain,
    w_mix,
    dense_gate,
    dense_up,
    dense_down,
    routes,
    route_weight,
    expert_gate,
    expert_up,
    expert_down,
):
    seq_dev = resid.shape[0]
    tp_count = lax.axis_size("tp")
    ep_count = lax.axis_size("ep")
    retained, new_state = front(
        resid, norm_gain, positions, head_gain, (w_query, w_key, w_value, w_gate), state
    )
    capacity = max(2, 2 * seq_dev * routes.shape[1] // ep_count)
    slots = -(-capacity // 16) * 16
    final = tail(
        retained,
        resid,
        ffn_gain,
        w_mix,
        routes.T,
        route_weight.T,
        slots,
        (w_output, dense_gate.T, dense_up.T, dense_down, expert_gate, expert_up, expert_down),
        tp_count,
        ep_count,
    )
    return (final, new_state)


def solution(mesh):
    in_specs = (
        P("ep", None),
        P(),
        P(None, "tp"),
        P(None, "tp"),
        P(None, "tp"),
        P(None, "tp"),
        P("tp"),
        P("tp", None),
        P("ep", "tp", None, None),
        P("ep"),
        P(),
        P(),
        P("tp", "ep"),
        P("tp", "ep"),
        P("ep", "tp"),
        P("ep", None),
        P("ep", None),
        P("ep", None, "tp"),
        P("ep", None, "tp"),
        P("ep", "tp", None),
    )
    out_specs = (P("ep", "tp"), P("ep", "tp", None, None))
    return jax.shard_map(
        per_device, mesh=mesh, in_specs=in_specs, out_specs=out_specs, check_vma=False
    )
```

```python
import functools

import jax
import jax.numpy as jnp
import numpy as np
from jax import lax
from jax.experimental import pallas as pl
from jax.experimental.pallas import tpu as pltpu
from jax.sharding import PartitionSpec as P

EPSILON = 1e-06
THETA = 10000.0


def rms_norm(inputs, scaling):
    square = jnp.mean(inputs * inputs, axis=-1, keepdims=True)
    return inputs * lax.rsqrt(square + EPSILON) * scaling.astype(jnp.float32)


def front_kernel(
    key_scale,
    resid,
    norm_gain,
    positions,
    freq,
    head_gain,
    w_query,
    w_key,
    w_value,
    w_gate,
    state,
    out_ref,
    new_state,
    resid_ref,
    gain_ref,
    place_ref,
    freq_ref,
    head_gain_ref,
    weights,
    memory,
    carried,
    small_sem,
    weight_sem,
    load_sem,
    store_sem,
):
    f32 = jnp.float32
    bf16 = jnp.bfloat16
    seqs, heads, size, _ = memory.shape
    chunks = load_sem.shape[0]
    chunk = seqs // chunks
    smalls = [
        pltpu.make_async_copy(source, target, small_sem.at[index])
        for index, (source, target) in enumerate(
            (
                (resid, resid_ref),
                (norm_gain, gain_ref),
                (positions, place_ref),
                (freq, freq_ref),
                (head_gain, head_gain_ref),
            )
        )
    ]
    fetches = [
        pltpu.make_async_copy(source, weights.at[index], weight_sem.at[index])
        for index, source in enumerate((w_query, w_key, w_value, w_gate))
    ]
    loads = [
        pltpu.make_async_copy(
            state.at[pl.ds(c * chunk, chunk)], memory.at[pl.ds(c * chunk, chunk)], load_sem.at[c]
        )
        for c in range(chunks)
    ]
    stores = [
        pltpu.make_async_copy(
            memory.at[pl.ds(c * chunk, chunk)],
            new_state.at[pl.ds(c * chunk, chunk)],
            store_sem.at[c],
        )
        for c in range(chunks)
    ]
    for copy in smalls + fetches + loads:
        copy.start()
    for copy in smalls:
        copy.wait()
    resid = resid_ref[...].astype(f32)
    normed = rms_norm(resid, gain_ref[...].reshape(1, -1)).astype(bf16)
    places = jnp.broadcast_to(place_ref[...].astype(f32).reshape(1, seqs), (size, seqs)).T
    angles = places * freq_ref[...]
    cosine = jnp.cos(angles)
    lane = lax.broadcasted_iota(jnp.int32, (seqs, size), 1)
    sine = jnp.where(lane < size // 2, -jnp.sin(angles), jnp.sin(angles))

    def project(index):
        fetches[index].wait()
        return (
            jnp.dot(normed, weights[index], preferred_element_type=f32).astype(bf16).astype(f32)
        )

    def rotate(inputs):
        return inputs * cosine + pltpu.roll(inputs, size // 2, 1) * sine

    def split(inputs):
        return [inputs[:, h * size : (h + 1) * size] for h in range(heads)]

    query = [rotate(part) for part in split(project(0))]
    key = [rotate(part) * key_scale for part in split(project(1))]
    value = split(project(2))
    query_t = [part.T for part in query]
    key_t = [part.T for part in key]
    head_first = lax.axis_index("tp") * heads
    decays = [
        1.0 - jnp.exp2(-1.0 - 1.5 * jnp.full((1, size), head_first + h, jnp.int32).astype(f32))
        for h in range(heads)
    ]
    gating = split(project(3))
    for c in range(chunks):
        loads[c].wait()
        for s in range(c * chunk, (c + 1) * chunk):
            for h in range(heads):
                block = memory[s, h]
                carried[h, s : s + 1, :] = jnp.sum(
                    block * query_t[h][:, s : s + 1], axis=0, keepdims=True
                )
                memory[s, h] = (
                    block * decays[h] + key_t[h][:, s : s + 1] * value[h][s : s + 1, :]
                )
        stores[c].start()
    gains = head_gain_ref[...].astype(f32).reshape(1, -1)
    for h in range(heads):
        within = jnp.sum(query[h] * key[h], axis=-1, keepdims=True) * value[h]
        mixture = within + carried[h] * decays[h]
        centre = jnp.mean(mixture, axis=-1, keepdims=True)
        spread = jnp.mean(jnp.square(mixture - centre), axis=-1, keepdims=True)
        place = slice(h * size, (h + 1) * size)
        scaled = (mixture - centre) * lax.rsqrt(spread + EPSILON) * gains[:, place]
        out_ref[:, place] = (jax.nn.silu(gating[h]) * scaled).astype(bf16)
    for copy in stores:
        copy.wait()


def front(resid, norm_gain, positions, head_gain, weights, state):
    seqs, heads, size, _ = state.shape
    half = size // 2
    inverse = THETA ** (-np.arange(half, dtype=np.float64) / half)
    freq = jnp.asarray(np.concatenate([inverse, inverse])[None, :].astype(np.float32))
    chunks = min(8, seqs)
    vmem = pl.BlockSpec(memory_space=pltpu.VMEM)
    anywhere = pl.BlockSpec(memory_space=pltpu.HBM)
    return pl.pallas_call(
        functools.partial(front_kernel, size ** (-0.5)),
        out_shape=(
            jax.ShapeDtypeStruct((seqs, heads * size), jnp.bfloat16),
            jax.ShapeDtypeStruct(state.shape, jnp.float32),
        ),
        in_specs=[anywhere] * 10,
        out_specs=(vmem, anywhere),
        scratch_shapes=[
            pltpu.VMEM(resid.shape, resid.dtype),
            pltpu.VMEM(norm_gain.shape, norm_gain.dtype),
            pltpu.VMEM(positions.shape, positions.dtype),
            pltpu.VMEM(freq.shape, freq.dtype),
            pltpu.VMEM(head_gain.shape, head_gain.dtype),
            pltpu.VMEM((4,) + weights[0].shape, jnp.bfloat16),
            pltpu.VMEM(state.shape, jnp.float32),
            pltpu.VMEM((heads, seqs, size), jnp.float32),
            pltpu.SemaphoreType.DMA((5,)),
            pltpu.SemaphoreType.DMA((4,)),
            pltpu.SemaphoreType.DMA((chunks,)),
            pltpu.SemaphoreType.DMA((chunks,)),
        ],
        compiler_params=pltpu.CompilerParams(vmem_limit_bytes=61 * 1024 * 1024),
        name="front",
    )(resid, norm_gain, positions, freq, head_gain, *weights, state)


def flip(index, mask):
    result = index
    bit = 1
    while bit <= mask:
        if mask & bit:
            result = result + bit * (1 - 2 * lax.rem(lax.div(index, bit), 2))
        bit *= 2
    return result


def tail_kernel(
    tp_count,
    ep_count,
    slots,
    retained,
    resid,
    ffn_gain,
    w_mix,
    routes,
    route_weight,
    w_output,
    dense_gate,
    dense_up,
    dense_down,
    expert_gate,
    expert_up,
    expert_down,
    out_ref,
    retained_ref,
    resid_ref,
    gain_ref,
    mix_ref,
    routes_ref,
    route_weight_ref,
    wo,
    wg,
    wu,
    wd,
    eg,
    eu,
    ed,
    scales,
    dispatch,
    combine,
    part,
    att_rx,
    middle,
    stat_tx,
    stat_rx,
    inverses,
    rows,
    hot,
    tokens,
    token_scale,
    gu_tx,
    gu_rx,
    gu_pair,
    gu_far,
    hidden,
    eh,
    er_tx,
    er_rx,
    er_pair,
    er_far,
    do_tx,
    do_rx,
    mo_tx,
    mo_rx,
    load_sem,
    send_sem,
    recv_sem,
):
    me_t = lax.axis_index("tp")
    me_e = lax.axis_index("ep")
    seq_dev, model_width = resid_ref.shape
    width = model_width // tp_count
    block = hidden.shape[0] // tp_count
    f32 = jnp.float32
    bf16 = jnp.bfloat16

    loads = [
        pltpu.make_async_copy(source, target, load_sem.at[index])
        for index, (source, target) in enumerate(
            (
                (retained, retained_ref),
                (resid, resid_ref),
                (ffn_gain, gain_ref),
                (w_mix, mix_ref),
                (routes, routes_ref),
                (route_weight, route_weight_ref),
                (w_output, wo),
                (dense_gate, wg),
                (dense_up, wu),
                (expert_gate.at[0], eg),
                (expert_up.at[0], eu),
                (expert_down.at[0], ed),
                (dense_down, wd),
            )
        )
    ]
    for load in loads:
        load.start()

    def ready(*indices):
        for index in indices:
            loads[index].wait()

    def peer_t(step):
        return flip(me_t, step)

    def peer_e(step):
        return flip(me_e, step)

    tp_steps = list(range(1, tp_count))
    ep_steps = list(range(ep_count - 1, 0, -1))
    barrier = pltpu.get_barrier_semaphore()
    for step in tp_steps:
        pl.semaphore_signal(
            barrier,
            inc=1,
            device_id=(me_e, peer_t(step)),
            device_id_type=pl.DeviceIdType.MESH,
        )
    for step in ep_steps:
        pl.semaphore_signal(
            barrier,
            inc=1,
            device_id=(peer_e(step), me_t),
            device_id_type=pl.DeviceIdType.MESH,
        )

    used = [0]
    started = []

    def send(source, target, device):
        index = used[0]
        used[0] = index + 1
        copy = pltpu.make_async_remote_copy(
            src_ref=source,
            dst_ref=target,
            send_sem=send_sem.at[index],
            recv_sem=recv_sem.at[index],
            device_id=device,
            device_id_type=pl.DeviceIdType.MESH,
        )
        copy.start()
        started.append(copy)
        return copy

    def span(index, size):
        return pl.ds(pl.multiple_of(index * size, size), size)

    def dot(left, right):
        return jnp.dot(left, right, preferred_element_type=f32)

    def arrive(copies):
        for copy in copies:
            copy.wait_recv()

    half = tp_count // 2
    sibling = peer_t(1)

    def across(step):
        return peer_t(2 * step)

    def spread(at):
        return [
            send(at(me_t), at(me_t), (me_e, target))
            for target in [sibling] + [across(k) for k in range(1, half)]
        ]

    def pass_on(copies, at):
        waiting = [copies[0]]
        for k in range(1, half):
            arrive(copies[k : k + 1])
            waiting.append(send(at(across(k)), at(across(k)), (me_e, sibling)))
        return waiting

    own = span(me_t, width)
    ready(2, 3, 4, 5)
    scales[0:1, :] = gain_ref[...].astype(f32).reshape(1, -1)
    scales[1:2, :] = mix_ref[...].astype(f32).reshape(1, -1)
    gain = scales[0:1, own]
    mix = scales[1:2, own]

    top_count = routes_ref.shape[0]
    expert_ids = lax.broadcasted_iota(jnp.int32, (ep_count, seq_dev), 0)
    taken = jnp.zeros((ep_count, seq_dev), f32)
    weight_of = jnp.zeros((ep_count, seq_dev), f32)
    for j in range(top_count):
        named = routes_ref[j : j + 1, :] == expert_ids
        taken = taken + jnp.where(named, 1.0, 0.0)
        weight_of = weight_of + jnp.where(
            named, route_weight_ref[j : j + 1, :].astype(f32), 0.0
        )
    earlier = lax.broadcasted_iota(jnp.int32, (seq_dev, seq_dev), 0)
    later = lax.broadcasted_iota(jnp.int32, (seq_dev, seq_dev), 1)
    ranks = dot(taken.astype(bf16), jnp.where(earlier < later, 1.0, 0.0).astype(bf16))
    slot_ids = lax.broadcasted_iota(jnp.int32, (slots, seq_dev), 0).astype(f32)
    for e in range(ep_count):
        hits = (ranks[e : e + 1, :] == slot_ids) & (taken[e : e + 1, :] > 0.0)
        dispatch[e] = jnp.where(hits, 1.0, 0.0).astype(bf16)
        combine[e * slots : (e + 1) * slots, :] = jnp.where(
            hits, weight_of[e : e + 1, :], 0.0
        ).astype(bf16)

    ready(0, 1, 6)
    kept = retained_ref[...]
    for d in tp_steps[1:] + tp_steps[:1] + [0]:
        part[d] = dot(kept, wo[:, span(peer_t(d), width)]).astype(bf16)
    pl.semaphore_wait(barrier, tp_count - 1 + ep_count - 1)
    att = [
        send(part.at[d], att_rx.at[d - 1], (me_e, peer_t(d)))
        for d in tp_steps[1:] + tp_steps[:1]
    ]
    hots = [send(dispatch.at[peer_e(d)], hot.at[me_e], (peer_e(d), me_t)) for d in ep_steps]
    hot[me_e] = dispatch[me_e]
    arrive(att)
    total = part[0].astype(f32)
    for d in tp_steps:
        total = total + att_rx[d - 1].astype(f32)
    mid = resid_ref[:, own].astype(f32) + total
    scaled = mid * gain
    rows[me_e] = scaled.astype(bf16)
    gathered = [send(rows.at[me_e], rows.at[me_e], (peer_e(d), me_t)) for d in ep_steps]
    middle[...] = mid

    lane = lax.broadcasted_iota(jnp.int32, (seq_dev, 128), 1)
    diagonal = lane == lax.broadcasted_iota(jnp.int32, (seq_dev, 128), 0)

    def to_row(column):
        return jnp.sum(jnp.where(diagonal, column, 0.0), axis=0, keepdims=True)

    def to_column(row):
        return jnp.sum(jnp.where(diagonal, row, 0.0), axis=1, keepdims=True)

    stat_tx[0:1, :] = to_row(jnp.sum(mid * mid, axis=-1, keepdims=True))
    stat_tx[1:2, :] = to_row(jnp.sum(scaled * mix, axis=-1, keepdims=True))
    stats = [send(stat_tx, stat_rx.at[d - 1], (me_e, peer_t(d))) for d in tp_steps]
    arrive(stats)
    stat = stat_tx[0:2, :]
    for d in tp_steps:
        stat = stat + stat_rx[d - 1, 0:2, :]
    inverse = lax.rsqrt(stat[0:1, :] / model_width + EPSILON)
    mixing = to_column(jax.nn.sigmoid(inverse * stat[1:2, :]))
    inverses[me_e, 0:1, :] = inverse
    factors = [
        send(inverses.at[me_e], inverses.at[me_e], (peer_e(d), me_t)) for d in ep_steps
    ]

    arrive(hots)
    arrive(gathered)
    for s in range(ep_count):
        tokens[me_t, s * slots : (s + 1) * slots, :] = dot(hot[s], rows[s]).astype(bf16)
    toks = spread(lambda index: tokens.at[index])
    near = []
    all_rows = rows[...].reshape(ep_count * seq_dev, width)
    for which, weight in enumerate((wg, wu)):
        ready(7 + which)
        gu_tx[which] = lax.dot_general(
            all_rows, weight[...], (((1,), (1,)), ((), ())), preferred_element_type=f32
        ).astype(bf16)
        near.append(
            [
                send(
                    gu_tx.at[which, span(flip(sibling, 2 * k), block), :],
                    gu_rx.at[which, k],
                    (me_e, sibling),
                )
                for k in range(half)
            ]
        )
    toks = pass_on(toks, lambda index: tokens.at[index])
    far = []
    for which in range(2):
        arrive(near[which])
        for k in range(1, half):
            target = across(k)
            gu_pair[which, k - 1] = (
                gu_tx[which, span(target, block), :].astype(f32) + gu_rx[which, k].astype(f32)
            ).astype(bf16)
            far.append(
                send(gu_pair.at[which, k - 1], gu_far.at[which, k - 1], (me_e, target))
            )
    arrive(factors)
    for s in range(ep_count):
        token_scale[s * slots : (s + 1) * slots, :] = jnp.sum(
            hot[s].astype(f32) * inverses[s, 0:1, 0:seq_dev], axis=1, keepdims=True
        )
    ready(9, 10)
    arrive(toks)
    tile = min(256, eg.shape[1])

    def expert_tile(index, carry):
        columns = span(index, tile)
        gate = jnp.zeros((tokens.shape[1], tile), f32)
        up = jnp.zeros((tokens.shape[1], tile), f32)
        for c in range(tp_count):
            features = slice(c * width, (c + 1) * width)
            gate = gate + dot(tokens[c], eg[features, columns])
            up = up + dot(tokens[c], eu[features, columns])
        factor = token_scale[...]
        eh[:, columns] = (jax.nn.silu(gate * factor) * (up * factor)).astype(bf16)
        return carry

    lax.fori_loop(0, eg.shape[1] // tile, expert_tile, 0)
    arrive(far)
    factor = jnp.concatenate(
        [
            to_column(inverses[me_t * (block // seq_dev) + i, 0:1, :])
            for i in range(block // seq_dev)
        ],
        axis=0,
    )
    gate = gu_tx[0, span(me_t, block), :].astype(f32) + gu_rx[0, 0].astype(f32)
    up = gu_tx[1, span(me_t, block), :].astype(f32) + gu_rx[1, 0].astype(f32)
    for k in range(1, half):
        gate = gate + gu_far[0, k - 1].astype(f32)
        up = up + gu_far[1, k - 1].astype(f32)
    hidden[span(me_t, block), :] = (jax.nn.silu(gate * factor) * (up * factor)).astype(bf16)
    hids = spread(lambda index: hidden.at[span(index, block), :])
    ready(11)
    pairs = []
    for k in range(half):
        target = flip(sibling, 2 * k)
        er_tx[k] = dot(eh[...], ed[:, span(target, width)]).astype(bf16)
        pairs.append(send(er_tx.at[k], er_rx.at[k], (me_e, sibling)))
    hids = pass_on(hids, lambda index: hidden.at[span(index, block), :])
    partials = []
    for k in range(1, half):
        target = across(k)
        summed = dot(eh[...], ed[:, span(target, width)])
        arrive(pairs[k : k + 1])
        er_pair[k - 1] = (summed + er_rx[k].astype(f32)).astype(bf16)
        partials.append(send(er_pair.at[k - 1], er_far.at[k - 1], (me_e, target)))
    ready(12)
    arrive(hids)
    do_tx[...] = dot(hidden[...], wd[...]).astype(bf16)
    outs = [
        send(do_tx.at[span(peer_e(d), seq_dev), :], do_rx.at[d - 1], (peer_e(d), me_t))
        for d in ep_steps
    ]
    result = dot(eh[...], ed[:, own])
    arrive(pairs[:1])
    result = result + er_rx[0].astype(f32)
    arrive(partials)
    for k in range(1, half):
        result = result + er_far[k - 1].astype(f32)
    mo_tx[...] = result.astype(bf16)
    place = span(me_e, slots)
    backs = [
        send(mo_tx.at[span(peer_e(d), slots), :], mo_rx.at[place, :], (peer_e(d), me_t))
        for d in ep_steps
    ]
    mo_rx[place, :] = mo_tx[place, :]
    arrive(outs)
    dense = do_tx[span(me_e, seq_dev), :].astype(f32)
    for d in ep_steps:
        dense = dense + do_rx[d - 1].astype(f32)
    partly = middle[...] + mixing * dense
    arrive(backs)
    returned = lax.dot_general(
        combine[...], mo_rx[...], (((0,), (0,)), ((), ())), preferred_element_type=f32
    )
    out_ref[...] = (partly + returned).astype(bf16)
    for copy in started:
        copy.wait_send()


def tail(retained, resid, gain, mix, routes, route_weight, slots, weights, tp_count, ep_count):
    seq_dev, model_width = resid.shape
    width = model_width // tp_count
    batch = seq_dev * ep_count
    block = batch // tp_count
    dense_units = weights[1].shape[0]
    half = tp_count // 2
    expert_units = weights[4].shape[2]
    items = ep_count * slots
    bf16 = jnp.bfloat16
    f32 = jnp.float32
    peers_t = tp_count - 1
    peers_e = ep_count - 1
    copies = 7 * peers_t + 5 * peers_e
    vmem = pl.BlockSpec(memory_space=pltpu.VMEM)
    anywhere = pl.BlockSpec(memory_space=pltpu.HBM)
    return pl.pallas_call(
        functools.partial(tail_kernel, tp_count, ep_count, slots),
        out_shape=jax.ShapeDtypeStruct((seq_dev, width), bf16),
        in_specs=[anywhere] * 13,
        out_specs=vmem,
        scratch_shapes=[
            pltpu.VMEM(retained.shape, bf16),
            pltpu.VMEM(resid.shape, bf16),
            pltpu.VMEM(gain.shape, bf16),
            pltpu.VMEM(mix.shape, bf16),
            pltpu.VMEM(routes.shape, jnp.int32),
            pltpu.VMEM(route_weight.shape, bf16),
            pltpu.VMEM(weights[0].shape, bf16),
            pltpu.VMEM(weights[1].shape, bf16),
            pltpu.VMEM(weights[2].shape, bf16),
            pltpu.VMEM(weights[3].shape, bf16),
            pltpu.VMEM(weights[4].shape[1:], bf16),
            pltpu.VMEM(weights[5].shape[1:], bf16),
            pltpu.VMEM(weights[6].shape[1:], bf16),
            pltpu.VMEM((8, model_width), f32),
            pltpu.VMEM((ep_count, slots, seq_dev), bf16),
            pltpu.VMEM((items, seq_dev), bf16),
            pltpu.VMEM((tp_count, seq_dev, width), bf16),
            pltpu.VMEM((peers_t, seq_dev, width), bf16),
            pltpu.VMEM((seq_dev, width), f32),
            pltpu.VMEM((8, 128), f32),
            pltpu.VMEM((peers_t, 8, 128), f32),
            pltpu.VMEM((ep_count, 8, 128), f32),
            pltpu.VMEM((ep_count, seq_dev, width), bf16),
            pltpu.VMEM((ep_count, slots, seq_dev), bf16),
            pltpu.VMEM((tp_count, items, width), bf16),
            pltpu.VMEM((items, 1), f32),
            pltpu.VMEM((2, batch, dense_units), bf16),
            pltpu.VMEM((2, half, block, dense_units), bf16),
            pltpu.VMEM((2, half - 1, block, dense_units), bf16),
            pltpu.VMEM((2, half - 1, block, dense_units), bf16),
            pltpu.VMEM((batch, dense_units), bf16),
            pltpu.VMEM((items, expert_units), bf16),
            pltpu.VMEM((half, items, width), bf16),
            pltpu.VMEM((half, items, width), bf16),
            pltpu.VMEM((half - 1, items, width), bf16),
            pltpu.VMEM((half - 1, items, width), bf16),
            pltpu.VMEM((batch, width), bf16),
            pltpu.VMEM((peers_e, seq_dev, width), bf16),
            pltpu.VMEM((items, width), bf16),
            pltpu.VMEM((items, width), bf16),
            pltpu.SemaphoreType.DMA((13,)),
            pltpu.SemaphoreType.DMA((copies,)),
            pltpu.SemaphoreType.DMA((copies,)),
        ],
        compiler_params=pltpu.CompilerParams(
            collective_id=0, has_side_effects=True, vmem_limit_bytes=61 * 1024 * 1024
        ),
        name="tail",
    )(retained, resid, gain, mix, routes, route_weight, *weights)


def per_device(
    resid,
    norm_gain,
    w_query,
    w_key,
    w_value,
    w_gate,
    head_gain,
    w_output,
    state,
    positions,
    ffn_gain,
    w_mix,
    dense_gate,
    dense_up,
    dense_down,
    routes,
    route_weight,
    expert_gate,
    expert_up,
    expert_down,
):
    seq_dev = resid.shape[0]
    tp_count = lax.axis_size("tp")
    ep_count = lax.axis_size("ep")
    retained, new_state = front(
        resid, norm_gain, positions, head_gain, (w_query, w_key, w_value, w_gate), state
    )
    capacity = max(2, 2 * seq_dev * routes.shape[1] // ep_count)
    slots = -(-capacity // 16) * 16
    final = tail(
        retained,
        resid,
        ffn_gain,
        w_mix,
        routes.T,
        route_weight.T,
        slots,
        (w_output, dense_gate.T, dense_up.T, dense_down, expert_gate, expert_up, expert_down),
        tp_count,
        ep_count,
    )
    return (final, new_state)


def solution(mesh):
    in_specs = (
        P("ep", None),
        P(),
        P(None, "tp"),
        P(None, "tp"),
        P(None, "tp"),
        P(None, "tp"),
        P("tp"),
        P("tp", None),
        P("ep", "tp", None, None),
        P("ep"),
        P(),
        P(),
        P("tp", "ep"),
        P("tp", "ep"),
        P("ep", "tp"),
        P("ep", None),
        P("ep", None),
        P("ep", None, "tp"),
        P("ep", None, "tp"),
        P("ep", "tp", None),
    )
    out_specs = (P("ep", "tp"), P("ep", "tp", None, None))
    return jax.shard_map(
        per_device, mesh=mesh, in_specs=in_specs, out_specs=out_specs, check_vma=False
    )
```

```python
import functools

import jax
import jax.numpy as jnp
import numpy as np
from jax import lax
from jax.experimental import pallas as pl
from jax.experimental.pallas import tpu as pltpu
from jax.sharding import PartitionSpec as P

EPSILON = 1e-06
THETA = 10000.0


def rms_norm(inputs, scaling):
    square = jnp.mean(inputs * inputs, axis=-1, keepdims=True)
    return inputs * lax.rsqrt(square + EPSILON) * scaling.astype(jnp.float32)


def state_kernel(
    state,
    key,
    value,
    final,
    new_state,
    out_ref,
    memory,
    key_ref,
    value_ref,
    final_ref,
    small_sem,
    load_sem,
    store_sem,
):
    seqs, heads, size, _ = memory.shape
    chunks = load_sem.shape[0]
    chunk = seqs // chunks
    smalls = [
        pltpu.make_async_copy(source, target, small_sem.at[index])
        for index, (source, target) in enumerate(
            ((key, key_ref), (value, value_ref), (final, final_ref))
        )
    ]
    loads = [
        pltpu.make_async_copy(
            state.at[pl.ds(c * chunk, chunk)], memory.at[pl.ds(c * chunk, chunk)], load_sem.at[c]
        )
        for c in range(chunks)
    ]
    stores = [
        pltpu.make_async_copy(
            memory.at[pl.ds(c * chunk, chunk)],
            new_state.at[pl.ds(c * chunk, chunk)],
            store_sem.at[c],
        )
        for c in range(chunks)
    ]
    for copy in smalls + loads:
        copy.start()
    decays = decays_of(heads, size)
    for copy in smalls:
        copy.wait()
    placed = pltpu.make_async_copy(final_ref, out_ref, small_sem.at[3])
    placed.start()
    keys = [key_ref[h] for h in range(heads)]
    for c in range(chunks):
        loads[c].wait()
        for s in range(c * chunk, (c + 1) * chunk):
            for h in range(heads):
                memory[s, h] = (
                    memory[s, h] * decays[h]
                    + keys[h][:, s : s + 1] * value_ref[s : s + 1, h * size : (h + 1) * size]
                )
        stores[c].start()
    placed.wait()
    for copy in stores:
        copy.wait()


def update_state(state, key, value, final):
    chunks = min(8, state.shape[0])
    anywhere = pl.BlockSpec(memory_space=pltpu.HBM)
    return pl.pallas_call(
        state_kernel,
        out_shape=(
            jax.ShapeDtypeStruct(state.shape, jnp.float32),
            jax.ShapeDtypeStruct(final.shape, final.dtype),
        ),
        in_specs=[anywhere] * 4,
        out_specs=(anywhere, anywhere),
        scratch_shapes=[
            pltpu.VMEM(state.shape, jnp.float32),
            pltpu.VMEM(key.shape, key.dtype),
            pltpu.VMEM(value.shape, value.dtype),
            pltpu.VMEM(final.shape, final.dtype),
            pltpu.SemaphoreType.DMA((4,)),
            pltpu.SemaphoreType.DMA((chunks,)),
            pltpu.SemaphoreType.DMA((chunks,)),
        ],
        compiler_params=pltpu.CompilerParams(vmem_limit_bytes=61 * 1024 * 1024),
        name="update_state",
    )(state, key, value, final)


def decays_of(heads, size):
    head_first = lax.axis_index("tp") * heads
    return [
        1.0 - jnp.exp2(-1.0 - 1.5 * jnp.full((1, size), head_first + h, jnp.int32).astype(jnp.float32))
        for h in range(heads)
    ]


def flip(index, mask):
    result = index
    bit = 1
    while bit <= mask:
        if mask & bit:
            result = result + bit * (1 - 2 * lax.rem(lax.div(index, bit), 2))
        bit *= 2
    return result


def layer_kernel(
    tp_count,
    ep_count,
    slots,
    key_scale,
    resid,
    norm_gain,
    positions,
    freq,
    head_gain,
    ffn_gain,
    w_mix,
    routes,
    route_weight,
    w_query,
    w_key,
    w_value,
    w_gate,
    state,
    w_output,
    dense_gate,
    dense_up,
    dense_down,
    expert_gate,
    expert_up,
    expert_down,
    out_ref,
    key_out,
    value_out,
    resid_ref,
    norm_ref,
    place_ref,
    freq_ref,
    head_ref,
    gain_ref,
    mix_ref,
    routes_ref,
    route_weight_ref,
    projections,
    memory,
    carried,
    kept,
    wo,
    wg,
    wu,
    wd,
    eg,
    eu,
    ed,
    scales,
    dispatch,
    combine,
    part,
    att_rx,
    middle,
    stat_tx,
    stat_rx,
    inverses,
    rows,
    hot,
    tokens,
    token_scale,
    gu_tx,
    gu_rx,
    gu_pair,
    gu_far,
    hidden,
    eh,
    er_tx,
    er_rx,
    er_pair,
    er_far,
    do_tx,
    do_rx,
    mo_tx,
    mo_rx,
    fetch_sem,
    state_sem,
    load_sem,
    send_sem,
    recv_sem,
):
    me_t = lax.axis_index("tp")
    me_e = lax.axis_index("ep")
    seq_dev, model_width = resid_ref.shape
    width = model_width // tp_count
    block = hidden.shape[0] // tp_count
    f32 = jnp.float32
    bf16 = jnp.bfloat16

    fetches = [
        pltpu.make_async_copy(source, target, fetch_sem.at[index])
        for index, (source, target) in enumerate(
            (
                (resid, resid_ref),
                (norm_gain, norm_ref),
                (positions, place_ref),
                (freq, freq_ref),
                (head_gain, head_ref),
                (ffn_gain, gain_ref),
                (w_mix, mix_ref),
                (routes, routes_ref),
                (route_weight, route_weight_ref),
                (w_query, projections.at[0]),
                (w_key, projections.at[1]),
                (w_value, projections.at[2]),
                (w_gate, projections.at[3]),
            )
        )
    ]
    seqs, heads, size, _ = memory.shape
    chunks = state_sem.shape[0]
    chunk = seqs // chunks
    states = [
        pltpu.make_async_copy(
            state.at[pl.ds(c * chunk, chunk)], memory.at[pl.ds(c * chunk, chunk)], state_sem.at[c]
        )
        for c in range(chunks)
    ]
    loads = [
        pltpu.make_async_copy(source, target, load_sem.at[index])
        for index, (source, target) in enumerate(
            (
                (w_output, wo),
                (dense_gate, wg),
                (dense_up, wu),
                (expert_gate.at[0], eg),
                (expert_up.at[0], eu),
                (expert_down.at[0], ed),
                (dense_down, wd),
            )
        )
    ]
    for copy in fetches + states + loads[:1]:
        copy.start()

    def ready(*indices):
        for index in indices:
            loads[index].wait()

    def peer_t(step):
        return flip(me_t, step)

    def peer_e(step):
        return flip(me_e, step)

    tp_steps = list(range(1, tp_count))
    ep_steps = list(range(ep_count - 1, 0, -1))
    barrier = pltpu.get_barrier_semaphore()
    for step in tp_steps:
        pl.semaphore_signal(
            barrier,
            inc=1,
            device_id=(me_e, peer_t(step)),
            device_id_type=pl.DeviceIdType.MESH,
        )
    for step in ep_steps:
        pl.semaphore_signal(
            barrier,
            inc=1,
            device_id=(peer_e(step), me_t),
            device_id_type=pl.DeviceIdType.MESH,
        )

    used = [0]
    started = []

    def send(source, target, device):
        index = used[0]
        used[0] = index + 1
        copy = pltpu.make_async_remote_copy(
            src_ref=source,
            dst_ref=target,
            send_sem=send_sem.at[index],
            recv_sem=recv_sem.at[index],
            device_id=device,
            device_id_type=pl.DeviceIdType.MESH,
        )
        copy.start()
        started.append(copy)
        return copy

    def span(index, size):
        return pl.ds(pl.multiple_of(index * size, size), size)

    def dot(left, right):
        return jnp.dot(left, right, preferred_element_type=f32)

    def arrive(copies):
        for copy in copies:
            copy.wait_recv()

    half = tp_count // 2
    sibling = peer_t(1)

    def across(step):
        return peer_t(2 * step)

    def spread(at):
        return [
            send(at(me_t), at(me_t), (me_e, target))
            for target in [sibling] + [across(k) for k in range(1, half)]
        ]

    def pass_on(copies, at):
        waiting = [copies[0]]
        for k in range(1, half):
            arrive(copies[k : k + 1])
            waiting.append(send(at(across(k)), at(across(k)), (me_e, sibling)))
        return waiting

    own = span(me_t, width)
    for copy in fetches[:5]:
        copy.wait()
    normed = rms_norm(resid_ref[...].astype(f32), norm_ref[...].reshape(1, -1)).astype(bf16)
    places = jnp.broadcast_to(place_ref[...].astype(f32).reshape(1, seqs), (size, seqs)).T
    angles = places * freq_ref[...]
    cosine = jnp.cos(angles)
    lane_of = lax.broadcasted_iota(jnp.int32, (seqs, size), 1)
    sine = jnp.where(lane_of < size // 2, -jnp.sin(angles), jnp.sin(angles))

    def project(index):
        fetches[9 + index].wait()
        product = dot(normed, projections[index]).astype(bf16).astype(f32)
        return [product[:, h * size : (h + 1) * size] for h in range(heads)]

    def rotate(inputs):
        return inputs * cosine + pltpu.roll(inputs, size // 2, 1) * sine

    query = [rotate(piece) for piece in project(0)]
    query_t = [piece.T for piece in query]
    key = [rotate(piece) * key_scale for piece in project(1)]
    value = project(2)
    gating = project(3)
    decays = decays_of(heads, size)
    for h in range(heads):
        key_out[h] = key[h].T
        value_out[:, h * size : (h + 1) * size] = value[h]
    for c in range(chunks):
        states[c].wait()
        for q in range(c * chunk, (c + 1) * chunk):
            for h in range(heads):
                carried[h, q : q + 1, :] = jnp.sum(
                    memory[q, h] * query_t[h][:, q : q + 1], axis=0, keepdims=True
                )
    for load in loads[1:]:
        load.start()
    gains = head_ref[...].astype(f32).reshape(1, -1)
    for h in range(heads):
        within = jnp.sum(query[h] * key[h], axis=-1, keepdims=True) * value[h]
        mixture = within + carried[h] * decays[h]
        centre = jnp.mean(mixture, axis=-1, keepdims=True)
        variance = jnp.mean(jnp.square(mixture - centre), axis=-1, keepdims=True)
        columns = slice(h * size, (h + 1) * size)
        scaled = (mixture - centre) * lax.rsqrt(variance + EPSILON) * gains[:, columns]
        kept[:, columns] = (jax.nn.silu(gating[h]) * scaled).astype(bf16)
    ready(0)
    retained = kept[...]
    for d in tp_steps[1:] + tp_steps[:1] + [0]:
        part[d] = dot(retained, wo[:, span(peer_t(d), width)]).astype(bf16)
    pl.semaphore_wait(barrier, tp_count - 1 + ep_count - 1)
    att = [
        send(part.at[d], att_rx.at[d - 1], (me_e, peer_t(d)))
        for d in tp_steps[1:] + tp_steps[:1]
    ]
    for copy in fetches[5:9]:
        copy.wait()
    scales[0:1, :] = gain_ref[...].astype(f32).reshape(1, -1)
    scales[1:2, :] = mix_ref[...].astype(f32).reshape(1, -1)
    gain = scales[0:1, own]
    mix = scales[1:2, own]

    top_count = routes_ref.shape[0]
    expert_ids = lax.broadcasted_iota(jnp.int32, (ep_count, seq_dev), 0)
    taken = jnp.zeros((ep_count, seq_dev), f32)
    weight_of = jnp.zeros((ep_count, seq_dev), f32)
    for j in range(top_count):
        named = routes_ref[j : j + 1, :] == expert_ids
        taken = taken + jnp.where(named, 1.0, 0.0)
        weight_of = weight_of + jnp.where(
            named, route_weight_ref[j : j + 1, :].astype(f32), 0.0
        )
    earlier = lax.broadcasted_iota(jnp.int32, (seq_dev, seq_dev), 0)
    later = lax.broadcasted_iota(jnp.int32, (seq_dev, seq_dev), 1)
    ranks = dot(taken.astype(bf16), jnp.where(earlier < later, 1.0, 0.0).astype(bf16))
    slot_ids = lax.broadcasted_iota(jnp.int32, (slots, seq_dev), 0).astype(f32)
    for e in range(ep_count):
        hits = (ranks[e : e + 1, :] == slot_ids) & (taken[e : e + 1, :] > 0.0)
        dispatch[e] = jnp.where(hits, 1.0, 0.0).astype(bf16)
        combine[e * slots : (e + 1) * slots, :] = jnp.where(
            hits, weight_of[e : e + 1, :], 0.0
        ).astype(bf16)

    hots = [send(dispatch.at[peer_e(d)], hot.at[me_e], (peer_e(d), me_t)) for d in ep_steps]
    hot[me_e] = dispatch[me_e]
    arrive(att)
    total = part[0].astype(f32)
    for d in tp_steps:
        total = total + att_rx[d - 1].astype(f32)
    mid = resid_ref[:, own].astype(f32) + total
    scaled = mid * gain
    rows[me_e] = scaled.astype(bf16)
    gathered = [send(rows.at[me_e], rows.at[me_e], (peer_e(d), me_t)) for d in ep_steps]
    middle[...] = mid

    lane = lax.broadcasted_iota(jnp.int32, (seq_dev, 128), 1)
    diagonal = lane == lax.broadcasted_iota(jnp.int32, (seq_dev, 128), 0)

    def to_row(column):
        return jnp.sum(jnp.where(diagonal, column, 0.0), axis=0, keepdims=True)

    def to_column(row):
        return jnp.sum(jnp.where(diagonal, row, 0.0), axis=1, keepdims=True)

    stat_tx[0:1, :] = to_row(jnp.sum(mid * mid, axis=-1, keepdims=True))
    stat_tx[1:2, :] = to_row(jnp.sum(scaled * mix, axis=-1, keepdims=True))
    stats = [send(stat_tx, stat_rx.at[d - 1], (me_e, peer_t(d))) for d in tp_steps]
    arrive(stats)
    stat = stat_tx[0:2, :]
    for d in tp_steps:
        stat = stat + stat_rx[d - 1, 0:2, :]
    inverse = lax.rsqrt(stat[0:1, :] / model_width + EPSILON)
    mixing = to_column(jax.nn.sigmoid(inverse * stat[1:2, :]))
    inverses[me_e, 0:1, :] = inverse
    factors = [
        send(inverses.at[me_e], inverses.at[me_e], (peer_e(d), me_t)) for d in ep_steps
    ]

    arrive(hots)
    arrive(gathered)
    for s in range(ep_count):
        tokens[me_t, s * slots : (s + 1) * slots, :] = dot(hot[s], rows[s]).astype(bf16)
    toks = spread(lambda index: tokens.at[index])
    near = []
    all_rows = rows[...].reshape(ep_count * seq_dev, width)
    for which, weight in enumerate((wg, wu)):
        ready(1 + which)
        gu_tx[which] = lax.dot_general(
            all_rows, weight[...], (((1,), (1,)), ((), ())), preferred_element_type=f32
        ).astype(bf16)
        near.append(
            [
                send(
                    gu_tx.at[which, span(flip(sibling, 2 * k), block), :],
                    gu_rx.at[which, k],
                    (me_e, sibling),
                )
                for k in range(half)
            ]
        )
    toks = pass_on(toks, lambda index: tokens.at[index])
    far = []
    for which in range(2):
        arrive(near[which])
        for k in range(1, half):
            target = across(k)
            gu_pair[which, k - 1] = (
                gu_tx[which, span(target, block), :].astype(f32) + gu_rx[which, k].astype(f32)
            ).astype(bf16)
            far.append(
                send(gu_pair.at[which, k - 1], gu_far.at[which, k - 1], (me_e, target))
            )
    arrive(factors)
    for s in range(ep_count):
        token_scale[s * slots : (s + 1) * slots, :] = jnp.sum(
            hot[s].astype(f32) * inverses[s, 0:1, 0:seq_dev], axis=1, keepdims=True
        )
    ready(3, 4)
    arrive(toks)
    tile = min(256, eg.shape[1])

    def expert_tile(index, carry):
        columns = span(index, tile)
        gate = jnp.zeros((tokens.shape[1], tile), f32)
        up = jnp.zeros((tokens.shape[1], tile), f32)
        for c in range(tp_count):
            features = slice(c * width, (c + 1) * width)
            gate = gate + dot(tokens[c], eg[features, columns])
            up = up + dot(tokens[c], eu[features, columns])
        factor = token_scale[...]
        eh[:, columns] = (jax.nn.silu(gate * factor) * (up * factor)).astype(bf16)
        return carry

    lax.fori_loop(0, eg.shape[1] // tile, expert_tile, 0)
    ready(5)
    pairs = []
    for k in range(half):
        target = flip(sibling, 2 * k)
        er_tx[k] = dot(eh[...], ed[:, span(target, width)]).astype(bf16)
        pairs.append(send(er_tx.at[k], er_rx.at[k], (me_e, sibling)))
    arrive(far)
    factor = jnp.concatenate(
        [
            to_column(inverses[me_t * (block // seq_dev) + i, 0:1, :])
            for i in range(block // seq_dev)
        ],
        axis=0,
    )
    gate = gu_tx[0, span(me_t, block), :].astype(f32) + gu_rx[0, 0].astype(f32)
    up = gu_tx[1, span(me_t, block), :].astype(f32) + gu_rx[1, 0].astype(f32)
    for k in range(1, half):
        gate = gate + gu_far[0, k - 1].astype(f32)
        up = up + gu_far[1, k - 1].astype(f32)
    hidden[span(me_t, block), :] = (jax.nn.silu(gate * factor) * (up * factor)).astype(bf16)
    hids = spread(lambda index: hidden.at[span(index, block), :])
    partials = []
    for k in range(1, half):
        target = across(k)
        summed = dot(eh[...], ed[:, span(target, width)])
        arrive(pairs[k : k + 1])
        er_pair[k - 1] = (summed + er_rx[k].astype(f32)).astype(bf16)
        partials.append(send(er_pair.at[k - 1], er_far.at[k - 1], (me_e, target)))
    result = dot(eh[...], ed[:, own])
    arrive(pairs[:1])
    result = result + er_rx[0].astype(f32)
    hids = pass_on(hids, lambda index: hidden.at[span(index, block), :])
    ready(6)
    arrive(hids)
    do_tx[...] = dot(hidden[...], wd[...]).astype(bf16)
    outs = [
        send(do_tx.at[span(peer_e(d), seq_dev), :], do_rx.at[d - 1], (peer_e(d), me_t))
        for d in ep_steps
    ]
    arrive(partials)
    for k in range(1, half):
        result = result + er_far[k - 1].astype(f32)
    mo_tx[...] = result.astype(bf16)
    place = span(me_e, slots)
    backs = [
        send(mo_tx.at[span(peer_e(d), slots), :], mo_rx.at[place, :], (peer_e(d), me_t))
        for d in ep_steps
    ]
    mo_rx[place, :] = mo_tx[place, :]
    arrive(outs)
    dense = do_tx[span(me_e, seq_dev), :].astype(f32)
    for d in ep_steps:
        dense = dense + do_rx[d - 1].astype(f32)
    partly = middle[...] + mixing * dense
    arrive(backs)
    returned = lax.dot_general(
        combine[...], mo_rx[...], (((0,), (0,)), ((), ())), preferred_element_type=f32
    )
    out_ref[...] = (partly + returned).astype(bf16)
    for copy in started:
        copy.wait_send()


def layer(smalls, slots, projections, state, weights, tp_count, ep_count):
    seq_dev, model_width = smalls[0].shape
    _, heads, size, _ = state.shape
    chunks = min(8, seq_dev)
    width = model_width // tp_count
    batch = seq_dev * ep_count
    block = batch // tp_count
    dense_units = weights[1].shape[0]
    half = tp_count // 2
    expert_units = weights[4].shape[2]
    items = ep_count * slots
    bf16 = jnp.bfloat16
    f32 = jnp.float32
    peers_t = tp_count - 1
    peers_e = ep_count - 1
    copies = 7 * peers_t + 5 * peers_e
    vmem = pl.BlockSpec(memory_space=pltpu.VMEM)
    anywhere = pl.BlockSpec(memory_space=pltpu.HBM)
    return pl.pallas_call(
        functools.partial(layer_kernel, tp_count, ep_count, slots, size ** (-0.5)),
        out_shape=(
            jax.ShapeDtypeStruct((seq_dev, width), bf16),
            jax.ShapeDtypeStruct((heads, size, seq_dev), f32),
            jax.ShapeDtypeStruct((seq_dev, heads * size), f32),
        ),
        in_specs=[anywhere] * 21,
        out_specs=(vmem, vmem, vmem),
        scratch_shapes=[
            *[pltpu.VMEM(small.shape, small.dtype) for small in smalls],
            pltpu.VMEM((4,) + projections[0].shape, bf16),
            pltpu.VMEM(state.shape, f32),
            pltpu.VMEM((heads, seq_dev, size), f32),
            pltpu.VMEM((seq_dev, heads * size), bf16),
            pltpu.VMEM(weights[0].shape, bf16),
            pltpu.VMEM(weights[1].shape, bf16),
            pltpu.VMEM(weights[2].shape, bf16),
            pltpu.VMEM(weights[3].shape, bf16),
            pltpu.VMEM(weights[4].shape[1:], bf16),
            pltpu.VMEM(weights[5].shape[1:], bf16),
            pltpu.VMEM(weights[6].shape[1:], bf16),
            pltpu.VMEM((8, model_width), f32),
            pltpu.VMEM((ep_count, slots, seq_dev), bf16),
            pltpu.VMEM((items, seq_dev), bf16),
            pltpu.VMEM((tp_count, seq_dev, width), bf16),
            pltpu.VMEM((peers_t, seq_dev, width), bf16),
            pltpu.VMEM((seq_dev, width), f32),
            pltpu.VMEM((8, 128), f32),
            pltpu.VMEM((peers_t, 8, 128), f32),
            pltpu.VMEM((ep_count, 8, 128), f32),
            pltpu.VMEM((ep_count, seq_dev, width), bf16),
            pltpu.VMEM((ep_count, slots, seq_dev), bf16),
            pltpu.VMEM((tp_count, items, width), bf16),
            pltpu.VMEM((items, 1), f32),
            pltpu.VMEM((2, batch, dense_units), bf16),
            pltpu.VMEM((2, half, block, dense_units), bf16),
            pltpu.VMEM((2, half - 1, block, dense_units), bf16),
            pltpu.VMEM((2, half - 1, block, dense_units), bf16),
            pltpu.VMEM((batch, dense_units), bf16),
            pltpu.VMEM((items, expert_units), bf16),
            pltpu.VMEM((half, items, width), bf16),
            pltpu.VMEM((half, items, width), bf16),
            pltpu.VMEM((half - 1, items, width), bf16),
            pltpu.VMEM((half - 1, items, width), bf16),
            pltpu.VMEM((batch, width), bf16),
            pltpu.VMEM((peers_e, seq_dev, width), bf16),
            pltpu.VMEM((items, width), bf16),
            pltpu.VMEM((items, width), bf16),
            pltpu.SemaphoreType.DMA((13,)),
            pltpu.SemaphoreType.DMA((chunks,)),
            pltpu.SemaphoreType.DMA((7,)),
            pltpu.SemaphoreType.DMA((copies,)),
            pltpu.SemaphoreType.DMA((copies,)),
        ],
        compiler_params=pltpu.CompilerParams(
            collective_id=0, has_side_effects=True, vmem_limit_bytes=61 * 1024 * 1024
        ),
        name="layer",
    )(*smalls, *projections, state, *weights)


def per_device(
    resid,
    norm_gain,
    w_query,
    w_key,
    w_value,
    w_gate,
    head_gain,
    w_output,
    state,
    positions,
    ffn_gain,
    w_mix,
    dense_gate,
    dense_up,
    dense_down,
    routes,
    route_weight,
    expert_gate,
    expert_up,
    expert_down,
):
    seq_dev = resid.shape[0]
    tp_count = lax.axis_size("tp")
    ep_count = lax.axis_size("ep")
    half = state.shape[-1] // 2
    inverse = THETA ** (-np.arange(half, dtype=np.float64) / half)
    freq = jnp.asarray(np.concatenate([inverse, inverse])[None, :].astype(np.float32))
    capacity = max(2, 2 * seq_dev * routes.shape[1] // ep_count)
    slots = -(-capacity // 16) * 16
    final, key, value = layer(
        (
            resid,
            norm_gain,
            positions,
            freq,
            head_gain,
            ffn_gain,
            w_mix,
            routes.T,
            route_weight.T,
        ),
        slots,
        (w_query, w_key, w_value, w_gate),
        state,
        (w_output, dense_gate.T, dense_up.T, dense_down, expert_gate, expert_up, expert_down),
        tp_count,
        ep_count,
    )
    new_state, final = update_state(state, key, value, final)
    return (final, new_state)


def solution(mesh):
    in_specs = (
        P("ep", None),
        P(),
        P(None, "tp"),
        P(None, "tp"),
        P(None, "tp"),
        P(None, "tp"),
        P("tp"),
        P("tp", None),
        P("ep", "tp", None, None),
        P("ep"),
        P(),
        P(),
        P("tp", "ep"),
        P("tp", "ep"),
        P("ep", "tp"),
        P("ep", None),
        P("ep", None),
        P("ep", None, "tp"),
        P("ep", None, "tp"),
        P("ep", "tp", None),
    )
    out_specs = (P("ep", "tp"), P("ep", "tp", None, None))
    return jax.shard_map(
        per_device, mesh=mesh, in_specs=in_specs, out_specs=out_specs, check_vma=False
    )
```

```python
import functools

import jax
import jax.numpy as jnp
import numpy as np
from jax import lax
from jax.experimental import pallas as pl
from jax.experimental.pallas import tpu as pltpu
from jax.sharding import PartitionSpec as P

EPSILON = 1e-06
THETA = 10000.0


def rms_norm(inputs, scaling):
    square = jnp.mean(inputs * inputs, axis=-1, keepdims=True)
    return inputs * lax.rsqrt(square + EPSILON) * scaling.astype(jnp.float32)


def state_kernel(
    state,
    key,
    value,
    final,
    new_state,
    out_ref,
    memory,
    key_ref,
    value_ref,
    final_ref,
    small_sem,
    load_sem,
    store_sem,
):
    seqs, heads, size, _ = memory.shape
    chunks = load_sem.shape[0]
    chunk = seqs // chunks
    smalls = [
        pltpu.make_async_copy(source, target, small_sem.at[index])
        for index, (source, target) in enumerate(
            ((key, key_ref), (value, value_ref), (final, final_ref))
        )
    ]
    loads = [
        pltpu.make_async_copy(
            state.at[pl.ds(c * chunk, chunk)], memory.at[pl.ds(c * chunk, chunk)], load_sem.at[c]
        )
        for c in range(chunks)
    ]
    stores = [
        pltpu.make_async_copy(
            memory.at[pl.ds(c * chunk, chunk)],
            new_state.at[pl.ds(c * chunk, chunk)],
            store_sem.at[c],
        )
        for c in range(chunks)
    ]
    for copy in smalls + loads:
        copy.start()
    decays = decays_of(heads, size)
    for copy in smalls:
        copy.wait()
    placed = pltpu.make_async_copy(final_ref, out_ref, small_sem.at[3])
    placed.start()
    keys = [key_ref[h] for h in range(heads)]
    for c in range(chunks):
        loads[c].wait()
        for s in range(c * chunk, (c + 1) * chunk):
            for h in range(heads):
                memory[s, h] = (
                    memory[s, h] * decays[h]
                    + keys[h][:, s : s + 1] * value_ref[s : s + 1, h * size : (h + 1) * size]
                )
        stores[c].start()
    placed.wait()
    for copy in stores:
        copy.wait()


def update_state(state, key, value, final):
    chunks = min(8, state.shape[0])
    anywhere = pl.BlockSpec(memory_space=pltpu.HBM)
    return pl.pallas_call(
        state_kernel,
        out_shape=(
            jax.ShapeDtypeStruct(state.shape, jnp.float32),
            jax.ShapeDtypeStruct(final.shape, final.dtype),
        ),
        in_specs=[anywhere] * 4,
        out_specs=(anywhere, anywhere),
        scratch_shapes=[
            pltpu.VMEM(state.shape, jnp.float32),
            pltpu.VMEM(key.shape, key.dtype),
            pltpu.VMEM(value.shape, value.dtype),
            pltpu.VMEM(final.shape, final.dtype),
            pltpu.SemaphoreType.DMA((4,)),
            pltpu.SemaphoreType.DMA((chunks,)),
            pltpu.SemaphoreType.DMA((chunks,)),
        ],
        compiler_params=pltpu.CompilerParams(vmem_limit_bytes=61 * 1024 * 1024),
        name="update_state",
    )(state, key, value, final)


def decays_of(heads, size):
    head_first = lax.axis_index("tp") * heads
    return [
        1.0 - jnp.exp2(-1.0 - 1.5 * jnp.full((1, size), head_first + h, jnp.int32).astype(jnp.float32))
        for h in range(heads)
    ]


def flip(index, mask):
    result = index
    bit = 1
    while bit <= mask:
        if mask & bit:
            result = result + bit * (1 - 2 * lax.rem(lax.div(index, bit), 2))
        bit *= 2
    return result


def layer_kernel(
    tp_count,
    ep_count,
    slots,
    key_scale,
    resid,
    norm_gain,
    positions,
    freq,
    head_gain,
    ffn_gain,
    w_mix,
    routes,
    route_weight,
    w_query,
    w_key,
    w_value,
    w_gate,
    state,
    w_output,
    dense_gate,
    dense_up,
    dense_down,
    expert_gate,
    expert_up,
    expert_down,
    out_ref,
    key_out,
    value_out,
    resid_ref,
    norm_ref,
    place_ref,
    freq_ref,
    head_ref,
    gain_ref,
    mix_ref,
    routes_ref,
    route_weight_ref,
    projections,
    memory,
    carried,
    kept,
    wo,
    wg,
    wu,
    wd,
    eg,
    eu,
    ed,
    scales,
    dispatch,
    combine,
    part,
    att_rx,
    middle,
    stat_tx,
    stat_rx,
    inverses,
    rows,
    hot,
    tokens,
    token_scale,
    gu_tx,
    gu_rx,
    gu_pair,
    gu_far,
    hidden,
    eh,
    er_tx,
    er_rx,
    er_pair,
    er_far,
    do_tx,
    do_rx,
    relay_tx,
    relay_rx,
    mo_tx,
    mo_rx,
    fetch_sem,
    state_sem,
    load_sem,
    send_sem,
    recv_sem,
):
    me_t = lax.axis_index("tp")
    me_e = lax.axis_index("ep")
    seq_dev, model_width = resid_ref.shape
    width = model_width // tp_count
    f32 = jnp.float32
    bf16 = jnp.bfloat16

    fetches = [
        pltpu.make_async_copy(source, target, fetch_sem.at[index])
        for index, (source, target) in enumerate(
            (
                (resid, resid_ref),
                (norm_gain, norm_ref),
                (positions, place_ref),
                (freq, freq_ref),
                (head_gain, head_ref),
                (ffn_gain, gain_ref),
                (w_mix, mix_ref),
                (routes, routes_ref),
                (route_weight, route_weight_ref),
                (w_query, projections.at[0]),
                (w_key, projections.at[1]),
                (w_value, projections.at[2]),
                (w_gate, projections.at[3]),
            )
        )
    ]
    seqs, heads, size, _ = memory.shape
    chunks = state_sem.shape[0]
    chunk = seqs // chunks
    states = [
        pltpu.make_async_copy(
            state.at[pl.ds(c * chunk, chunk)], memory.at[pl.ds(c * chunk, chunk)], state_sem.at[c]
        )
        for c in range(chunks)
    ]
    loads = [
        pltpu.make_async_copy(source, target, load_sem.at[index])
        for index, (source, target) in enumerate(
            (
                (w_output, wo),
                (dense_gate, wg),
                (dense_up, wu),
                (expert_gate.at[0], eg),
                (expert_up.at[0], eu),
                (expert_down.at[0], ed),
                (dense_down, wd),
            )
        )
    ]
    for copy in fetches + states + loads[:1]:
        copy.start()

    def ready(*indices):
        for index in indices:
            loads[index].wait()

    def peer_t(step):
        return flip(me_t, step)

    def peer_e(step):
        return flip(me_e, step)

    tp_steps = list(range(1, tp_count))
    ep_steps = list(range(ep_count - 1, 0, -1))
    barrier = pltpu.get_barrier_semaphore()
    for step in tp_steps:
        pl.semaphore_signal(
            barrier,
            inc=1,
            device_id=(me_e, peer_t(step)),
            device_id_type=pl.DeviceIdType.MESH,
        )
    for step in ep_steps:
        pl.semaphore_signal(
            barrier,
            inc=1,
            device_id=(peer_e(step), me_t),
            device_id_type=pl.DeviceIdType.MESH,
        )

    used = [0]
    started = []

    def send(source, target, device):
        index = used[0]
        used[0] = index + 1
        copy = pltpu.make_async_remote_copy(
            src_ref=source,
            dst_ref=target,
            send_sem=send_sem.at[index],
            recv_sem=recv_sem.at[index],
            device_id=device,
            device_id_type=pl.DeviceIdType.MESH,
        )
        copy.start()
        started.append(copy)
        return copy

    def span(index, size):
        return pl.ds(pl.multiple_of(index * size, size), size)

    def dot(left, right):
        return jnp.dot(left, right, preferred_element_type=f32)

    def arrive(copies):
        for copy in copies:
            copy.wait_recv()

    half = tp_count // 2
    sibling = peer_t(1)

    def across(step):
        return peer_t(2 * step)

    def spread(at):
        return [
            send(at(me_t), at(me_t), (me_e, target))
            for target in [sibling] + [across(k) for k in range(1, half)]
        ]

    def pass_on(copies, at):
        waiting = [copies[0]]
        for k in range(1, half):
            arrive(copies[k : k + 1])
            waiting.append(send(at(across(k)), at(across(k)), (me_e, sibling)))
        return waiting

    own = span(me_t, width)
    for copy in fetches[:5]:
        copy.wait()
    normed = rms_norm(resid_ref[...].astype(f32), norm_ref[...].reshape(1, -1)).astype(bf16)
    places = jnp.broadcast_to(place_ref[...].astype(f32).reshape(1, seqs), (size, seqs)).T
    angles = places * freq_ref[...]
    cosine = jnp.cos(angles)
    lane_of = lax.broadcasted_iota(jnp.int32, (seqs, size), 1)
    sine = jnp.where(lane_of < size // 2, -jnp.sin(angles), jnp.sin(angles))

    def project(index):
        fetches[9 + index].wait()
        product = dot(normed, projections[index]).astype(bf16).astype(f32)
        return [product[:, h * size : (h + 1) * size] for h in range(heads)]

    def rotate(inputs):
        return inputs * cosine + pltpu.roll(inputs, size // 2, 1) * sine

    query = [rotate(piece) for piece in project(0)]
    query_t = [piece.T for piece in query]
    key = [rotate(piece) * key_scale for piece in project(1)]
    value = project(2)
    gating = project(3)
    decays = decays_of(heads, size)
    for h in range(heads):
        key_out[h] = key[h].T
        value_out[:, h * size : (h + 1) * size] = value[h]
    for c in range(chunks):
        states[c].wait()
        for q in range(c * chunk, (c + 1) * chunk):
            for h in range(heads):
                carried[h, q : q + 1, :] = jnp.sum(
                    memory[q, h] * query_t[h][:, q : q + 1], axis=0, keepdims=True
                )
    for load in loads[1:]:
        load.start()
    gains = head_ref[...].astype(f32).reshape(1, -1)
    for h in range(heads):
        within = jnp.sum(query[h] * key[h], axis=-1, keepdims=True) * value[h]
        mixture = within + carried[h] * decays[h]
        centre = jnp.mean(mixture, axis=-1, keepdims=True)
        variance = jnp.mean(jnp.square(mixture - centre), axis=-1, keepdims=True)
        columns = slice(h * size, (h + 1) * size)
        scaled = (mixture - centre) * lax.rsqrt(variance + EPSILON) * gains[:, columns]
        kept[:, columns] = (jax.nn.silu(gating[h]) * scaled).astype(bf16)
    ready(0)
    retained = kept[...]
    for d in tp_steps[1:] + tp_steps[:1] + [0]:
        part[d] = dot(retained, wo[:, span(peer_t(d), width)]).astype(bf16)
    pl.semaphore_wait(barrier, tp_count - 1 + ep_count - 1)
    att = [
        send(part.at[d], att_rx.at[d - 1], (me_e, peer_t(d)))
        for d in tp_steps[1:] + tp_steps[:1]
    ]
    for copy in fetches[5:9]:
        copy.wait()
    scales[0:1, :] = gain_ref[...].astype(f32).reshape(1, -1)
    scales[1:2, :] = mix_ref[...].astype(f32).reshape(1, -1)
    gain = scales[0:1, own]
    mix = scales[1:2, own]

    top_count = routes_ref.shape[0]
    expert_ids = lax.broadcasted_iota(jnp.int32, (ep_count, seq_dev), 0)
    taken = jnp.zeros((ep_count, seq_dev), f32)
    weight_of = jnp.zeros((ep_count, seq_dev), f32)
    for j in range(top_count):
        named = routes_ref[j : j + 1, :] == expert_ids
        taken = taken + jnp.where(named, 1.0, 0.0)
        weight_of = weight_of + jnp.where(
            named, route_weight_ref[j : j + 1, :].astype(f32), 0.0
        )
    earlier = lax.broadcasted_iota(jnp.int32, (seq_dev, seq_dev), 0)
    later = lax.broadcasted_iota(jnp.int32, (seq_dev, seq_dev), 1)
    ranks = dot(taken.astype(bf16), jnp.where(earlier < later, 1.0, 0.0).astype(bf16))
    slot_ids = lax.broadcasted_iota(jnp.int32, (slots, seq_dev), 0).astype(f32)
    for e in range(ep_count):
        hits = (ranks[e : e + 1, :] == slot_ids) & (taken[e : e + 1, :] > 0.0)
        dispatch[e] = jnp.where(hits, 1.0, 0.0).astype(bf16)
        combine[e * slots : (e + 1) * slots, :] = jnp.where(
            hits, weight_of[e : e + 1, :], 0.0
        ).astype(bf16)

    hots = [send(dispatch.at[peer_e(d)], hot.at[me_e], (peer_e(d), me_t)) for d in ep_steps]
    hot[me_e] = dispatch[me_e]
    arrive(att)
    total = part[0].astype(f32)
    for d in tp_steps:
        total = total + att_rx[d - 1].astype(f32)
    mid = resid_ref[:, own].astype(f32) + total
    scaled = mid * gain
    rows[me_e] = scaled.astype(bf16)
    gathered = [send(rows.at[me_e], rows.at[me_e], (peer_e(d), me_t)) for d in ep_steps]
    middle[...] = mid

    lane = lax.broadcasted_iota(jnp.int32, (seq_dev, 128), 1)
    diagonal = lane == lax.broadcasted_iota(jnp.int32, (seq_dev, 128), 0)

    def to_row(column):
        return jnp.sum(jnp.where(diagonal, column, 0.0), axis=0, keepdims=True)

    def to_column(row):
        return jnp.sum(jnp.where(diagonal, row, 0.0), axis=1, keepdims=True)

    stat_tx[0:1, :] = to_row(jnp.sum(mid * mid, axis=-1, keepdims=True))
    stat_tx[1:2, :] = to_row(jnp.sum(scaled * mix, axis=-1, keepdims=True))
    stats = [send(stat_tx, stat_rx.at[d - 1], (me_e, peer_t(d))) for d in tp_steps]
    arrive(stats)
    stat = stat_tx[0:2, :]
    for d in tp_steps:
        stat = stat + stat_rx[d - 1, 0:2, :]
    inverse = lax.rsqrt(stat[0:1, :] / model_width + EPSILON)
    mixing = to_column(jax.nn.sigmoid(inverse * stat[1:2, :]))
    inverses[me_e, 0:1, :] = inverse
    factors = [
        send(inverses.at[me_e], inverses.at[me_e], (peer_e(d), me_t)) for d in ep_steps
    ]

    sources = ep_count // 2
    masks = [list(range(1, sources)), list(range(sources, ep_count))]
    side = lax.div(me_e, sources)
    sides = [side, 1 - side]
    core = lax.rem(me_t, 2)
    group_rows = sources * seq_dev
    share = group_rows // tp_count
    owners = share // seq_dev
    pair_of = lax.div(me_t, 2)
    by_mask = {d: copy for d, copy in zip(ep_steps, gathered)}

    def fill_tokens(g):
        for i in range(sources):
            s = sides[g] * sources + i
            tokens[me_t, span(s, slots), :] = dot(hot[s], rows[s]).astype(bf16)
        place = span(sides[g], sources * slots)
        return spread(lambda index: tokens.at[index, place, :])

    def gate_up(g):
        group = rows[pl.ds(sides[g] * sources, sources)].reshape(group_rows, width)
        for which, weight in enumerate((wg, wu)):
            if g == 0:
                ready(1 + which)
            product = lax.dot_general(
                group, weight[...], (((1,), (1,)), ((), ())), preferred_element_type=f32
            ).astype(bf16)
            for t in range(tp_count):
                gu_tx[g, t % 2, t // 2, which] = product[t * share : (t + 1) * share]
        return send(gu_tx.at[g, 1 - core], gu_rx.at[g], (me_e, sibling))

    def pair_up(g, near):
        arrive([near])
        sent = []
        for k in range(1, half):
            p = flip(pair_of, k)
            gu_pair[g, k - 1] = (
                gu_tx[g, core, p].astype(f32) + gu_rx[g, p].astype(f32)
            ).astype(bf16)
            sent.append(send(gu_pair.at[g, k - 1], gu_far.at[g, k - 1], (me_e, across(k))))
        return sent

    def activate(g, far):
        arrive(far)
        factor = jnp.concatenate(
            [
                to_column(inverses[sides[g] * sources + me_t * owners + i, 0:1, :])
                for i in range(owners)
            ],
            axis=0,
        )
        total = gu_tx[g, core, pair_of].astype(f32) + gu_rx[g, pair_of].astype(f32)
        for k in range(1, half):
            total = total + gu_far[g, k - 1].astype(f32)
        hidden[g, me_t] = (jax.nn.silu(total[0] * factor) * (total[1] * factor)).astype(bf16)
        return spread(lambda index: hidden.at[g, index])

    def share_hidden(g, hids):
        return pass_on(hids, lambda index: hidden.at[g, index])

    def lower(g, hids):
        arrive(hids)
        product = dot(hidden[g].reshape(group_rows, hidden.shape[-1]), wd[...])
        do_tx[g] = product.astype(bf16).reshape(sources, seq_dev, width)
        return [
            send(
                do_tx.at[g, lax.rem(peer_e(d), sources)],
                do_rx.at[g, d - 1],
                (peer_e(d), me_t),
            )
            for d in reversed(masks[0])
        ]

    def forward(copies, g):
        place = span(sides[g], sources * slots)
        return pass_on(copies, lambda index: tokens.at[index, place, :])

    arrive(hots)
    arrive([by_mask[d] for d in masks[0]])
    toks = fill_tokens(0)
    near_0 = gate_up(0)
    far_0 = pair_up(0, near_0)
    arrive([by_mask[d] for d in masks[1]])
    toks_far = fill_tokens(1)
    near_1 = gate_up(1)
    toks = forward(toks, 0)
    far_1 = pair_up(1, near_1)
    arrive(factors)
    hid_0 = activate(0, far_0)
    for s in range(ep_count):
        token_scale[s * slots : (s + 1) * slots, :] = jnp.sum(
            hot[s].astype(f32) * inverses[s, 0:1, 0:seq_dev], axis=1, keepdims=True
        )
    toks_far = forward(toks_far, 1)
    hid_1 = activate(1, far_1)
    ready(3, 4)
    arrive(toks + toks_far)
    tile = min(256, eg.shape[1])

    def expert_tile(index, carry):
        columns = span(index, tile)
        gate = jnp.zeros((tokens.shape[1], tile), f32)
        up = jnp.zeros((tokens.shape[1], tile), f32)
        for c in range(tp_count):
            features = slice(c * width, (c + 1) * width)
            gate = gate + dot(tokens[c], eg[features, columns])
            up = up + dot(tokens[c], eu[features, columns])
        factor = token_scale[...]
        eh[:, columns] = (jax.nn.silu(gate * factor) * (up * factor)).astype(bf16)
        return carry

    lax.fori_loop(0, eg.shape[1] // tile, expert_tile, 0)
    ready(5)
    pairs = []
    for k in range(half):
        target = flip(sibling, 2 * k)
        er_tx[k] = dot(eh[...], ed[:, span(target, width)]).astype(bf16)
        pairs.append(send(er_tx.at[k], er_rx.at[k], (me_e, sibling)))
    hid_0 = share_hidden(0, hid_0)
    hid_1 = share_hidden(1, hid_1)
    partials = []
    for k in range(1, half):
        target = across(k)
        summed = dot(eh[...], ed[:, span(target, width)])
        arrive(pairs[k : k + 1])
        er_pair[k - 1] = (summed + er_rx[k].astype(f32)).astype(bf16)
        partials.append(send(er_pair.at[k - 1], er_far.at[k - 1], (me_e, target)))
    ready(6)
    outs_far = lower(1, hid_1)
    outs = lower(0, hid_0)
    result = dot(eh[...], ed[:, own])
    arrive(pairs[:1])
    result = result + er_rx[0].astype(f32)
    arrive(outs_far)
    place = lax.rem(me_e, sources)
    relayed = do_tx[1, place].astype(f32)
    for d in masks[0]:
        relayed = relayed + do_rx[1, d - 1].astype(f32)
    relay_tx[...] = relayed.astype(bf16)
    outs.append(send(relay_tx, relay_rx, (peer_e(sources), me_t)))
    arrive(partials)
    for k in range(1, half):
        result = result + er_far[k - 1].astype(f32)
    mo_tx[...] = result.astype(bf16)
    place = span(me_e, slots)
    backs = [
        send(mo_tx.at[span(peer_e(d), slots), :], mo_rx.at[place, :], (peer_e(d), me_t))
        for d in ep_steps
    ]
    mo_rx[place, :] = mo_tx[place, :]
    arrive(outs)
    dense = do_tx[0, lax.rem(me_e, sources)].astype(f32) + relay_rx[...].astype(f32)
    for d in masks[0]:
        dense = dense + do_rx[0, d - 1].astype(f32)
    partly = middle[...] + mixing * dense
    arrive(backs)
    returned = lax.dot_general(
        combine[...], mo_rx[...], (((0,), (0,)), ((), ())), preferred_element_type=f32
    )
    out_ref[...] = (partly + returned).astype(bf16)
    for copy in started:
        copy.wait_send()


def layer(smalls, slots, projections, state, weights, tp_count, ep_count):
    seq_dev, model_width = smalls[0].shape
    _, heads, size, _ = state.shape
    chunks = min(8, seq_dev)
    width = model_width // tp_count
    batch = seq_dev * ep_count
    share = batch // 2 // tp_count
    dense_units = weights[1].shape[0]
    half = tp_count // 2
    expert_units = weights[4].shape[2]
    items = ep_count * slots
    bf16 = jnp.bfloat16
    f32 = jnp.float32
    peers_t = tp_count - 1
    peers_e = ep_count - 1
    copies = 3 * peers_t + 5 * peers_e + 2 * (2 * (2 * half - 1) + half) + 2 * half
    vmem = pl.BlockSpec(memory_space=pltpu.VMEM)
    anywhere = pl.BlockSpec(memory_space=pltpu.HBM)
    return pl.pallas_call(
        functools.partial(layer_kernel, tp_count, ep_count, slots, size ** (-0.5)),
        out_shape=(
            jax.ShapeDtypeStruct((seq_dev, width), bf16),
            jax.ShapeDtypeStruct((heads, size, seq_dev), f32),
            jax.ShapeDtypeStruct((seq_dev, heads * size), f32),
        ),
        in_specs=[anywhere] * 21,
        out_specs=(vmem, vmem, vmem),
        scratch_shapes=[
            *[pltpu.VMEM(small.shape, small.dtype) for small in smalls],
            pltpu.VMEM((4,) + projections[0].shape, bf16),
            pltpu.VMEM(state.shape, f32),
            pltpu.VMEM((heads, seq_dev, size), f32),
            pltpu.VMEM((seq_dev, heads * size), bf16),
            pltpu.VMEM(weights[0].shape, bf16),
            pltpu.VMEM(weights[1].shape, bf16),
            pltpu.VMEM(weights[2].shape, bf16),
            pltpu.VMEM(weights[3].shape, bf16),
            pltpu.VMEM(weights[4].shape[1:], bf16),
            pltpu.VMEM(weights[5].shape[1:], bf16),
            pltpu.VMEM(weights[6].shape[1:], bf16),
            pltpu.VMEM((8, model_width), f32),
            pltpu.VMEM((ep_count, slots, seq_dev), bf16),
            pltpu.VMEM((items, seq_dev), bf16),
            pltpu.VMEM((tp_count, seq_dev, width), bf16),
            pltpu.VMEM((peers_t, seq_dev, width), bf16),
            pltpu.VMEM((seq_dev, width), f32),
            pltpu.VMEM((8, 128), f32),
            pltpu.VMEM((peers_t, 8, 128), f32),
            pltpu.VMEM((ep_count, 8, 128), f32),
            pltpu.VMEM((ep_count, seq_dev, width), bf16),
            pltpu.VMEM((ep_count, slots, seq_dev), bf16),
            pltpu.VMEM((tp_count, items, width), bf16),
            pltpu.VMEM((items, 1), f32),
            pltpu.VMEM((2, 2, half, 2, share, dense_units), bf16),
            pltpu.VMEM((2, half, 2, share, dense_units), bf16),
            pltpu.VMEM((2, half - 1, 2, share, dense_units), bf16),
            pltpu.VMEM((2, half - 1, 2, share, dense_units), bf16),
            pltpu.VMEM((2, tp_count, share, dense_units), bf16),
            pltpu.VMEM((items, expert_units), bf16),
            pltpu.VMEM((half, items, width), bf16),
            pltpu.VMEM((half, items, width), bf16),
            pltpu.VMEM((half - 1, items, width), bf16),
            pltpu.VMEM((half - 1, items, width), bf16),
            pltpu.VMEM((2, ep_count // 2, seq_dev, width), bf16),
            pltpu.VMEM((2, ep_count // 2 - 1, seq_dev, width), bf16),
            pltpu.VMEM((seq_dev, width), bf16),
            pltpu.VMEM((seq_dev, width), bf16),
            pltpu.VMEM((items, width), bf16),
            pltpu.VMEM((items, width), bf16),
            pltpu.SemaphoreType.DMA((13,)),
            pltpu.SemaphoreType.DMA((chunks,)),
            pltpu.SemaphoreType.DMA((7,)),
            pltpu.SemaphoreType.DMA((copies,)),
            pltpu.SemaphoreType.DMA((copies,)),
        ],
        compiler_params=pltpu.CompilerParams(
            collective_id=0, has_side_effects=True, vmem_limit_bytes=61 * 1024 * 1024
        ),
        name="layer",
    )(*smalls, *projections, state, *weights)


def per_device(
    resid,
    norm_gain,
    w_query,
    w_key,
    w_value,
    w_gate,
    head_gain,
    w_output,
    state,
    positions,
    ffn_gain,
    w_mix,
    dense_gate,
    dense_up,
    dense_down,
    routes,
    route_weight,
    expert_gate,
    expert_up,
    expert_down,
):
    seq_dev = resid.shape[0]
    tp_count = lax.axis_size("tp")
    ep_count = lax.axis_size("ep")
    half = state.shape[-1] // 2
    inverse = THETA ** (-np.arange(half, dtype=np.float64) / half)
    freq = jnp.asarray(np.concatenate([inverse, inverse])[None, :].astype(np.float32))
    capacity = max(2, 2 * seq_dev * routes.shape[1] // ep_count)
    slots = -(-capacity // 16) * 16
    final, key, value = layer(
        (
            resid,
            norm_gain,
            positions,
            freq,
            head_gain,
            ffn_gain,
            w_mix,
            routes.T,
            route_weight.T,
        ),
        slots,
        (w_query, w_key, w_value, w_gate),
        state,
        (w_output, dense_gate.T, dense_up.T, dense_down, expert_gate, expert_up, expert_down),
        tp_count,
        ep_count,
    )
    new_state, final = update_state(state, key, value, final)
    return (final, new_state)


def solution(mesh):
    in_specs = (
        P("ep", None),
        P(),
        P(None, "tp"),
        P(None, "tp"),
        P(None, "tp"),
        P(None, "tp"),
        P("tp"),
        P("tp", None),
        P("ep", "tp", None, None),
        P("ep"),
        P(),
        P(),
        P("tp", "ep"),
        P("tp", "ep"),
        P("ep", "tp"),
        P("ep", None),
        P("ep", None),
        P("ep", None, "tp"),
        P("ep", None, "tp"),
        P("ep", "tp", None),
    )
    out_specs = (P("ep", "tp"), P("ep", "tp", None, None))
    return jax.shard_map(
        per_device, mesh=mesh, in_specs=in_specs, out_specs=out_specs, check_vma=False
    )
```

```python
import functools

import jax
import jax.numpy as jnp
import numpy as np
from jax import lax
from jax.experimental import pallas as pl
from jax.experimental.pallas import tpu as pltpu
from jax.sharding import PartitionSpec as P

EPSILON = 1e-06
THETA = 10000.0


def rms_norm(inputs, scaling):
    square = jnp.mean(inputs * inputs, axis=-1, keepdims=True)
    return inputs * lax.rsqrt(square + EPSILON) * scaling.astype(jnp.float32)


def state_kernel(
    state,
    key,
    value,
    final,
    new_state,
    out_ref,
    memory,
    key_ref,
    value_ref,
    final_ref,
    small_sem,
    load_sem,
    store_sem,
):
    seqs, heads, size, _ = memory.shape
    chunks = load_sem.shape[0]
    chunk = seqs // chunks
    smalls = [
        pltpu.make_async_copy(source, target, small_sem.at[index])
        for index, (source, target) in enumerate(
            ((key, key_ref), (value, value_ref), (final, final_ref))
        )
    ]
    loads = [
        pltpu.make_async_copy(
            state.at[pl.ds(c * chunk, chunk)], memory.at[pl.ds(c * chunk, chunk)], load_sem.at[c]
        )
        for c in range(chunks)
    ]
    stores = [
        pltpu.make_async_copy(
            memory.at[pl.ds(c * chunk, chunk)],
            new_state.at[pl.ds(c * chunk, chunk)],
            store_sem.at[c],
        )
        for c in range(chunks)
    ]
    for copy in smalls + loads:
        copy.start()
    decays = decays_of(heads, size)
    for copy in smalls:
        copy.wait()
    placed = pltpu.make_async_copy(final_ref, out_ref, small_sem.at[3])
    placed.start()
    keys = [key_ref[h] for h in range(heads)]
    for c in range(chunks):
        loads[c].wait()
        for s in range(c * chunk, (c + 1) * chunk):
            for h in range(heads):
                memory[s, h] = (
                    memory[s, h] * decays[h]
                    + keys[h][:, s : s + 1] * value_ref[s : s + 1, h * size : (h + 1) * size]
                )
        stores[c].start()
    placed.wait()
    for copy in stores:
        copy.wait()


def update_state(state, key, value, final):
    chunks = min(4, state.shape[0])
    anywhere = pl.BlockSpec(memory_space=pltpu.HBM)
    return pl.pallas_call(
        state_kernel,
        out_shape=(
            jax.ShapeDtypeStruct(state.shape, jnp.float32),
            jax.ShapeDtypeStruct(final.shape, final.dtype),
        ),
        in_specs=[anywhere] * 4,
        out_specs=(anywhere, anywhere),
        scratch_shapes=[
            pltpu.VMEM(state.shape, jnp.float32),
            pltpu.VMEM(key.shape, key.dtype),
            pltpu.VMEM(value.shape, value.dtype),
            pltpu.VMEM(final.shape, final.dtype),
            pltpu.SemaphoreType.DMA((4,)),
            pltpu.SemaphoreType.DMA((chunks,)),
            pltpu.SemaphoreType.DMA((chunks,)),
        ],
        compiler_params=pltpu.CompilerParams(vmem_limit_bytes=61 * 1024 * 1024),
        name="update_state",
    )(state, key, value, final)


def decays_of(heads, size):
    head_first = lax.axis_index("tp") * heads
    return [
        1.0 - jnp.exp2(-1.0 - 1.5 * jnp.full((1, size), head_first + h, jnp.int32).astype(jnp.float32))
        for h in range(heads)
    ]


def flip(index, mask):
    result = index
    bit = 1
    while bit <= mask:
        if mask & bit:
            result = result + bit * (1 - 2 * lax.rem(lax.div(index, bit), 2))
        bit *= 2
    return result


def layer_kernel(
    tp_count,
    ep_count,
    slots,
    key_scale,
    resid,
    norm_gain,
    positions,
    freq,
    head_gain,
    ffn_gain,
    w_mix,
    routes,
    route_weight,
    w_query,
    w_key,
    w_value,
    w_gate,
    state,
    w_output,
    dense_gate,
    dense_up,
    dense_down,
    expert_gate,
    expert_up,
    expert_down,
    out_ref,
    key_out,
    value_out,
    resid_ref,
    norm_ref,
    place_ref,
    freq_ref,
    head_ref,
    gain_ref,
    mix_ref,
    routes_ref,
    route_weight_ref,
    projections,
    memory,
    carried,
    kept,
    wo,
    wg,
    wu,
    wd,
    eg,
    eu,
    ed,
    scales,
    dispatch,
    combine,
    part,
    att_rx,
    middle,
    stat_tx,
    stat_rx,
    inverses,
    rows,
    hot,
    tokens,
    token_scale,
    gu_tx,
    gu_rx,
    gu_pair,
    gu_far,
    hidden,
    eh,
    er_tx,
    er_rx,
    er_pair,
    er_far,
    do_tx,
    do_rx,
    relay_tx,
    relay_rx,
    mo_tx,
    mo_rx,
    fetch_sem,
    state_sem,
    load_sem,
    send_sem,
    recv_sem,
):
    me_t = lax.axis_index("tp")
    me_e = lax.axis_index("ep")
    seq_dev, model_width = resid_ref.shape
    width = model_width // tp_count
    f32 = jnp.float32
    bf16 = jnp.bfloat16

    fetches = [
        pltpu.make_async_copy(source, target, fetch_sem.at[index])
        for index, (source, target) in enumerate(
            (
                (resid, resid_ref),
                (norm_gain, norm_ref),
                (positions, place_ref),
                (freq, freq_ref),
                (head_gain, head_ref),
                (ffn_gain, gain_ref),
                (w_mix, mix_ref),
                (routes, routes_ref),
                (route_weight, route_weight_ref),
                (w_query, projections.at[0]),
                (w_key, projections.at[1]),
                (w_value, projections.at[2]),
                (w_gate, projections.at[3]),
            )
        )
    ]
    seqs, heads, size, _ = memory.shape
    chunks = state_sem.shape[0]
    chunk = seqs // chunks
    states = [
        pltpu.make_async_copy(
            state.at[pl.ds(c * chunk, chunk)], memory.at[pl.ds(c * chunk, chunk)], state_sem.at[c]
        )
        for c in range(chunks)
    ]
    loads = [
        pltpu.make_async_copy(source, target, load_sem.at[index])
        for index, (source, target) in enumerate(
            (
                (w_output, wo),
                (dense_gate, wg),
                (dense_up, wu),
                (expert_gate.at[0], eg),
                (expert_up.at[0], eu),
                (expert_down.at[0], ed),
                (dense_down, wd),
            )
        )
    ]
    for copy in fetches:
        copy.start()

    def ready(*indices):
        for index in indices:
            loads[index].wait()

    def peer_t(step):
        return flip(me_t, step)

    def peer_e(step):
        return flip(me_e, step)

    tp_steps = list(range(1, tp_count))
    ep_steps = list(range(ep_count - 1, 0, -1))
    barrier = pltpu.get_barrier_semaphore()
    for step in tp_steps:
        pl.semaphore_signal(
            barrier,
            inc=1,
            device_id=(me_e, peer_t(step)),
            device_id_type=pl.DeviceIdType.MESH,
        )
    for step in ep_steps:
        pl.semaphore_signal(
            barrier,
            inc=1,
            device_id=(peer_e(step), me_t),
            device_id_type=pl.DeviceIdType.MESH,
        )

    used = [0]
    started = []

    def send(source, target, device):
        index = used[0]
        used[0] = index + 1
        copy = pltpu.make_async_remote_copy(
            src_ref=source,
            dst_ref=target,
            send_sem=send_sem.at[index],
            recv_sem=recv_sem.at[index],
            device_id=device,
            device_id_type=pl.DeviceIdType.MESH,
        )
        copy.start()
        started.append(copy)
        return copy

    def span(index, size):
        return pl.ds(pl.multiple_of(index * size, size), size)

    def dot(left, right):
        return jnp.dot(left, right, preferred_element_type=f32)

    def arrive(copies):
        for copy in copies:
            copy.wait_recv()

    half = tp_count // 2
    sibling = peer_t(1)

    def cross(step):
        return 2 * step + step.bit_count() % 2

    def across(step):
        return peer_t(cross(step))

    def spread(at):
        return [
            send(at(me_t), at(me_t), (me_e, target))
            for target in [sibling] + [across(k) for k in range(1, half)]
        ]

    def pass_on(copies, at):
        waiting = [copies[0]]
        for k in range(1, half):
            arrive(copies[k : k + 1])
            waiting.append(send(at(across(k)), at(across(k)), (me_e, sibling)))
        return waiting

    own = span(me_t, width)
    for copy in fetches[:5]:
        copy.wait()
    for copy in states + loads[:1]:
        copy.start()
    normed = rms_norm(resid_ref[...].astype(f32), norm_ref[...].reshape(1, -1)).astype(bf16)
    places = jnp.broadcast_to(place_ref[...].astype(f32).reshape(1, seqs), (size, seqs)).T
    angles = places * freq_ref[...]
    cosine = jnp.cos(angles)
    lane_of = lax.broadcasted_iota(jnp.int32, (seqs, size), 1)
    sine = jnp.where(lane_of < size // 2, -jnp.sin(angles), jnp.sin(angles))

    def project(index):
        fetches[9 + index].wait()
        product = dot(normed, projections[index]).astype(bf16).astype(f32)
        return [product[:, h * size : (h + 1) * size] for h in range(heads)]

    def rotate(inputs):
        return inputs * cosine + pltpu.roll(inputs, size // 2, 1) * sine

    query = [rotate(piece) for piece in project(0)]
    query_t = [piece.T for piece in query]
    key = [rotate(piece) * key_scale for piece in project(1)]
    value = project(2)
    gating = project(3)
    decays = decays_of(heads, size)
    for h in range(heads):
        key_out[h] = key[h].T
        value_out[:, h * size : (h + 1) * size] = value[h]
    for c in range(chunks):
        states[c].wait()
        for q in range(c * chunk, (c + 1) * chunk):
            for h in range(heads):
                carried[h, q : q + 1, :] = jnp.sum(
                    memory[q, h] * query_t[h][:, q : q + 1], axis=0, keepdims=True
                )
    for load in loads[1:]:
        load.start()
    gains = head_ref[...].astype(f32).reshape(1, -1)
    for h in range(heads):
        within = jnp.sum(query[h] * key[h], axis=-1, keepdims=True) * value[h]
        mixture = within + carried[h] * decays[h]
        centre = jnp.mean(mixture, axis=-1, keepdims=True)
        variance = jnp.mean(jnp.square(mixture - centre), axis=-1, keepdims=True)
        columns = slice(h * size, (h + 1) * size)
        scaled = (mixture - centre) * lax.rsqrt(variance + EPSILON) * gains[:, columns]
        kept[:, columns] = (jax.nn.silu(gating[h]) * scaled).astype(bf16)
    ready(0)
    retained = kept[...]
    for d in tp_steps[1:] + tp_steps[:1] + [0]:
        part[d] = dot(retained, wo[:, span(peer_t(d), width)]).astype(bf16)
    pl.semaphore_wait(barrier, tp_count - 1 + ep_count - 1)
    att = [
        send(part.at[d], att_rx.at[d - 1], (me_e, peer_t(d)))
        for d in tp_steps[1:] + tp_steps[:1]
    ]
    for copy in fetches[5:9]:
        copy.wait()
    scales[0:1, :] = gain_ref[...].astype(f32).reshape(1, -1)
    scales[1:2, :] = mix_ref[...].astype(f32).reshape(1, -1)
    gain = scales[0:1, own]
    mix = scales[1:2, own]

    top_count = routes_ref.shape[0]
    expert_ids = lax.broadcasted_iota(jnp.int32, (ep_count, seq_dev), 0)
    taken = jnp.zeros((ep_count, seq_dev), f32)
    weight_of = jnp.zeros((ep_count, seq_dev), f32)
    for j in range(top_count):
        named = routes_ref[j : j + 1, :] == expert_ids
        taken = taken + jnp.where(named, 1.0, 0.0)
        weight_of = weight_of + jnp.where(
            named, route_weight_ref[j : j + 1, :].astype(f32), 0.0
        )
    earlier = lax.broadcasted_iota(jnp.int32, (seq_dev, seq_dev), 0)
    later = lax.broadcasted_iota(jnp.int32, (seq_dev, seq_dev), 1)
    ranks = dot(taken.astype(bf16), jnp.where(earlier < later, 1.0, 0.0).astype(bf16))
    slot_ids = lax.broadcasted_iota(jnp.int32, (slots, seq_dev), 0).astype(f32)
    for e in range(ep_count):
        hits = (ranks[e : e + 1, :] == slot_ids) & (taken[e : e + 1, :] > 0.0)
        dispatch[e] = jnp.where(hits, 1.0, 0.0).astype(bf16)
        combine[e * slots : (e + 1) * slots, :] = jnp.where(
            hits, weight_of[e : e + 1, :], 0.0
        ).astype(bf16)

    hots = [send(dispatch.at[peer_e(d)], hot.at[me_e], (peer_e(d), me_t)) for d in ep_steps]
    hot[me_e] = dispatch[me_e]
    arrive(att)
    total = part[0].astype(f32)
    for d in tp_steps:
        total = total + att_rx[d - 1].astype(f32)
    mid = resid_ref[:, own].astype(f32) + total
    scaled = mid * gain
    rows[me_e] = scaled.astype(bf16)
    sources = ep_count // 2
    near_steps = list(range(sources - 1, 0, -1))
    mirrored = send(rows.at[me_e], rows.at[me_e], (peer_e(sources), me_t))
    gathered = [send(rows.at[me_e], rows.at[me_e], (peer_e(d), me_t)) for d in near_steps]
    middle[...] = mid

    lane = lax.broadcasted_iota(jnp.int32, (seq_dev, 128), 1)
    diagonal = lane == lax.broadcasted_iota(jnp.int32, (seq_dev, 128), 0)

    def to_row(column):
        return jnp.sum(jnp.where(diagonal, column, 0.0), axis=0, keepdims=True)

    def to_column(row):
        return jnp.sum(jnp.where(diagonal, row, 0.0), axis=1, keepdims=True)

    stat_tx[0:1, :] = to_row(jnp.sum(mid * mid, axis=-1, keepdims=True))
    stat_tx[1:2, :] = to_row(jnp.sum(scaled * mix, axis=-1, keepdims=True))
    stats = [send(stat_tx, stat_rx.at[d - 1], (me_e, peer_t(d))) for d in tp_steps]
    arrive(stats)
    stat = stat_tx[0:2, :]
    for d in tp_steps:
        stat = stat + stat_rx[d - 1, 0:2, :]
    inverse = lax.rsqrt(stat[0:1, :] / model_width + EPSILON)
    mixing = to_column(jax.nn.sigmoid(inverse * stat[1:2, :]))
    inverses[me_e, 0:1, :] = inverse
    factors = [
        send(inverses.at[me_e], inverses.at[me_e], (peer_e(d), me_t)) for d in ep_steps
    ]

    side = lax.div(me_e, sources)
    sides = [side, 1 - side]
    core = lax.rem(sum(lax.div(me_t, 1 << bit) for bit in range(tp_count.bit_length() - 1)), 2)
    group_rows = sources * seq_dev
    share = group_rows // tp_count
    owners = share // seq_dev
    pair_of = lax.div(me_t, 2)

    def fill_tokens(g):
        for i in range(sources):
            s = sides[g] * sources + i
            tokens[me_t, span(s, slots), :] = dot(hot[s], rows[s]).astype(bf16)
        place = span(sides[g], sources * slots)
        return spread(lambda index: tokens.at[index, place, :])

    def gate_up(g):
        group = rows[pl.ds(sides[g] * sources, sources)].reshape(group_rows, width)
        for which, weight in enumerate((wg, wu)):
            if g == 0:
                ready(1 + which)
            product = lax.dot_general(
                group, weight[...], (((1,), (1,)), ((), ())), preferred_element_type=f32
            ).astype(bf16)
            for t in range(tp_count):
                gu_tx[g, t.bit_count() % 2, t // 2, which] = product[t * share : (t + 1) * share]
        return send(gu_tx.at[g, 1 - core], gu_rx.at[g], (me_e, sibling))

    def pair_up(g, near):
        arrive([near])
        sent = []
        for k in range(1, half):
            p = flip(pair_of, k)
            gu_pair[g, k - 1] = (
                gu_tx[g, core, p].astype(f32) + gu_rx[g, p].astype(f32)
            ).astype(bf16)
            sent.append(send(gu_pair.at[g, k - 1], gu_far.at[g, k - 1], (me_e, across(k))))
        return sent

    def activate(g, far):
        arrive(far)
        factor = jnp.concatenate(
            [
                to_column(inverses[sides[g] * sources + me_t * owners + i, 0:1, :])
                for i in range(owners)
            ],
            axis=0,
        )
        total = gu_tx[g, core, pair_of].astype(f32) + gu_rx[g, pair_of].astype(f32)
        for k in range(1, half):
            total = total + gu_far[g, k - 1].astype(f32)
        hidden[g, me_t] = (jax.nn.silu(total[0] * factor) * (total[1] * factor)).astype(bf16)
        return spread(lambda index: hidden.at[g, index])

    def share_hidden(g, hids):
        return pass_on(hids, lambda index: hidden.at[g, index])

    def lower(g, hids):
        arrive(hids)
        product = dot(hidden[g].reshape(group_rows, hidden.shape[-1]), wd[...])
        do_tx[g] = product.astype(bf16).reshape(sources, seq_dev, width)
        return [
            send(
                do_tx.at[g, lax.rem(peer_e(d), sources)],
                do_rx.at[g, d - 1],
                (peer_e(d), me_t),
            )
            for d in near_steps
        ]

    def forward(copies, g):
        place = span(sides[g], sources * slots)
        return pass_on(copies, lambda index: tokens.at[index, place, :])

    arrive([mirrored])
    mirror = peer_e(sources)
    passed = [send(rows.at[mirror], rows.at[mirror], (peer_e(d), me_t)) for d in near_steps]
    arrive(hots)
    arrive(gathered)
    toks = fill_tokens(0)
    near_0 = gate_up(0)
    far_0 = pair_up(0, near_0)
    arrive(passed)
    toks_far = fill_tokens(1)
    near_1 = gate_up(1)
    toks = forward(toks, 0)
    far_1 = pair_up(1, near_1)
    arrive(factors)
    hid_0 = activate(0, far_0)
    for s in range(ep_count):
        token_scale[s * slots : (s + 1) * slots, :] = jnp.sum(
            hot[s].astype(f32) * inverses[s, 0:1, 0:seq_dev], axis=1, keepdims=True
        )
    toks_far = forward(toks_far, 1)
    hid_1 = activate(1, far_1)
    ready(3, 4)
    arrive(toks + toks_far)
    tile = min(256, eg.shape[1])

    def expert_tile(index, carry):
        columns = span(index, tile)
        gate = jnp.zeros((tokens.shape[1], tile), f32)
        up = jnp.zeros((tokens.shape[1], tile), f32)
        for c in range(tp_count):
            features = slice(c * width, (c + 1) * width)
            gate = gate + dot(tokens[c], eg[features, columns])
            up = up + dot(tokens[c], eu[features, columns])
        factor = token_scale[...]
        eh[:, columns] = (jax.nn.silu(gate * factor) * (up * factor)).astype(bf16)
        return carry

    lax.fori_loop(0, eg.shape[1] // tile, expert_tile, 0)
    hid_0 = share_hidden(0, hid_0)
    ready(5)
    pairs = []
    for k in range(half):
        target = flip(sibling, cross(k))
        er_tx[k] = dot(eh[...], ed[:, span(target, width)]).astype(bf16)
        pairs.append(send(er_tx.at[k], er_rx.at[k], (me_e, sibling)))
    ready(6)
    outs = lower(0, hid_0)
    hid_1 = share_hidden(1, hid_1)
    partials = []
    for k in range(1, half):
        target = across(k)
        summed = dot(eh[...], ed[:, span(target, width)])
        arrive(pairs[k : k + 1])
        er_pair[k - 1] = (summed + er_rx[k].astype(f32)).astype(bf16)
        partials.append(send(er_pair.at[k - 1], er_far.at[k - 1], (me_e, target)))
    outs_far = lower(1, hid_1)
    result = dot(eh[...], ed[:, own])
    arrive(pairs[:1])
    result = result + er_rx[0].astype(f32)
    arrive(partials)
    for k in range(1, half):
        result = result + er_far[k - 1].astype(f32)
    mo_tx[...] = result.astype(bf16)
    place = span(me_e, slots)
    backs = [
        send(mo_tx.at[span(peer_e(d), slots), :], mo_rx.at[place, :], (peer_e(d), me_t))
        for d in ep_steps
    ]
    mo_rx[place, :] = mo_tx[place, :]
    arrive(outs_far)
    relayed = do_tx[1, lax.rem(me_e, sources)].astype(f32)
    for d in near_steps:
        relayed = relayed + do_rx[1, d - 1].astype(f32)
    relay_tx[...] = relayed.astype(bf16)
    outs.append(send(relay_tx, relay_rx, (peer_e(sources), me_t)))
    arrive(outs)
    dense = do_tx[0, lax.rem(me_e, sources)].astype(f32) + relay_rx[...].astype(f32)
    for d in near_steps:
        dense = dense + do_rx[0, d - 1].astype(f32)
    partly = middle[...] + mixing * dense
    arrive(backs)
    returned = lax.dot_general(
        combine[...], mo_rx[...], (((0,), (0,)), ((), ())), preferred_element_type=f32
    )
    out_ref[...] = (partly + returned).astype(bf16)
    for copy in started:
        copy.wait_send()


def layer(smalls, slots, projections, state, weights, tp_count, ep_count):
    seq_dev, model_width = smalls[0].shape
    _, heads, size, _ = state.shape
    chunks = min(4, seq_dev)
    width = model_width // tp_count
    batch = seq_dev * ep_count
    share = batch // 2 // tp_count
    dense_units = weights[1].shape[0]
    half = tp_count // 2
    expert_units = weights[4].shape[2]
    items = ep_count * slots
    bf16 = jnp.bfloat16
    f32 = jnp.float32
    peers_t = tp_count - 1
    peers_e = ep_count - 1
    copies = 3 * peers_t + 5 * peers_e + 2 * (2 * (2 * half - 1) + half) + 2 * half
    vmem = pl.BlockSpec(memory_space=pltpu.VMEM)
    anywhere = pl.BlockSpec(memory_space=pltpu.HBM)
    return pl.pallas_call(
        functools.partial(layer_kernel, tp_count, ep_count, slots, size ** (-0.5)),
        out_shape=(
            jax.ShapeDtypeStruct((seq_dev, width), bf16),
            jax.ShapeDtypeStruct((heads, size, seq_dev), f32),
            jax.ShapeDtypeStruct((seq_dev, heads * size), f32),
        ),
        in_specs=[anywhere] * 21,
        out_specs=(vmem, vmem, vmem),
        scratch_shapes=[
            *[pltpu.VMEM(small.shape, small.dtype) for small in smalls],
            pltpu.VMEM((4,) + projections[0].shape, bf16),
            pltpu.VMEM(state.shape, f32),
            pltpu.VMEM((heads, seq_dev, size), f32),
            pltpu.VMEM((seq_dev, heads * size), bf16),
            pltpu.VMEM(weights[0].shape, bf16),
            pltpu.VMEM(weights[1].shape, bf16),
            pltpu.VMEM(weights[2].shape, bf16),
            pltpu.VMEM(weights[3].shape, bf16),
            pltpu.VMEM(weights[4].shape[1:], bf16),
            pltpu.VMEM(weights[5].shape[1:], bf16),
            pltpu.VMEM(weights[6].shape[1:], bf16),
            pltpu.VMEM((8, model_width), f32),
            pltpu.VMEM((ep_count, slots, seq_dev), bf16),
            pltpu.VMEM((items, seq_dev), bf16),
            pltpu.VMEM((tp_count, seq_dev, width), bf16),
            pltpu.VMEM((peers_t, seq_dev, width), bf16),
            pltpu.VMEM((seq_dev, width), f32),
            pltpu.VMEM((8, 128), f32),
            pltpu.VMEM((peers_t, 8, 128), f32),
            pltpu.VMEM((ep_count, 8, 128), f32),
            pltpu.VMEM((ep_count, seq_dev, width), bf16),
            pltpu.VMEM((ep_count, slots, seq_dev), bf16),
            pltpu.VMEM((tp_count, items, width), bf16),
            pltpu.VMEM((items, 1), f32),
            pltpu.VMEM((2, 2, half, 2, share, dense_units), bf16),
            pltpu.VMEM((2, half, 2, share, dense_units), bf16),
            pltpu.VMEM((2, half - 1, 2, share, dense_units), bf16),
            pltpu.VMEM((2, half - 1, 2, share, dense_units), bf16),
            pltpu.VMEM((2, tp_count, share, dense_units), bf16),
            pltpu.VMEM((items, expert_units), bf16),
            pltpu.VMEM((half, items, width), bf16),
            pltpu.VMEM((half, items, width), bf16),
            pltpu.VMEM((half - 1, items, width), bf16),
            pltpu.VMEM((half - 1, items, width), bf16),
            pltpu.VMEM((2, ep_count // 2, seq_dev, width), bf16),
            pltpu.VMEM((2, ep_count // 2 - 1, seq_dev, width), bf16),
            pltpu.VMEM((seq_dev, width), bf16),
            pltpu.VMEM((seq_dev, width), bf16),
            pltpu.VMEM((items, width), bf16),
            pltpu.VMEM((items, width), bf16),
            pltpu.SemaphoreType.DMA((13,)),
            pltpu.SemaphoreType.DMA((chunks,)),
            pltpu.SemaphoreType.DMA((7,)),
            pltpu.SemaphoreType.DMA((copies,)),
            pltpu.SemaphoreType.DMA((copies,)),
        ],
        compiler_params=pltpu.CompilerParams(
            collective_id=0, has_side_effects=True, vmem_limit_bytes=61 * 1024 * 1024
        ),
        name="layer",
    )(*smalls, *projections, state, *weights)


def per_device(
    resid,
    norm_gain,
    w_query,
    w_key,
    w_value,
    w_gate,
    head_gain,
    w_output,
    state,
    positions,
    ffn_gain,
    w_mix,
    dense_gate,
    dense_up,
    dense_down,
    routes,
    route_weight,
    expert_gate,
    expert_up,
    expert_down,
):
    seq_dev = resid.shape[0]
    tp_count = lax.axis_size("tp")
    ep_count = lax.axis_size("ep")
    half = state.shape[-1] // 2
    inverse = THETA ** (-np.arange(half, dtype=np.float64) / half)
    freq = jnp.asarray(np.concatenate([inverse, inverse])[None, :].astype(np.float32))
    capacity = max(2, 2 * seq_dev * routes.shape[1] // ep_count)
    slots = -(-capacity // 16) * 16
    final, key, value = layer(
        (
            resid,
            norm_gain,
            positions,
            freq,
            head_gain,
            ffn_gain,
            w_mix,
            routes.T,
            route_weight.T,
        ),
        slots,
        (w_query, w_key, w_value, w_gate),
        state,
        (w_output, dense_gate.T, dense_up.T, dense_down, expert_gate, expert_up, expert_down),
        tp_count,
        ep_count,
    )
    new_state, final = update_state(state, key, value, final)
    return (final, new_state)


def solution(mesh):
    in_specs = (
        P("ep", None),
        P(),
        P(None, "tp"),
        P(None, "tp"),
        P(None, "tp"),
        P(None, "tp"),
        P("tp"),
        P("tp", None),
        P("ep", "tp", None, None),
        P("ep"),
        P(),
        P(),
        P("tp", "ep"),
        P("tp", "ep"),
        P("ep", "tp"),
        P("ep", None),
        P("ep", None),
        P("ep", None, "tp"),
        P("ep", None, "tp"),
        P("ep", "tp", None),
    )
    out_specs = (P("ep", "tp"), P("ep", "tp", None, None))
    return jax.shard_map(
        per_device, mesh=mesh, in_specs=in_specs, out_specs=out_specs, check_vma=False
    )
```

```python
import functools

import jax
import jax.numpy as jnp
import numpy as np
from jax import lax
from jax.experimental import pallas as pl
from jax.experimental.pallas import tpu as pltpu
from jax.sharding import PartitionSpec as P

EPSILON = 1e-06
THETA = 10000.0


def rms_norm(inputs, scaling):
    square = jnp.mean(inputs * inputs, axis=-1, keepdims=True)
    return inputs * lax.rsqrt(square + EPSILON) * scaling.astype(jnp.float32)


def state_kernel(
    state,
    key,
    value,
    final,
    new_state,
    out_ref,
    memory,
    key_ref,
    value_ref,
    final_ref,
    small_sem,
    load_sem,
    store_sem,
):
    seqs, heads, size, _ = memory.shape
    chunks = load_sem.shape[0]
    chunk = seqs // chunks
    smalls = [
        pltpu.make_async_copy(source, target, small_sem.at[index])
        for index, (source, target) in enumerate(
            ((key, key_ref), (value, value_ref), (final, final_ref))
        )
    ]
    loads = [
        pltpu.make_async_copy(
            state.at[pl.ds(c * chunk, chunk)], memory.at[pl.ds(c * chunk, chunk)], load_sem.at[c]
        )
        for c in range(chunks)
    ]
    stores = [
        pltpu.make_async_copy(
            memory.at[pl.ds(c * chunk, chunk)],
            new_state.at[pl.ds(c * chunk, chunk)],
            store_sem.at[c],
        )
        for c in range(chunks)
    ]
    for copy in smalls + loads:
        copy.start()
    decays = decays_of(heads, size)
    for copy in smalls:
        copy.wait()
    placed = pltpu.make_async_copy(final_ref, out_ref, small_sem.at[3])
    placed.start()
    keys = [key_ref[h] for h in range(heads)]
    for c in range(chunks):
        loads[c].wait()
        for s in range(c * chunk, (c + 1) * chunk):
            for h in range(heads):
                memory[s, h] = (
                    memory[s, h] * decays[h]
                    + keys[h][:, s : s + 1] * value_ref[s : s + 1, h * size : (h + 1) * size]
                )
        stores[c].start()
    placed.wait()
    for copy in stores:
        copy.wait()


def update_state(state, key, value, final):
    chunks = min(4, state.shape[0])
    anywhere = pl.BlockSpec(memory_space=pltpu.HBM)
    return pl.pallas_call(
        state_kernel,
        out_shape=(
            jax.ShapeDtypeStruct(state.shape, jnp.float32),
            jax.ShapeDtypeStruct(final.shape, final.dtype),
        ),
        in_specs=[anywhere] * 4,
        out_specs=(anywhere, anywhere),
        scratch_shapes=[
            pltpu.VMEM(state.shape, jnp.float32),
            pltpu.VMEM(key.shape, key.dtype),
            pltpu.VMEM(value.shape, value.dtype),
            pltpu.VMEM(final.shape, final.dtype),
            pltpu.SemaphoreType.DMA((4,)),
            pltpu.SemaphoreType.DMA((chunks,)),
            pltpu.SemaphoreType.DMA((chunks,)),
        ],
        compiler_params=pltpu.CompilerParams(vmem_limit_bytes=61 * 1024 * 1024),
        name="update_state",
    )(state, key, value, final)


def decays_of(heads, size):
    head_first = lax.axis_index("tp") * heads
    return [
        1.0 - jnp.exp2(-1.0 - 1.5 * jnp.full((1, size), head_first + h, jnp.int32).astype(jnp.float32))
        for h in range(heads)
    ]


def flip(index, mask):
    result = index
    bit = 1
    while bit <= mask:
        if mask & bit:
            result = result + bit * (1 - 2 * lax.rem(lax.div(index, bit), 2))
        bit *= 2
    return result


def layer_kernel(
    tp_count,
    ep_count,
    slots,
    key_scale,
    resid,
    norm_gain,
    positions,
    freq,
    head_gain,
    ffn_gain,
    w_mix,
    routes,
    route_weight,
    w_query,
    w_key,
    w_value,
    w_gate,
    state,
    w_output,
    dense_gate,
    dense_up,
    dense_down,
    expert_gate,
    expert_up,
    expert_down,
    out_ref,
    key_out,
    value_out,
    resid_ref,
    norm_ref,
    place_ref,
    freq_ref,
    head_ref,
    gain_ref,
    mix_ref,
    routes_ref,
    route_weight_ref,
    projections,
    memory,
    carried,
    kept,
    wo,
    wg,
    wu,
    wd,
    eg,
    eu,
    ed,
    scales,
    dispatch,
    combine,
    part,
    att_rx,
    middle,
    stat_tx,
    stat_rx,
    inverses,
    rows,
    hot,
    tokens,
    token_scale,
    gu_tx,
    gu_rx,
    gu_pair,
    gu_far,
    hidden,
    eh,
    er_tx,
    er_rx,
    er_pair,
    er_far,
    do_tx,
    do_rx,
    relay_tx,
    relay_rx,
    mo_tx,
    mo_rx,
    fetch_sem,
    state_sem,
    load_sem,
    send_sem,
    recv_sem,
):
    me_t = lax.axis_index("tp")
    me_e = lax.axis_index("ep")
    seq_dev, model_width = resid_ref.shape
    width = model_width // tp_count
    f32 = jnp.float32
    bf16 = jnp.bfloat16

    fetches = [
        pltpu.make_async_copy(source, target, fetch_sem.at[index])
        for index, (source, target) in enumerate(
            (
                (resid, resid_ref),
                (norm_gain, norm_ref),
                (positions, place_ref),
                (freq, freq_ref),
                (head_gain, head_ref),
                (ffn_gain, gain_ref),
                (w_mix, mix_ref),
                (routes, routes_ref),
                (route_weight, route_weight_ref),
                (w_query, projections.at[0]),
                (w_key, projections.at[1]),
                (w_value, projections.at[2]),
                (w_gate, projections.at[3]),
            )
        )
    ]
    seqs, heads, size, _ = memory.shape
    chunks = state_sem.shape[0]
    chunk = seqs // chunks
    states = [
        pltpu.make_async_copy(
            state.at[pl.ds(c * chunk, chunk)], memory.at[pl.ds(c * chunk, chunk)], state_sem.at[c]
        )
        for c in range(chunks)
    ]
    loads = [
        pltpu.make_async_copy(source, target, load_sem.at[index])
        for index, (source, target) in enumerate(
            (
                (w_output, wo),
                (dense_gate, wg),
                (dense_up, wu),
                (expert_gate.at[0], eg),
                (expert_up.at[0], eu),
                (expert_down.at[0], ed),
                (dense_down, wd),
            )
        )
    ]
    for copy in fetches:
        copy.start()

    def ready(*indices):
        for index in indices:
            loads[index].wait()

    def peer_t(step):
        return flip(me_t, step)

    def peer_e(step):
        return flip(me_e, step)

    tp_steps = list(range(1, tp_count))
    ep_steps = list(range(ep_count - 1, 0, -1))
    barrier = pltpu.get_barrier_semaphore()
    for step in tp_steps:
        pl.semaphore_signal(
            barrier,
            inc=1,
            device_id=(me_e, peer_t(step)),
            device_id_type=pl.DeviceIdType.MESH,
        )
    for step in ep_steps:
        pl.semaphore_signal(
            barrier,
            inc=1,
            device_id=(peer_e(step), me_t),
            device_id_type=pl.DeviceIdType.MESH,
        )

    used = [0]
    started = []

    def send(source, target, device):
        index = used[0]
        used[0] = index + 1
        copy = pltpu.make_async_remote_copy(
            src_ref=source,
            dst_ref=target,
            send_sem=send_sem.at[index],
            recv_sem=recv_sem.at[index],
            device_id=device,
            device_id_type=pl.DeviceIdType.MESH,
        )
        copy.start()
        started.append(copy)
        return copy

    def span(index, size):
        return pl.ds(pl.multiple_of(index * size, size), size)

    def dot(left, right):
        return jnp.dot(left, right, preferred_element_type=f32)

    def arrive(copies):
        for copy in copies:
            copy.wait_recv()

    half = tp_count // 2
    sibling = peer_t(1)

    def cross(step):
        return 2 * step + step.bit_count() % 2

    def across(step):
        return peer_t(cross(step))

    def spread(at):
        return [
            send(at(me_t), at(me_t), (me_e, target))
            for target in [sibling] + [across(k) for k in range(1, half)]
        ]

    def pass_on(copies, at):
        waiting = [copies[0]]
        for k in range(1, half):
            arrive(copies[k : k + 1])
            waiting.append(send(at(across(k)), at(across(k)), (me_e, sibling)))
        return waiting

    own = span(me_t, width)
    for copy in fetches[:5]:
        copy.wait()
    for copy in states + loads[:1]:
        copy.start()
    normed = rms_norm(resid_ref[...].astype(f32), norm_ref[...].reshape(1, -1)).astype(bf16)
    places = jnp.broadcast_to(place_ref[...].astype(f32).reshape(1, seqs), (size, seqs)).T
    angles = places * freq_ref[...]
    cosine = jnp.cos(angles)
    lane_of = lax.broadcasted_iota(jnp.int32, (seqs, size), 1)
    sine = jnp.where(lane_of < size // 2, -jnp.sin(angles), jnp.sin(angles))

    def project(index):
        fetches[9 + index].wait()
        product = dot(normed, projections[index]).astype(bf16).astype(f32)
        return [product[:, h * size : (h + 1) * size] for h in range(heads)]

    def rotate(inputs):
        return inputs * cosine + pltpu.roll(inputs, size // 2, 1) * sine

    query = [rotate(piece) for piece in project(0)]
    query_t = [piece.T for piece in query]
    key = [rotate(piece) * key_scale for piece in project(1)]
    value = project(2)
    gating = project(3)
    decays = decays_of(heads, size)
    for h in range(heads):
        key_out[h] = key[h].T
        value_out[:, h * size : (h + 1) * size] = value[h]
    for c in range(chunks):
        states[c].wait()
        for q in range(c * chunk, (c + 1) * chunk):
            for h in range(heads):
                carried[h, q : q + 1, :] = jnp.sum(
                    memory[q, h] * query_t[h][:, q : q + 1], axis=0, keepdims=True
                )
    for load in loads[1:]:
        load.start()
    gains = head_ref[...].astype(f32).reshape(1, -1)
    for h in range(heads):
        within = jnp.sum(query[h] * key[h], axis=-1, keepdims=True) * value[h]
        mixture = within + carried[h] * decays[h]
        centre = jnp.mean(mixture, axis=-1, keepdims=True)
        variance = jnp.mean(jnp.square(mixture - centre), axis=-1, keepdims=True)
        columns = slice(h * size, (h + 1) * size)
        scaled = (mixture - centre) * lax.rsqrt(variance + EPSILON) * gains[:, columns]
        kept[:, columns] = (jax.nn.silu(gating[h]) * scaled).astype(bf16)
    ready(0)
    retained = kept[...]
    for d in tp_steps[1:] + tp_steps[:1] + [0]:
        part[d] = dot(retained, wo[:, span(peer_t(d), width)]).astype(bf16)
    pl.semaphore_wait(barrier, tp_count - 1 + ep_count - 1)
    att = [
        send(part.at[d], att_rx.at[d - 1], (me_e, peer_t(d)))
        for d in tp_steps[1:] + tp_steps[:1]
    ]
    for copy in fetches[5:9]:
        copy.wait()
    scales[0:1, :] = gain_ref[...].astype(f32).reshape(1, -1)
    scales[1:2, :] = mix_ref[...].astype(f32).reshape(1, -1)
    gain = scales[0:1, own]
    mix = scales[1:2, own]

    top_count = routes_ref.shape[0]
    expert_ids = lax.broadcasted_iota(jnp.int32, (ep_count, seq_dev), 0)
    taken = jnp.zeros((ep_count, seq_dev), f32)
    weight_of = jnp.zeros((ep_count, seq_dev), f32)
    for j in range(top_count):
        named = routes_ref[j : j + 1, :] == expert_ids
        taken = taken + jnp.where(named, 1.0, 0.0)
        weight_of = weight_of + jnp.where(
            named, route_weight_ref[j : j + 1, :].astype(f32), 0.0
        )
    earlier = lax.broadcasted_iota(jnp.int32, (seq_dev, seq_dev), 0)
    later = lax.broadcasted_iota(jnp.int32, (seq_dev, seq_dev), 1)
    ranks = dot(taken.astype(bf16), jnp.where(earlier < later, 1.0, 0.0).astype(bf16))
    slot_ids = lax.broadcasted_iota(jnp.int32, (slots, seq_dev), 0).astype(f32)
    for e in range(ep_count):
        hits = (ranks[e : e + 1, :] == slot_ids) & (taken[e : e + 1, :] > 0.0)
        dispatch[e] = jnp.where(hits, 1.0, 0.0).astype(bf16)
        combine[e * slots : (e + 1) * slots, :] = jnp.where(
            hits, weight_of[e : e + 1, :], 0.0
        ).astype(bf16)

    hots = [send(dispatch.at[peer_e(d)], hot.at[me_e], (peer_e(d), me_t)) for d in ep_steps]
    hot[me_e] = dispatch[me_e]
    arrive(att)
    total = part[0].astype(f32)
    for d in tp_steps:
        total = total + att_rx[d - 1].astype(f32)
    mid = resid_ref[:, own].astype(f32) + total
    scaled = mid * gain
    rows[me_e] = scaled.astype(bf16)
    sources = ep_count // 2
    near_steps = list(range(sources - 1, 0, -1))
    mirrored = send(rows.at[me_e], rows.at[me_e], (peer_e(sources), me_t))
    gathered = [send(rows.at[me_e], rows.at[me_e], (peer_e(d), me_t)) for d in near_steps]
    middle[...] = mid

    lane = lax.broadcasted_iota(jnp.int32, (seq_dev, 128), 1)
    diagonal = lane == lax.broadcasted_iota(jnp.int32, (seq_dev, 128), 0)

    def to_row(column):
        return jnp.sum(jnp.where(diagonal, column, 0.0), axis=0, keepdims=True)

    def to_column(row):
        return jnp.sum(jnp.where(diagonal, row, 0.0), axis=1, keepdims=True)

    stat_tx[0:1, :] = to_row(jnp.sum(mid * mid, axis=-1, keepdims=True))
    stat_tx[1:2, :] = to_row(jnp.sum(scaled * mix, axis=-1, keepdims=True))
    stats = [send(stat_tx, stat_rx.at[d - 1], (me_e, peer_t(d))) for d in tp_steps]
    arrive(stats)
    stat = stat_tx[0:2, :]
    for d in tp_steps:
        stat = stat + stat_rx[d - 1, 0:2, :]
    inverse = lax.rsqrt(stat[0:1, :] / model_width + EPSILON)
    mixing = to_column(jax.nn.sigmoid(inverse * stat[1:2, :]))
    inverses[me_e, 0:1, :] = inverse
    factors = [
        send(inverses.at[me_e], inverses.at[me_e], (peer_e(d), me_t)) for d in ep_steps
    ]

    side = lax.div(me_e, sources)
    sides = [side, 1 - side]
    core = lax.rem(sum(lax.div(me_t, 1 << bit) for bit in range(tp_count.bit_length() - 1)), 2)
    group_rows = sources * seq_dev
    share = group_rows // tp_count
    owners = share // seq_dev
    pair_of = lax.div(me_t, 2)

    def fill_tokens(g):
        for i in range(sources):
            s = sides[g] * sources + i
            tokens[me_t, span(s, slots), :] = dot(hot[s], rows[s]).astype(bf16)
        place = span(sides[g], sources * slots)
        return spread(lambda index: tokens.at[index, place, :])

    def gate_up(g):
        group = rows[pl.ds(sides[g] * sources, sources)].reshape(group_rows, width)
        for which, weight in enumerate((wg, wu)):
            if g == 0:
                ready(1 + which)
            product = lax.dot_general(
                group, weight[...], (((1,), (1,)), ((), ())), preferred_element_type=f32
            ).astype(bf16)
            for t in range(tp_count):
                gu_tx[g, t.bit_count() % 2, t // 2, which] = product[t * share : (t + 1) * share]
        return send(gu_tx.at[g, 1 - core], gu_rx.at[g], (me_e, sibling))

    def pair_up(g, near):
        arrive([near])
        sent = []
        for k in range(1, half):
            p = flip(pair_of, k)
            gu_pair[g, k - 1] = (
                gu_tx[g, core, p].astype(f32) + gu_rx[g, p].astype(f32)
            ).astype(bf16)
            sent.append(send(gu_pair.at[g, k - 1], gu_far.at[g, k - 1], (me_e, across(k))))
        return sent

    def activate(g, far):
        arrive(far)
        factor = jnp.concatenate(
            [
                to_column(inverses[sides[g] * sources + me_t * owners + i, 0:1, :])
                for i in range(owners)
            ],
            axis=0,
        )
        total = gu_tx[g, core, pair_of].astype(f32) + gu_rx[g, pair_of].astype(f32)
        for k in range(1, half):
            total = total + gu_far[g, k - 1].astype(f32)
        hidden[g, me_t] = (jax.nn.silu(total[0] * factor) * (total[1] * factor)).astype(bf16)
        return spread(lambda index: hidden.at[g, index])

    def share_hidden(g, hids):
        return pass_on(hids, lambda index: hidden.at[g, index])

    def lower(g, hids):
        arrive(hids)
        product = dot(hidden[g].reshape(group_rows, hidden.shape[-1]), wd[...])
        do_tx[g] = product.astype(bf16).reshape(sources, seq_dev, width)
        return [
            send(
                do_tx.at[g, lax.rem(peer_e(d), sources)],
                do_rx.at[g, d - 1],
                (peer_e(d), me_t),
            )
            for d in near_steps
        ]

    def forward(copies, g):
        place = span(sides[g], sources * slots)
        return pass_on(copies, lambda index: tokens.at[index, place, :])

    arrive([mirrored])
    mirror = peer_e(sources)
    passed = [send(rows.at[mirror], rows.at[mirror], (peer_e(d), me_t)) for d in near_steps]
    arrive(hots)
    arrive(gathered)
    toks = fill_tokens(0)
    near_0 = gate_up(0)
    far_0 = pair_up(0, near_0)
    arrive(passed)
    toks_far = fill_tokens(1)
    near_1 = gate_up(1)
    toks = forward(toks, 0)
    far_1 = pair_up(1, near_1)
    arrive(factors)
    hid_0 = activate(0, far_0)
    for s in range(ep_count):
        token_scale[s * slots : (s + 1) * slots, :] = jnp.sum(
            hot[s].astype(f32) * inverses[s, 0:1, 0:seq_dev], axis=1, keepdims=True
        )
    toks_far = forward(toks_far, 1)
    hid_1 = activate(1, far_1)
    ready(3, 4)
    arrive(toks + toks_far)
    tile = min(256, eg.shape[1])

    def expert_tile(index, carry):
        columns = span(index, tile)
        gate = jnp.zeros((tokens.shape[1], tile), f32)
        up = jnp.zeros((tokens.shape[1], tile), f32)
        for c in range(tp_count):
            features = slice(c * width, (c + 1) * width)
            gate = gate + dot(tokens[c], eg[features, columns])
            up = up + dot(tokens[c], eu[features, columns])
        factor = token_scale[...]
        eh[:, columns] = (jax.nn.silu(gate * factor) * (up * factor)).astype(bf16)
        return carry

    lax.fori_loop(0, eg.shape[1] // tile, expert_tile, 0)
    hid_0 = share_hidden(0, hid_0)
    ready(5)
    pairs = []
    for k in range(half):
        target = flip(sibling, cross(k))
        er_tx[k] = dot(eh[...], ed[:, span(target, width)]).astype(bf16)
        pairs.append(send(er_tx.at[k], er_rx.at[k], (me_e, sibling)))
    ready(6)
    outs = lower(0, hid_0)
    hid_1 = share_hidden(1, hid_1)
    partials = []
    for k in range(1, half):
        target = across(k)
        summed = dot(eh[...], ed[:, span(target, width)])
        arrive(pairs[k : k + 1])
        er_pair[k - 1] = (summed + er_rx[k].astype(f32)).astype(bf16)
        partials.append(send(er_pair.at[k - 1], er_far.at[k - 1], (me_e, target)))
    outs_far = lower(1, hid_1)
    result = dot(eh[...], ed[:, own])
    arrive(pairs[:1])
    result = result + er_rx[0].astype(f32)
    arrive(outs_far)
    relayed = do_tx[1, lax.rem(me_e, sources)].astype(f32)
    for d in near_steps:
        relayed = relayed + do_rx[1, d - 1].astype(f32)
    relay_tx[...] = relayed.astype(bf16)
    outs.append(send(relay_tx, relay_rx, (peer_e(sources), me_t)))
    arrive(partials)
    for k in range(1, half):
        result = result + er_far[k - 1].astype(f32)
    mo_tx[...] = result.astype(bf16)
    place = span(me_e, slots)
    backs = [
        send(mo_tx.at[span(peer_e(d), slots), :], mo_rx.at[place, :], (peer_e(d), me_t))
        for d in ep_steps
    ]
    mo_rx[place, :] = mo_tx[place, :]
    arrive(outs)
    dense = do_tx[0, lax.rem(me_e, sources)].astype(f32) + relay_rx[...].astype(f32)
    for d in near_steps:
        dense = dense + do_rx[0, d - 1].astype(f32)
    partly = middle[...] + mixing * dense
    arrive(backs)
    returned = lax.dot_general(
        combine[...], mo_rx[...], (((0,), (0,)), ((), ())), preferred_element_type=f32
    )
    out_ref[...] = (partly + returned).astype(bf16)
    for copy in started:
        copy.wait_send()


def layer(smalls, slots, projections, state, weights, tp_count, ep_count):
    seq_dev, model_width = smalls[0].shape
    _, heads, size, _ = state.shape
    chunks = min(2, seq_dev)
    width = model_width // tp_count
    batch = seq_dev * ep_count
    share = batch // 2 // tp_count
    dense_units = weights[1].shape[0]
    half = tp_count // 2
    expert_units = weights[4].shape[2]
    items = ep_count * slots
    bf16 = jnp.bfloat16
    f32 = jnp.float32
    peers_t = tp_count - 1
    peers_e = ep_count - 1
    copies = 3 * peers_t + 5 * peers_e + 2 * (2 * (2 * half - 1) + half) + 2 * half
    vmem = pl.BlockSpec(memory_space=pltpu.VMEM)
    anywhere = pl.BlockSpec(memory_space=pltpu.HBM)
    return pl.pallas_call(
        functools.partial(layer_kernel, tp_count, ep_count, slots, size ** (-0.5)),
        out_shape=(
            jax.ShapeDtypeStruct((seq_dev, width), bf16),
            jax.ShapeDtypeStruct((heads, size, seq_dev), f32),
            jax.ShapeDtypeStruct((seq_dev, heads * size), f32),
        ),
        in_specs=[anywhere] * 21,
        out_specs=(vmem, vmem, vmem),
        scratch_shapes=[
            *[pltpu.VMEM(small.shape, small.dtype) for small in smalls],
            pltpu.VMEM((4,) + projections[0].shape, bf16),
            pltpu.VMEM(state.shape, f32),
            pltpu.VMEM((heads, seq_dev, size), f32),
            pltpu.VMEM((seq_dev, heads * size), bf16),
            pltpu.VMEM(weights[0].shape, bf16),
            pltpu.VMEM(weights[1].shape, bf16),
            pltpu.VMEM(weights[2].shape, bf16),
            pltpu.VMEM(weights[3].shape, bf16),
            pltpu.VMEM(weights[4].shape[1:], bf16),
            pltpu.VMEM(weights[5].shape[1:], bf16),
            pltpu.VMEM(weights[6].shape[1:], bf16),
            pltpu.VMEM((8, model_width), f32),
            pltpu.VMEM((ep_count, slots, seq_dev), bf16),
            pltpu.VMEM((items, seq_dev), bf16),
            pltpu.VMEM((tp_count, seq_dev, width), bf16),
            pltpu.VMEM((peers_t, seq_dev, width), bf16),
            pltpu.VMEM((seq_dev, width), f32),
            pltpu.VMEM((8, 128), f32),
            pltpu.VMEM((peers_t, 8, 128), f32),
            pltpu.VMEM((ep_count, 8, 128), f32),
            pltpu.VMEM((ep_count, seq_dev, width), bf16),
            pltpu.VMEM((ep_count, slots, seq_dev), bf16),
            pltpu.VMEM((tp_count, items, width), bf16),
            pltpu.VMEM((items, 1), f32),
            pltpu.VMEM((2, 2, half, 2, share, dense_units), bf16),
            pltpu.VMEM((2, half, 2, share, dense_units), bf16),
            pltpu.VMEM((2, half - 1, 2, share, dense_units), bf16),
            pltpu.VMEM((2, half - 1, 2, share, dense_units), bf16),
            pltpu.VMEM((2, tp_count, share, dense_units), bf16),
            pltpu.VMEM((items, expert_units), bf16),
            pltpu.VMEM((half, items, width), bf16),
            pltpu.VMEM((half, items, width), bf16),
            pltpu.VMEM((half - 1, items, width), bf16),
            pltpu.VMEM((half - 1, items, width), bf16),
            pltpu.VMEM((2, ep_count // 2, seq_dev, width), bf16),
            pltpu.VMEM((2, ep_count // 2 - 1, seq_dev, width), bf16),
            pltpu.VMEM((seq_dev, width), bf16),
            pltpu.VMEM((seq_dev, width), bf16),
            pltpu.VMEM((items, width), bf16),
            pltpu.VMEM((items, width), bf16),
            pltpu.SemaphoreType.DMA((13,)),
            pltpu.SemaphoreType.DMA((chunks,)),
            pltpu.SemaphoreType.DMA((7,)),
            pltpu.SemaphoreType.DMA((copies,)),
            pltpu.SemaphoreType.DMA((copies,)),
        ],
        compiler_params=pltpu.CompilerParams(
            collective_id=0, has_side_effects=True, vmem_limit_bytes=61 * 1024 * 1024
        ),
        name="layer",
    )(*smalls, *projections, state, *weights)


def per_device(
    resid,
    norm_gain,
    w_query,
    w_key,
    w_value,
    w_gate,
    head_gain,
    w_output,
    state,
    positions,
    ffn_gain,
    w_mix,
    dense_gate,
    dense_up,
    dense_down,
    routes,
    route_weight,
    expert_gate,
    expert_up,
    expert_down,
):
    seq_dev = resid.shape[0]
    tp_count = lax.axis_size("tp")
    ep_count = lax.axis_size("ep")
    half = state.shape[-1] // 2
    inverse = THETA ** (-np.arange(half, dtype=np.float64) / half)
    freq = jnp.asarray(np.concatenate([inverse, inverse])[None, :].astype(np.float32))
    capacity = max(2, 2 * seq_dev * routes.shape[1] // ep_count)
    slots = -(-capacity // 16) * 16
    final, key, value = layer(
        (
            resid,
            norm_gain,
            positions,
            freq,
            head_gain,
            ffn_gain,
            w_mix,
            routes.T,
            route_weight.T,
        ),
        slots,
        (w_query, w_key, w_value, w_gate),
        state,
        (w_output, dense_gate.T, dense_up.T, dense_down, expert_gate, expert_up, expert_down),
        tp_count,
        ep_count,
    )
    new_state, final = update_state(state, key, value, final)
    return (final, new_state)


def solution(mesh):
    in_specs = (
        P("ep", None),
        P(),
        P(None, "tp"),
        P(None, "tp"),
        P(None, "tp"),
        P(None, "tp"),
        P("tp"),
        P("tp", None),
        P("ep", "tp", None, None),
        P("ep"),
        P(),
        P(),
        P("tp", "ep"),
        P("tp", "ep"),
        P("ep", "tp"),
        P("ep", None),
        P("ep", None),
        P("ep", None, "tp"),
        P("ep", None, "tp"),
        P("ep", "tp", None),
    )
    out_specs = (P("ep", "tp"), P("ep", "tp", None, None))
    return jax.shard_map(
        per_device, mesh=mesh, in_specs=in_specs, out_specs=out_specs, check_vma=False
    )
```

```python
import functools

import jax
import jax.numpy as jnp
import numpy as np
from jax import lax
from jax.experimental import pallas as pl
from jax.experimental.pallas import tpu as pltpu
from jax.sharding import PartitionSpec as P

EPSILON = 1e-06
THETA = 10000.0


def rms_norm(inputs, scaling):
    square = jnp.mean(inputs * inputs, axis=-1, keepdims=True)
    return inputs * lax.rsqrt(square + EPSILON) * scaling.astype(jnp.float32)


def state_kernel(
    state,
    key,
    value,
    final,
    new_state,
    out_ref,
    memory,
    key_ref,
    value_ref,
    final_ref,
    small_sem,
    load_sem,
    store_sem,
):
    seqs, heads, size, _ = memory.shape
    chunks = load_sem.shape[0]
    chunk = seqs // chunks
    smalls = [
        pltpu.make_async_copy(source, target, small_sem.at[index])
        for index, (source, target) in enumerate(
            ((key, key_ref), (value, value_ref), (final, final_ref))
        )
    ]
    loads = [
        pltpu.make_async_copy(
            state.at[pl.ds(c * chunk, chunk)], memory.at[pl.ds(c * chunk, chunk)], load_sem.at[c]
        )
        for c in range(chunks)
    ]
    stores = [
        pltpu.make_async_copy(
            memory.at[pl.ds(c * chunk, chunk)],
            new_state.at[pl.ds(c * chunk, chunk)],
            store_sem.at[c],
        )
        for c in range(chunks)
    ]
    for copy in smalls + loads:
        copy.start()
    decays = decays_of(heads, size)
    for copy in smalls:
        copy.wait()
    placed = pltpu.make_async_copy(final_ref, out_ref, small_sem.at[3])
    placed.start()
    keys = [key_ref[h] for h in range(heads)]
    for c in range(chunks):
        loads[c].wait()
        for s in range(c * chunk, (c + 1) * chunk):
            for h in range(heads):
                memory[s, h] = (
                    memory[s, h] * decays[h]
                    + keys[h][:, s : s + 1] * value_ref[s : s + 1, h * size : (h + 1) * size]
                )
        stores[c].start()
    placed.wait()
    for copy in stores:
        copy.wait()


def update_state(state, key, value, final):
    chunks = min(4, state.shape[0])
    anywhere = pl.BlockSpec(memory_space=pltpu.HBM)
    return pl.pallas_call(
        state_kernel,
        out_shape=(
            jax.ShapeDtypeStruct(state.shape, jnp.float32),
            jax.ShapeDtypeStruct(final.shape, final.dtype),
        ),
        in_specs=[anywhere] * 4,
        out_specs=(anywhere, anywhere),
        scratch_shapes=[
            pltpu.VMEM(state.shape, jnp.float32),
            pltpu.VMEM(key.shape, key.dtype),
            pltpu.VMEM(value.shape, value.dtype),
            pltpu.VMEM(final.shape, final.dtype),
            pltpu.SemaphoreType.DMA((4,)),
            pltpu.SemaphoreType.DMA((chunks,)),
            pltpu.SemaphoreType.DMA((chunks,)),
        ],
        compiler_params=pltpu.CompilerParams(vmem_limit_bytes=61 * 1024 * 1024),
        name="update_state",
    )(state, key, value, final)


def decays_of(heads, size):
    head_first = lax.axis_index("tp") * heads
    return [
        1.0 - jnp.exp2(-1.0 - 1.5 * jnp.full((1, size), head_first + h, jnp.int32).astype(jnp.float32))
        for h in range(heads)
    ]


def flip(index, mask):
    result = index
    bit = 1
    while bit <= mask:
        if mask & bit:
            result = result + bit * (1 - 2 * lax.rem(lax.div(index, bit), 2))
        bit *= 2
    return result


def layer_kernel(
    tp_count,
    ep_count,
    slots,
    key_scale,
    resid,
    norm_gain,
    positions,
    freq,
    head_gain,
    ffn_gain,
    w_mix,
    routes,
    route_weight,
    w_query,
    w_key,
    w_value,
    w_gate,
    state,
    w_output,
    dense_gate,
    dense_up,
    dense_down,
    expert_gate,
    expert_up,
    expert_down,
    out_ref,
    key_out,
    value_out,
    resid_ref,
    norm_ref,
    place_ref,
    freq_ref,
    head_ref,
    gain_ref,
    mix_ref,
    routes_ref,
    route_weight_ref,
    projections,
    memory,
    carried,
    kept,
    wo,
    wg,
    wu,
    wd,
    eg,
    eu,
    ed,
    scales,
    dispatch,
    combine,
    part,
    att_rx,
    middle,
    stat_tx,
    stat_rx,
    inverses,
    rows,
    hot,
    tokens,
    token_scale,
    gu_tx,
    gu_rx,
    gu_pair,
    gu_far,
    hidden,
    eh,
    er_tx,
    er_rx,
    er_pair,
    er_far,
    do_tx,
    do_rx,
    relay_tx,
    relay_rx,
    own_sum,
    mo_tx,
    mo_rx,
    fetch_sem,
    state_sem,
    load_sem,
    send_sem,
    recv_sem,
):
    me_t = lax.axis_index("tp")
    me_e = lax.axis_index("ep")
    seq_dev, model_width = resid_ref.shape
    width = model_width // tp_count
    f32 = jnp.float32
    bf16 = jnp.bfloat16

    fetches = [
        pltpu.make_async_copy(source, target, fetch_sem.at[index])
        for index, (source, target) in enumerate(
            (
                (resid, resid_ref),
                (norm_gain, norm_ref),
                (positions, place_ref),
                (freq, freq_ref),
                (head_gain, head_ref),
                (ffn_gain, gain_ref),
                (w_mix, mix_ref),
                (routes, routes_ref),
                (route_weight, route_weight_ref),
                (w_query, projections.at[0]),
                (w_key, projections.at[1]),
                (w_value, projections.at[2]),
                (w_gate, projections.at[3]),
            )
        )
    ]
    seqs, heads, size, _ = memory.shape
    chunks = state_sem.shape[0]
    chunk = seqs // chunks
    states = [
        pltpu.make_async_copy(
            state.at[pl.ds(c * chunk, chunk)], memory.at[pl.ds(c * chunk, chunk)], state_sem.at[c]
        )
        for c in range(chunks)
    ]
    loads = [
        pltpu.make_async_copy(source, target, load_sem.at[index])
        for index, (source, target) in enumerate(
            (
                (w_output, wo),
                (dense_gate, wg),
                (dense_up, wu),
                (expert_gate.at[0], eg),
                (expert_up.at[0], eu),
                (expert_down.at[0], ed),
                (dense_down, wd),
            )
        )
    ]
    for copy in fetches:
        copy.start()

    def ready(*indices):
        for index in indices:
            loads[index].wait()

    def peer_t(step):
        return flip(me_t, step)

    def peer_e(step):
        return flip(me_e, step)

    tp_steps = list(range(1, tp_count))
    ep_steps = list(range(ep_count - 1, 0, -1))
    barrier = pltpu.get_barrier_semaphore()
    for step in tp_steps:
        pl.semaphore_signal(
            barrier,
            inc=1,
            device_id=(me_e, peer_t(step)),
            device_id_type=pl.DeviceIdType.MESH,
        )
    for step in ep_steps:
        pl.semaphore_signal(
            barrier,
            inc=1,
            device_id=(peer_e(step), me_t),
            device_id_type=pl.DeviceIdType.MESH,
        )

    used = [0]
    started = []

    def send(source, target, device):
        index = used[0]
        used[0] = index + 1
        copy = pltpu.make_async_remote_copy(
            src_ref=source,
            dst_ref=target,
            send_sem=send_sem.at[index],
            recv_sem=recv_sem.at[index],
            device_id=device,
            device_id_type=pl.DeviceIdType.MESH,
        )
        copy.start()
        started.append(copy)
        return copy

    def span(index, size):
        return pl.ds(pl.multiple_of(index * size, size), size)

    def dot(left, right):
        return jnp.dot(left, right, preferred_element_type=f32)

    def arrive(copies):
        for copy in copies:
            copy.wait_recv()

    half = tp_count // 2
    sibling = peer_t(1)

    def cross(step):
        return 2 * step + step.bit_count() % 2

    def across(step):
        return peer_t(cross(step))

    def spread(at):
        return [
            send(at(me_t), at(me_t), (me_e, target))
            for target in [sibling] + [across(k) for k in range(1, half)]
        ]

    def pass_on(copies, at):
        waiting = [copies[0]]
        for k in range(1, half):
            arrive(copies[k : k + 1])
            waiting.append(send(at(across(k)), at(across(k)), (me_e, sibling)))
        return waiting

    own = span(me_t, width)
    for copy in fetches[:5]:
        copy.wait()
    for copy in states + loads[:1]:
        copy.start()
    normed = rms_norm(resid_ref[...].astype(f32), norm_ref[...].reshape(1, -1)).astype(bf16)
    places = jnp.broadcast_to(place_ref[...].astype(f32).reshape(1, seqs), (size, seqs)).T
    angles = places * freq_ref[...]
    cosine = jnp.cos(angles)
    lane_of = lax.broadcasted_iota(jnp.int32, (seqs, size), 1)
    sine = jnp.where(lane_of < size // 2, -jnp.sin(angles), jnp.sin(angles))

    def project(index):
        fetches[9 + index].wait()
        product = dot(normed, projections[index]).astype(bf16).astype(f32)
        return [product[:, h * size : (h + 1) * size] for h in range(heads)]

    def rotate(inputs):
        return inputs * cosine + pltpu.roll(inputs, size // 2, 1) * sine

    query = [rotate(piece) for piece in project(0)]
    query_t = [piece.T for piece in query]
    key = [rotate(piece) * key_scale for piece in project(1)]
    value = project(2)
    gating = project(3)
    decays = decays_of(heads, size)
    for h in range(heads):
        key_out[h] = key[h].T
        value_out[:, h * size : (h + 1) * size] = value[h]
    for c in range(chunks):
        states[c].wait()
        for q in range(c * chunk, (c + 1) * chunk):
            for h in range(heads):
                carried[h, q : q + 1, :] = jnp.sum(
                    memory[q, h] * query_t[h][:, q : q + 1], axis=0, keepdims=True
                )
    for load in loads[1:]:
        load.start()
    gains = head_ref[...].astype(f32).reshape(1, -1)
    for h in range(heads):
        within = jnp.sum(query[h] * key[h], axis=-1, keepdims=True) * value[h]
        mixture = within + carried[h] * decays[h]
        centre = jnp.mean(mixture, axis=-1, keepdims=True)
        variance = jnp.mean(jnp.square(mixture - centre), axis=-1, keepdims=True)
        columns = slice(h * size, (h + 1) * size)
        scaled = (mixture - centre) * lax.rsqrt(variance + EPSILON) * gains[:, columns]
        kept[:, columns] = (jax.nn.silu(gating[h]) * scaled).astype(bf16)
    ready(0)
    retained = kept[...]
    for d in tp_steps[1:] + tp_steps[:1] + [0]:
        part[d] = dot(retained, wo[:, span(peer_t(d), width)]).astype(bf16)
    pl.semaphore_wait(barrier, tp_count - 1 + ep_count - 1)
    att = [
        send(part.at[d], att_rx.at[d - 1], (me_e, peer_t(d)))
        for d in tp_steps[1:] + tp_steps[:1]
    ]
    for copy in fetches[5:9]:
        copy.wait()
    scales[0:1, :] = gain_ref[...].astype(f32).reshape(1, -1)
    scales[1:2, :] = mix_ref[...].astype(f32).reshape(1, -1)
    gain = scales[0:1, own]
    mix = scales[1:2, own]

    top_count = routes_ref.shape[0]
    expert_ids = lax.broadcasted_iota(jnp.int32, (ep_count, seq_dev), 0)
    taken = jnp.zeros((ep_count, seq_dev), f32)
    weight_of = jnp.zeros((ep_count, seq_dev), f32)
    for j in range(top_count):
        named = routes_ref[j : j + 1, :] == expert_ids
        taken = taken + jnp.where(named, 1.0, 0.0)
        weight_of = weight_of + jnp.where(
            named, route_weight_ref[j : j + 1, :].astype(f32), 0.0
        )
    earlier = lax.broadcasted_iota(jnp.int32, (seq_dev, seq_dev), 0)
    later = lax.broadcasted_iota(jnp.int32, (seq_dev, seq_dev), 1)
    ranks = dot(taken.astype(bf16), jnp.where(earlier < later, 1.0, 0.0).astype(bf16))
    slot_ids = lax.broadcasted_iota(jnp.int32, (slots, seq_dev), 0).astype(f32)
    for e in range(ep_count):
        hits = (ranks[e : e + 1, :] == slot_ids) & (taken[e : e + 1, :] > 0.0)
        dispatch[e] = jnp.where(hits, 1.0, 0.0).astype(bf16)
        combine[e * slots : (e + 1) * slots, :] = jnp.where(
            hits, weight_of[e : e + 1, :], 0.0
        ).astype(bf16)

    hots = [send(dispatch.at[peer_e(d)], hot.at[me_e], (peer_e(d), me_t)) for d in ep_steps]
    hot[me_e] = dispatch[me_e]
    arrive(att)
    total = part[0].astype(f32)
    for d in tp_steps:
        total = total + att_rx[d - 1].astype(f32)
    mid = resid_ref[:, own].astype(f32) + total
    scaled = mid * gain
    rows[me_e] = scaled.astype(bf16)
    sources = ep_count // 2
    near_steps = list(range(sources - 1, 0, -1))
    mirrored = send(rows.at[me_e], rows.at[me_e], (peer_e(sources), me_t))
    gathered = [send(rows.at[me_e], rows.at[me_e], (peer_e(d), me_t)) for d in near_steps]
    middle[...] = mid

    lane = lax.broadcasted_iota(jnp.int32, (seq_dev, 128), 1)
    diagonal = lane == lax.broadcasted_iota(jnp.int32, (seq_dev, 128), 0)

    def to_row(column):
        return jnp.sum(jnp.where(diagonal, column, 0.0), axis=0, keepdims=True)

    def to_column(row):
        return jnp.sum(jnp.where(diagonal, row, 0.0), axis=1, keepdims=True)

    stat_tx[0:1, :] = to_row(jnp.sum(mid * mid, axis=-1, keepdims=True))
    stat_tx[1:2, :] = to_row(jnp.sum(scaled * mix, axis=-1, keepdims=True))
    stats = [send(stat_tx, stat_rx.at[d - 1], (me_e, peer_t(d))) for d in tp_steps]
    arrive(stats)
    stat = stat_tx[0:2, :]
    for d in tp_steps:
        stat = stat + stat_rx[d - 1, 0:2, :]
    inverse = lax.rsqrt(stat[0:1, :] / model_width + EPSILON)
    mixing = to_column(jax.nn.sigmoid(inverse * stat[1:2, :]))
    inverses[me_e, 0:1, :] = inverse
    factors = [
        send(inverses.at[me_e], inverses.at[me_e], (peer_e(d), me_t)) for d in ep_steps
    ]

    side = lax.div(me_e, sources)
    sides = [side, 1 - side]
    core = lax.rem(sum(lax.div(me_t, 1 << bit) for bit in range(tp_count.bit_length() - 1)), 2)
    group_rows = sources * seq_dev
    share = group_rows // tp_count
    owners = share // seq_dev
    pair_of = lax.div(me_t, 2)

    def fill_tokens(g):
        for i in range(sources):
            s = sides[g] * sources + i
            tokens[me_t, span(s, slots), :] = dot(hot[s], rows[s]).astype(bf16)
        place = span(sides[g], sources * slots)
        return spread(lambda index: tokens.at[index, place, :])

    def gate_up(g):
        group = rows[pl.ds(sides[g] * sources, sources)].reshape(group_rows, width)
        for which, weight in enumerate((wg, wu)):
            if g == 0:
                ready(1 + which)
            product = lax.dot_general(
                group, weight[...], (((1,), (1,)), ((), ())), preferred_element_type=f32
            ).astype(bf16)
            for t in range(tp_count):
                gu_tx[g, t.bit_count() % 2, t // 2, which] = product[t * share : (t + 1) * share]
        return send(gu_tx.at[g, 1 - core], gu_rx.at[g], (me_e, sibling))

    def pair_up(g, near):
        arrive([near])
        sent = []
        for k in range(1, half):
            p = flip(pair_of, k)
            gu_pair[g, k - 1] = (
                gu_tx[g, core, p].astype(f32) + gu_rx[g, p].astype(f32)
            ).astype(bf16)
            sent.append(send(gu_pair.at[g, k - 1], gu_far.at[g, k - 1], (me_e, across(k))))
        return sent

    def activate(g, far):
        arrive(far)
        factor = jnp.concatenate(
            [
                to_column(inverses[sides[g] * sources + me_t * owners + i, 0:1, :])
                for i in range(owners)
            ],
            axis=0,
        )
        total = gu_tx[g, core, pair_of].astype(f32) + gu_rx[g, pair_of].astype(f32)
        for k in range(1, half):
            total = total + gu_far[g, k - 1].astype(f32)
        hidden[g, me_t] = (jax.nn.silu(total[0] * factor) * (total[1] * factor)).astype(bf16)
        return spread(lambda index: hidden.at[g, index])

    def share_hidden(g, hids):
        return pass_on(hids, lambda index: hidden.at[g, index])

    def lower(g, hids):
        arrive(hids)
        product = dot(hidden[g].reshape(group_rows, hidden.shape[-1]), wd[...])
        do_tx[g] = product.astype(bf16).reshape(sources, seq_dev, width)
        return [
            send(
                do_tx.at[g, lax.rem(peer_e(d), sources)],
                do_rx.at[g, d - 1],
                (peer_e(d), me_t),
            )
            for d in near_steps
        ]

    def forward(copies, g):
        place = span(sides[g], sources * slots)
        return pass_on(copies, lambda index: tokens.at[index, place, :])

    arrive([mirrored])
    mirror = peer_e(sources)
    passed = [send(rows.at[mirror], rows.at[mirror], (peer_e(d), me_t)) for d in near_steps]
    arrive(hots)
    arrive(gathered)
    toks = fill_tokens(0)
    near_0 = gate_up(0)
    far_0 = pair_up(0, near_0)
    arrive(passed)
    toks_far = fill_tokens(1)
    near_1 = gate_up(1)
    toks = forward(toks, 0)
    far_1 = pair_up(1, near_1)
    arrive(factors)
    hid_0 = activate(0, far_0)
    for s in range(ep_count):
        token_scale[s * slots : (s + 1) * slots, :] = jnp.sum(
            hot[s].astype(f32) * inverses[s, 0:1, 0:seq_dev], axis=1, keepdims=True
        )
    toks_far = forward(toks_far, 1)
    hid_1 = activate(1, far_1)
    ready(3, 4)
    arrive(toks + toks_far)
    tile = min(256, eg.shape[1])

    def expert_tile(index, carry):
        columns = span(index, tile)
        gate = jnp.zeros((tokens.shape[1], tile), f32)
        up = jnp.zeros((tokens.shape[1], tile), f32)
        for c in range(tp_count):
            features = slice(c * width, (c + 1) * width)
            gate = gate + dot(tokens[c], eg[features, columns])
            up = up + dot(tokens[c], eu[features, columns])
        factor = token_scale[...]
        eh[:, columns] = (jax.nn.silu(gate * factor) * (up * factor)).astype(bf16)
        return carry

    lax.fori_loop(0, eg.shape[1] // tile, expert_tile, 0)
    hid_0 = share_hidden(0, hid_0)
    ready(5)
    pairs = []
    for k in range(half):
        target = flip(sibling, cross(k))
        er_tx[k] = dot(eh[...], ed[:, span(target, width)]).astype(bf16)
        pairs.append(send(er_tx.at[k], er_rx.at[k], (me_e, sibling)))
    ready(6)
    outs = lower(0, hid_0)
    hid_1 = share_hidden(1, hid_1)
    partials = [[], []]
    slot_places = [span(sides[g], sources * slots) for g in range(2)]
    for k in range(1, half):
        target = across(k)
        summed = dot(eh[...], ed[:, span(target, width)])
        arrive(pairs[k : k + 1])
        er_pair[k - 1] = (summed + er_rx[k].astype(f32)).astype(bf16)
        for g in (1, 0):
            at = slot_places[g]
            partials[g].append(
                send(er_pair.at[k - 1, at], er_far.at[k - 1, at], (me_e, target))
            )
    outs_far = lower(1, hid_1)
    result = dot(eh[...], ed[:, own])
    arrive(pairs[:1])
    own_sum[...] = result + er_rx[0].astype(f32)
    arrive(outs_far)
    relayed = do_tx[1, lax.rem(me_e, sources)].astype(f32)
    for d in near_steps:
        relayed = relayed + do_rx[1, d - 1].astype(f32)
    relay_tx[...] = relayed.astype(bf16)
    outs.append(send(relay_tx, relay_rx, (peer_e(sources), me_t)))
    place = span(me_e, slots)
    backs = []
    for g in (1, 0):
        arrive(partials[g])
        at = slot_places[g]
        result = own_sum[at, :]
        for k in range(1, half):
            result = result + er_far[k - 1, at].astype(f32)
        mo_tx[at, :] = result.astype(bf16)
        steps = near_steps if g == 0 else list(range(ep_count - 1, sources - 1, -1))
        backs += [
            send(mo_tx.at[span(peer_e(d), slots), :], mo_rx.at[place, :], (peer_e(d), me_t))
            for d in steps
        ]
    mo_rx[place, :] = mo_tx[place, :]
    arrive(outs)
    dense = do_tx[0, lax.rem(me_e, sources)].astype(f32) + relay_rx[...].astype(f32)
    for d in near_steps:
        dense = dense + do_rx[0, d - 1].astype(f32)
    partly = middle[...] + mixing * dense
    arrive(backs)
    returned = lax.dot_general(
        combine[...], mo_rx[...], (((0,), (0,)), ((), ())), preferred_element_type=f32
    )
    out_ref[...] = (partly + returned).astype(bf16)
    for copy in started:
        copy.wait_send()


def layer(smalls, slots, projections, state, weights, tp_count, ep_count):
    seq_dev, model_width = smalls[0].shape
    _, heads, size, _ = state.shape
    chunks = min(2, seq_dev)
    width = model_width // tp_count
    batch = seq_dev * ep_count
    share = batch // 2 // tp_count
    dense_units = weights[1].shape[0]
    half = tp_count // 2
    expert_units = weights[4].shape[2]
    items = ep_count * slots
    bf16 = jnp.bfloat16
    f32 = jnp.float32
    peers_t = tp_count - 1
    peers_e = ep_count - 1
    copies = 3 * peers_t + 5 * peers_e + 2 * (2 * (2 * half - 1) + half) + 3 * half
    vmem = pl.BlockSpec(memory_space=pltpu.VMEM)
    anywhere = pl.BlockSpec(memory_space=pltpu.HBM)
    return pl.pallas_call(
        functools.partial(layer_kernel, tp_count, ep_count, slots, size ** (-0.5)),
        out_shape=(
            jax.ShapeDtypeStruct((seq_dev, width), bf16),
            jax.ShapeDtypeStruct((heads, size, seq_dev), f32),
            jax.ShapeDtypeStruct((seq_dev, heads * size), f32),
        ),
        in_specs=[anywhere] * 21,
        out_specs=(vmem, vmem, vmem),
        scratch_shapes=[
            *[pltpu.VMEM(small.shape, small.dtype) for small in smalls],
            pltpu.VMEM((4,) + projections[0].shape, bf16),
            pltpu.VMEM(state.shape, f32),
            pltpu.VMEM((heads, seq_dev, size), f32),
            pltpu.VMEM((seq_dev, heads * size), bf16),
            pltpu.VMEM(weights[0].shape, bf16),
            pltpu.VMEM(weights[1].shape, bf16),
            pltpu.VMEM(weights[2].shape, bf16),
            pltpu.VMEM(weights[3].shape, bf16),
            pltpu.VMEM(weights[4].shape[1:], bf16),
            pltpu.VMEM(weights[5].shape[1:], bf16),
            pltpu.VMEM(weights[6].shape[1:], bf16),
            pltpu.VMEM((8, model_width), f32),
            pltpu.VMEM((ep_count, slots, seq_dev), bf16),
            pltpu.VMEM((items, seq_dev), bf16),
            pltpu.VMEM((tp_count, seq_dev, width), bf16),
            pltpu.VMEM((peers_t, seq_dev, width), bf16),
            pltpu.VMEM((seq_dev, width), f32),
            pltpu.VMEM((8, 128), f32),
            pltpu.VMEM((peers_t, 8, 128), f32),
            pltpu.VMEM((ep_count, 8, 128), f32),
            pltpu.VMEM((ep_count, seq_dev, width), bf16),
            pltpu.VMEM((ep_count, slots, seq_dev), bf16),
            pltpu.VMEM((tp_count, items, width), bf16),
            pltpu.VMEM((items, 1), f32),
            pltpu.VMEM((2, 2, half, 2, share, dense_units), bf16),
            pltpu.VMEM((2, half, 2, share, dense_units), bf16),
            pltpu.VMEM((2, half - 1, 2, share, dense_units), bf16),
            pltpu.VMEM((2, half - 1, 2, share, dense_units), bf16),
            pltpu.VMEM((2, tp_count, share, dense_units), bf16),
            pltpu.VMEM((items, expert_units), bf16),
            pltpu.VMEM((half, items, width), bf16),
            pltpu.VMEM((half, items, width), bf16),
            pltpu.VMEM((half - 1, items, width), bf16),
            pltpu.VMEM((half - 1, items, width), bf16),
            pltpu.VMEM((2, ep_count // 2, seq_dev, width), bf16),
            pltpu.VMEM((2, ep_count // 2 - 1, seq_dev, width), bf16),
            pltpu.VMEM((seq_dev, width), bf16),
            pltpu.VMEM((seq_dev, width), bf16),
            pltpu.VMEM((items, width), f32),
            pltpu.VMEM((items, width), bf16),
            pltpu.VMEM((items, width), bf16),
            pltpu.SemaphoreType.DMA((13,)),
            pltpu.SemaphoreType.DMA((chunks,)),
            pltpu.SemaphoreType.DMA((7,)),
            pltpu.SemaphoreType.DMA((copies,)),
            pltpu.SemaphoreType.DMA((copies,)),
        ],
        compiler_params=pltpu.CompilerParams(
            collective_id=0, has_side_effects=True, vmem_limit_bytes=61 * 1024 * 1024
        ),
        name="layer",
    )(*smalls, *projections, state, *weights)


def per_device(
    resid,
    norm_gain,
    w_query,
    w_key,
    w_value,
    w_gate,
    head_gain,
    w_output,
    state,
    positions,
    ffn_gain,
    w_mix,
    dense_gate,
    dense_up,
    dense_down,
    routes,
    route_weight,
    expert_gate,
    expert_up,
    expert_down,
):
    seq_dev = resid.shape[0]
    tp_count = lax.axis_size("tp")
    ep_count = lax.axis_size("ep")
    half = state.shape[-1] // 2
    inverse = THETA ** (-np.arange(half, dtype=np.float64) / half)
    freq = jnp.asarray(np.concatenate([inverse, inverse])[None, :].astype(np.float32))
    capacity = max(2, 2 * seq_dev * routes.shape[1] // ep_count)
    slots = -(-capacity // 16) * 16
    final, key, value = layer(
        (
            resid,
            norm_gain,
            positions,
            freq,
            head_gain,
            ffn_gain,
            w_mix,
            routes.T,
            route_weight.T,
        ),
        slots,
        (w_query, w_key, w_value, w_gate),
        state,
        (w_output, dense_gate.T, dense_up.T, dense_down, expert_gate, expert_up, expert_down),
        tp_count,
        ep_count,
    )
    new_state, final = update_state(state, key, value, final)
    return (final, new_state)


def solution(mesh):
    in_specs = (
        P("ep", None),
        P(),
        P(None, "tp"),
        P(None, "tp"),
        P(None, "tp"),
        P(None, "tp"),
        P("tp"),
        P("tp", None),
        P("ep", "tp", None, None),
        P("ep"),
        P(),
        P(),
        P("tp", "ep"),
        P("tp", "ep"),
        P("ep", "tp"),
        P("ep", None),
        P("ep", None),
        P("ep", None, "tp"),
        P("ep", None, "tp"),
        P("ep", "tp", None),
    )
    out_specs = (P("ep", "tp"), P("ep", "tp", None, None))
    return jax.shard_map(
        per_device, mesh=mesh, in_specs=in_specs, out_specs=out_specs, check_vma=False
    )
```
